32 devices in a mesh: fs: 8 (over z, y), tp: 4 (over x, core).
Axes of the slice: x: 2, y: 2, z: 4, core: 2. Of those that a mesh axis runs over, the one named last changes fastest.
Arguments:
- later_input: bfloat16 [4096, 2048], P(('fs', 'tp')), may hold values from -6 to 6
- earlier_input: bfloat16 [4096, 2048], P('fs'), may hold values from -6 to 6
- earlier_hidden: bfloat16 [4096, 4096], P('fs', 'tp'), may hold values from -6 to 6
- cotangent: bfloat16 [4096, 2048], P('fs'), may hold values from -6 to 6
- up_weight: bfloat16 [2048, 4096], P('fs', 'tp'), may hold values from -0.125 to 0.125
- down_weight: bfloat16 [4096, 2048], P(('tp', 'fs')), may hold values from -0.09375 to 0.09375
- up_sum: float32 [2048, 4096], P('fs', 'tp'), may hold values from -4 to 4
- down_sum: float32 [4096, 2048], P(('tp', 'fs')), may hold values from -4 to 4
Outputs:
- later_output: bfloat16 [4096, 2048], P(('fs', 'tp'))
- later_hidden: bfloat16 [4096, 4096], P('fs', 'tp')
- earlier_grad: bfloat16 [4096, 2048], P(('fs', 'tp'))
- up_sum_next: float32 [2048, 4096], P('fs', 'tp')
- down_sum_next: float32 [4096, 2048], P(('tp', 'fs'))
The draws below stay inside these ranges and needn't reach their ends.
All inputs are finite; a program needn't handle non-finite values.
Results may differ from the reference program's by a relative error of at most 0.0095.
Values may be sent and summed in bfloat16 or wider, within the bound.
A program may use at most 128 MiB of HBM per device.

```python
import jax
import jax.numpy as jnp
from jax import lax

D = 2048
FF = 4096
TOKENS = 4096
N_FS = 8
N_TP = 4


def spiked(entries, key, source, target, shards_of, factor):
    owner, partner = [(jnp.arange(entries.shape[dim]) // (entries.shape[dim] // shards_of)).reshape([-1 if axis == dim else 1 for axis in range(entries.ndim)]) for dim in (source, target)]
    chosen = jax.random.permutation(key, shards_of)[partner]
    strong = (owner == chosen) | (owner == (partner + shards_of // 2) % shards_of)
    return jnp.where(strong, factor * entries, entries)


def shard_levels(key, shape, split, low, largest):
    loudness = 1.0
    for dim, blocks in split:
        heights = jax.random.uniform(jax.random.fold_in(jax.random.fold_in(key, 6), dim), (blocks,), jnp.float32, low / len(split), largest / len(split))
        loudness = loudness * jnp.repeat(jnp.exp(heights), shape[dim] // blocks).reshape((-1,) + (1,) * (len(shape) - 1 - dim))
    return loudness


def scatter_about(key, shape, deviation, reach, split=(), held_as=jnp.bfloat16):
    entries = jax.random.normal(key, shape, jnp.float32) * deviation
    if len(split) > 0:
        entries = shard_levels(key, shape, split, -0.22, 0.18) * entries
    return jnp.clip(entries, min=-reach, max=reach).astype(held_as)


def heavy_noise(own_key, shape, scale, reach, cuts, heavy, kind=jnp.bfloat16):
    array = scale * jax.random.normal(own_key, shape, jnp.float32)
    if cuts:
        array = array * shard_levels(own_key, shape, cuts, -0.22, 0.18)
    return jnp.clip(spiked(array, jax.random.fold_in(own_key, 3), *heavy), -reach, reach).astype(kind)


def setup_inputs(seed: int = 0) -> dict:
    arg_keys = jax.random.split(jax.random.key(seed), 9)
    later_input = scatter_about(arg_keys[0], (TOKENS, D), 1.0, 6.0, ((0, 32),))
    earlier_input = heavy_noise(arg_keys[1], (TOKENS, D), 1.0, 6.0, ((0, 8),), (0, 1, 8, 2.0))
    earlier_hidden = scatter_about(arg_keys[2], (TOKENS, FF), 1.0, 6.0, ((0, 8), (1, 4)))
    cotangent = heavy_noise(arg_keys[3], (TOKENS, D), 1.0, 6.0, ((0, 8),), (0, 1, 8, 2.0))
    up_weight = scatter_about(arg_keys[4], (D, FF), D ** -0.5, 0.125, ((0, 8), (1, 4)))
    down_weight = scatter_about(arg_keys[5], (FF, D), FF ** -0.5, 0.09375, ((0, 32),))
    up_sum = scatter_about(arg_keys[6], (D, FF), 0.5, 4.0, ((0, 8), (1, 4)), jnp.float32)
    down_sum = scatter_about(arg_keys[7], (FF, D), 0.5, 4.0, ((0, 32),), jnp.float32)
    return dict(later_input=later_input, earlier_input=earlier_input, earlier_hidden=earlier_hidden, cotangent=cotangent, up_weight=up_weight, down_weight=down_weight, up_sum=up_sum, down_sum=down_sum)


def squared_relu(pre_values):
    lifted = jnp.maximum(pre_values.astype(jnp.float32), 0.0)
    return lifted, lifted * lifted


def rounded_split_sum(left_rows, right_rows):
    span_width = left_rows.shape[1] // N_TP
    running = jnp.zeros((left_rows.shape[0], right_rows.shape[1]), jnp.float32)
    for block_index in range(N_TP):
        lower_edge = block_index * span_width
        upper_edge = lower_edge + span_width
        partial_value = jnp.dot(left_rows[:, lower_edge:upper_edge], right_rows[lower_edge:upper_edge],
                          preferred_element_type=jnp.float32)
        rounded = lax.optimization_barrier(partial_value.astype(jnp.bfloat16))
        running = running + rounded.astype(jnp.float32)
    return running.astype(jnp.bfloat16)


def reference(later_input, earlier_input, earlier_hidden, cotangent, up_weight, down_weight, up_sum, down_sum):
    later_hidden = jnp.dot(later_input, up_weight, preferred_element_type=jnp.float32).astype(jnp.bfloat16)
    lifted_later, squared_later = squared_relu(later_hidden)
    later_output = rounded_split_sum(squared_later.astype(jnp.bfloat16), down_weight)
    row_total = earlier_input.shape[0]
    grad_scale = float(row_total) ** -0.5
    group_rows = row_total // N_FS

    def backward_block(totals, pieces):
        inputs, hidden, upstream = pieces
        lifted, squared = squared_relu(hidden)
        activation = squared.astype(jnp.bfloat16)
        act_slope = jnp.dot(upstream, down_weight.T, preferred_element_type=jnp.float32)
        pre_grad = (2.0 * act_slope * lifted).astype(jnp.bfloat16)
        up_total = totals[0] + jnp.dot(inputs.T, pre_grad, preferred_element_type=jnp.float32)
        down_total = totals[1] + jnp.dot(activation.T, upstream, preferred_element_type=jnp.float32)
        return (up_total, down_total), rounded_split_sum(pre_grad, up_weight.T)

    stacked = (earlier_input.reshape(N_FS, group_rows, -1),
               earlier_hidden.reshape(N_FS, group_rows, -1),
               cotangent.reshape(N_FS, group_rows, -1))
    initial = (jnp.zeros(up_weight.shape, jnp.float32), jnp.zeros(down_weight.shape, jnp.float32))
    (up_total, down_total), grads = lax.scan(backward_block, initial, stacked)
    earlier_grad = grads.reshape(row_total, -1)
    return (later_output, later_hidden, earlier_grad,
            up_sum + grad_scale * up_total, down_sum + grad_scale * down_total)
```

```python
import functools

import jax
import jax.numpy as jnp
from jax import lax
from jax.experimental import pallas as pl
from jax.experimental.pallas import tpu as pltpu
from jax.sharding import PartitionSpec as P

F32, BF16 = jnp.float32, jnp.bfloat16
MESH = pl.DeviceIdType.MESH
LANES = 128
VMEM_BYTES = 67_043_328


def dot(a, b, ca=1, cb=0):
    return lax.dot_general(a, b, (((ca,), (cb,)), ((), ())), preferred_element_type=F32)


def loop(n, body):
    def step(i, carry):
        body(i)
        return carry

    lax.fori_loop(0, n, step, 0)


def squared(h):
    lifted = jnp.maximum(h.astype(F32), 0.0)
    return (lifted * lifted).astype(BF16)


def both(a, b):
    return jnp.logical_and(a, b)


class Wire:
    def __init__(self, send, recv, local):
        self.send, self.recv, self.local = send, recv, local
        self.n_remote = self.n_local = 0
        self.open = []

    def slot(self):
        self.n_remote += 1
        return self.n_remote - 1

    def remote(self, src, dst, device, slot=None):
        i = self.slot() if slot is None else slot
        return pltpu.make_async_remote_copy(
            src_ref=src, dst_ref=dst, send_sem=self.send.at[i], recv_sem=self.recv.at[i],
            device_id=device, device_id_type=MESH,
        )

    def start(self, copy, when=None):
        if when is None:
            copy.start()
        else:
            pl.when(when)(copy.start)
        self.open.append((copy, when))

    def copy(self, src, dst):
        i = self.n_local
        self.n_local += 1
        made = pltpu.make_async_copy(src, dst, self.local.at[i])
        made.start()
        return made

    def drain(self):
        for copy, when in self.open:
            if when is None:
                copy.wait_send()
            else:
                pl.when(when)(copy.wait_send)


class Line:
    def __init__(self, wire, full, rows, own, z, n, left, right):
        self.wire, self.z, self.n = wire, z, n
        self.right, self.left = {}, {}

        def block(i):
            return full.at[pl.ds(pl.multiple_of(lax.rem(i + n, n) * rows, rows), rows)]

        for r in range(1, n):
            src = own if r == 1 else block(z - r + 1)
            self.right[r] = wire.remote(src, block(z - r + 1), right)
            src = own if r == 1 else block(z + r - 1)
            self.left[r] = wire.remote(src, block(z + r - 1), left)

    def begin(self):
        self.wire.start(self.right[1], self.z < self.n - 1)
        self.wire.start(self.left[1], self.z > 0)

    def wave(self, r):
        z, n = self.z, self.n
        pl.when(z >= r)(self.right[r].wait_recv)
        if r < n - 1:
            self.wire.start(self.right[r + 1], both(z >= r, z < n - 1))
        pl.when(z <= n - 1 - r)(self.left[r].wait_recv)
        if r < n - 1:
            self.wire.start(self.left[r + 1], both(z <= n - 1 - r, z > 0))


class Sums:
    def __init__(self, wire, part, inbox, relayed, rows, z, n, left, right):
        self.wire, self.part, self.inbox, self.relayed = wire, part, inbox, relayed
        self.rows, self.z, self.n = rows, z, n
        self.seed, self.pass_on = {}, {}
        for way, device in ((0, right), (1, left)):
            for m in range(n - 1):
                slot = wire.slot()
                dst = inbox.at[way, m]
                self.seed[way, m] = wire.remote(part.at[self.span(way, m)], dst, device, slot)
                if m < n - 2:
                    self.pass_on[way, m] = wire.remote(relayed.at[way, m], dst, device, slot)

    def span(self, way, m, lo=0, size=None):
        ahead = self.z + 1 + m if way == 0 else self.z - 1 - m
        base = lax.rem(ahead + 2 * self.n, self.n) * self.rows
        size = self.rows if size is None else size
        return pl.ds(pl.multiple_of(base + lo, size), size)

    def seeds(self, ms):
        for m in ms:
            self.wire.start(self.seed[0, m], self.z == 0)
            self.wire.start(self.seed[1, m], self.z == self.n - 1)

    def relay(self, m):
        z, n = self.z, self.n
        tile = self.rows // 4
        for way in (0, 1):
            if way == 0:
                when = both(z >= 1, z + 1 + m <= n - 1)
            else:
                when = both(z <= n - 2, z - 1 - m >= 0)

            def add(way=way):
                self.seed[way, m + 1].wait_recv()

                def body(i):
                    lo = pl.multiple_of(i * tile, tile)
                    mine = self.part[self.span(way, m, lo, tile), :].astype(F32)
                    came = self.inbox[way, m + 1, pl.ds(lo, tile), :].astype(F32)
                    self.relayed[way, m, pl.ds(lo, tile), :] = (mine + came).astype(BF16)

                loop(4, body)

            pl.when(when)(add)
            self.wire.start(self.pass_on[way, m], when)

    def final(self, out, order, tile):
        z, n = self.z, self.n
        pl.when(z >= 1)(self.seed[0, 0].wait_recv)
        pl.when(z <= n - 2)(self.seed[1, 0].wait_recv)
        up, down = (z >= 1).astype(F32), (z <= n - 2).astype(F32)
        base = z * self.rows

        def body(i):
            lo = pl.multiple_of(order(i) * tile, tile)
            rows = pl.ds(lo, tile)
            mine = self.part[pl.ds(pl.multiple_of(base + lo, tile), tile), :].astype(F32)
            first = jnp.where(z >= 1, self.inbox[0, 0, rows, :].astype(F32), 0.0)
            second = jnp.where(z <= n - 2, self.inbox[1, 0, rows, :].astype(F32), 0.0)
            out[rows, :] = mine + first + second

        loop(self.rows // tile, body)


class Plane:
    def __init__(self, wire, bufs, k, at, peers):
        part, in_a, to_b, in_b, to_c, in_c = (buf.at[k] for buf in bufs)
        self.part, self.in_a, self.to_b, self.in_b, self.to_c, self.in_c = (
            part, in_a, to_b, in_b, to_c, in_c
        )
        self.wire, self.at = wire, at
        x, y, c = at
        self.a = wire.remote(part.at[1 - c], in_a, peers[2])
        self.b = wire.remote(to_b, in_b, peers[0])
        self.c = wire.remote(to_c, in_c, peers[1])

    def begin(self):
        self.wire.start(self.a)

    def second(self):
        x, y, c = self.at
        self.a.wait_recv()
        for j in (0, 1):
            total = self.part[c, 1 - x, j].astype(F32) + self.in_a[1 - x, j].astype(F32)
            self.to_b[j] = total.astype(BF16)
        self.wire.start(self.b)

    def mine(self, j):
        x, y, c = self.at
        return (
            self.part[c, x, j].astype(F32) + self.in_a[x, j].astype(F32) + self.in_b[j].astype(F32)
        )

    def third(self):
        x, y, c = self.at
        self.b.wait_recv()
        self.to_c[...] = self.mine(1 - y).astype(BF16)
        self.wire.start(self.c)

    def last(self, out, columns):
        x, y, c = self.at
        self.c.wait_recv()
        out[:, columns] = (self.mine(y) + self.in_c[...].astype(F32)).astype(BF16)


def layer(
    n, later_in, earlier_in, hidden, cot, up, down,
    out_o, lh_o, eg_o, gu_o, gd_o,
    c_all, e_all, x_all, h_all, act_t, pg, up_full, down_full, gd_part, gu_part,
    gd_in, gd_relay, gu_in, gu_relay, swap_out, swap_in, lh, act_l,
    part, in_a, to_b, in_b, to_c, in_c, eg_fin, out_fin, gd_fin, gu_fin, gu_out,
    send, recv, local,
):
    fs, tp = lax.axis_index("fs"), lax.axis_index("tp")
    z, y = fs // 2, fs % 2
    x, c = tp // 2, tp % 2
    py, px, pc = (fs + 1 - 2 * y, tp), (fs, tp + 2 - 4 * x), (fs, tp + 1 - 2 * c)
    left, right = (lax.rem(fs + 2 * n - 2, 2 * n), tp), (lax.rem(fs + 2, 2 * n), tp)

    group, width = earlier_in.shape
    block = later_in.shape[0]
    hb = down.shape[0]
    half = n * hb
    up_rows = up.shape[0]
    chunk = 2 * up_rows
    wire = Wire(send, recv, local)

    def cols(i, parity):
        return pl.ds(pl.multiple_of((2 * i + parity) * hb, hb), hb)

    def strip(i):
        return pl.ds(i * hb, hb)

    def rows_of(parity, q):
        return pl.ds(pl.multiple_of(parity * group + q * block, block), block)

    def half_of(parity):
        return pl.ds(pl.multiple_of(parity * group, group), group)

    barrier = pltpu.get_barrier_semaphore()

    def greet(device):
        pl.semaphore_signal(barrier, inc=1, device_id=device, device_id_type=MESH)

    for device in (py, px, pc):
        greet(device)
    pl.when(z > 0)(lambda: greet(left))
    pl.when(z < n - 1)(lambda: greet(right))

    own_h = [wire.copy(hidden.at[:, cols(i, y)], h_all.at[half_of(y), strip(i)]) for i in range(n)]
    my_rows = pl.ds(pl.multiple_of(fs * up_rows, up_rows), up_rows)
    own_up = [wire.copy(up.at[:, cols(i, y)], up_full.at[my_rows, strip(i)]) for i in range(n)]
    own_c = wire.copy(cot, c_all.at[half_of(y)])
    own_down = wire.copy(down, down_full.at[pl.ds(pl.multiple_of(z * hb, hb), hb)])
    own_e = wire.copy(earlier_in, e_all.at[half_of(y)])
    own_x = wire.copy(later_in, x_all.at[rows_of(y, tp)])

    pl.semaphore_wait(barrier, 3 + (z > 0).astype(jnp.int32) + (z < n - 1).astype(jnp.int32))

    def spread(whole, source, src_rows):
        there = whole.at[rows_of(y, tp)]
        came = whole.at[rows_of(1 - y, tp)]
        beside = whole.at[rows_of(1 - y, tp + 2 - 4 * x)]
        return (
            wire.remote(source.at[src_rows], there, py),
            wire.remote(came, came, px),
            wire.remote(came, came, pc),
            wire.remote(beside, beside, pc),
        )

    quarter = pl.ds(pl.multiple_of(tp * block, block), block)
    downs = Line(wire, down_full, hb, down, z, n, left, right)
    up_block = up_full.at[pl.ds(pl.multiple_of(z * chunk, chunk), chunk)]
    ups = Line(wire, up_full, chunk, up_block, z, n, left, right)
    c_y, c_x, c_c, c_xc = spread(c_all, cot, quarter)
    e_y, e_x, e_c, e_xc = spread(e_all, earlier_in, quarter)
    x_y, x_x, x_c, x_xc = spread(x_all, later_in, pl.ds(0, block))
    mine_x = x_all.at[rows_of(y, tp)]
    beside_x = x_all.at[rows_of(y, tp + 2 - 4 * x)]
    x_own_x = wire.remote(later_in, mine_x, px)
    x_own_c = wire.remote(later_in, mine_x, pc)
    x_own_xc = wire.remote(beside_x, beside_x, pc)
    up_y = [
        wire.remote(up.at[:, cols(i, 1 - y)], up_full.at[my_rows, strip(i)], py) for i in range(n)
    ]
    h_y = [
        wire.remote(hidden.at[:, cols(i, 1 - y)], h_all.at[half_of(y), strip(i)], py)
        for i in range(n)
    ]

    downs.begin()
    wire.start(c_y)
    for copy in up_y + h_y:
        wire.start(copy)
    wire.start(e_y)
    wire.start(x_y)
    wire.start(x_own_x)
    wire.start(x_own_c)

    gds = Sums(wire, gd_part, gd_in, gd_relay, hb, z, n, left, right)
    gus = Sums(wire, gu_part, gu_in, gu_relay, chunk, z, n, left, right)
    bufs = (part, in_a, to_b, in_b, to_c, in_c)
    planes = [Plane(wire, bufs, k, (x, y, c), (px, py, pc)) for k in range(2 * n)]
    egs, outs = planes[:n], planes[n:]

    def activate(parity):
        def body(i):
            rows = rows_of(parity, i)
            act_t[:, rows] = squared(h_all[rows, :]).T

        loop(group // block, body)

    for copy in own_h:
        copy.wait()
    activate(y)

    downs.wave(1)
    c_y.wait_recv()
    wire.start(c_x)
    wire.start(c_c)
    for copy in own_up:
        copy.wait()
    for copy in up_y:
        copy.wait_recv()
    ups.begin()
    if n > 2:
        downs.wave(2)
    c_x.wait_recv()
    wire.start(c_xc)
    for copy in h_y:
        copy.wait_recv()
    activate(1 - y)
    c_c.wait_recv()
    c_xc.wait_recv()
    own_c.wait()

    tile = min(256, chunk)

    def gd_body(i):
        columns = pl.ds(pl.multiple_of(i * tile, tile), tile)
        gd_part[:, columns] = dot(act_t[...], c_all[:, columns]).astype(BF16)

    loop(width // tile, gd_body)
    gds.seeds(range(n - 2, 0, -1))

    for r in range(3, n):
        downs.wave(r)
    own_down.wait()

    slope_rows = min(256, 2 * group)

    def pg_body(i):
        rows = pl.ds(pl.multiple_of(i * slope_rows, slope_rows), slope_rows)
        lifted = jnp.maximum(h_all[rows, :].astype(F32), 0.0)
        pg[rows, :] = (2.0 * dot(c_all[rows, :], down_full[...], 1, 1) * lifted).astype(BF16)

    loop(2 * group // slope_rows, pg_body)

    e_y.wait_recv()
    wire.start(e_x)
    wire.start(e_c)

    def store_part(k, parity, value):
        for q in range(4):
            part[k, q % 2, q // 2, parity] = value[q * block : (q + 1) * block].astype(BF16)

    def column_block(k):
        where = 0
        for i in range(n):
            order = sorted(range(n), key=lambda b: (abs(b - i), b))
            where = where + jnp.where(z == i, order[k], 0)
        return pl.ds(pl.multiple_of(where * chunk, chunk), chunk)

    def eg_chunk(k):
        wide = column_block(k)

        def body(parity):
            store_part(k, parity, dot(pg[half_of(parity), :], up_full[wide, :], 1, 1))

        loop(2, body)
        egs[k].begin()

    def out_chunk(k):
        wide = pl.ds(k * chunk, chunk)

        def body(parity):
            store_part(n + k, parity, dot(act_l[half_of(parity), :], down_full[:, wide]))

        loop(2, body)
        outs[k].begin()

    eg_chunk(0)
    for m in range(n - 3, 0, -1):
        gds.relay(m)
    ups.wave(1)
    egs[0].second()
    eg_chunk(1)
    e_x.wait_recv()
    wire.start(e_xc)
    e_c.wait_recv()
    e_xc.wait_recv()
    own_e.wait()

    def gu_body(i):
        wide = pl.ds(pl.multiple_of(i * tile, tile), tile)
        gu_part[wide, :] = dot(e_all[:, wide], pg[...], 0, 0).astype(BF16)

    loop(width // tile, gu_body)
    gus.seeds(range(n - 2, -1, -1))
    gds.seeds([0])

    x_y.wait_recv()
    wire.start(x_x)
    wire.start(x_c)
    egs[0].third()
    egs[1].second()
    for r in range(2, n - 1):
        ups.wave(r)
        eg_chunk(r)
    if n > 2:
        gds.relay(0)
    x_own_x.wait_recv()
    wire.start(x_own_xc)
    egs[1].third()
    for r in range(2, n - 1):
        egs[r].second()
    x_x.wait_recv()
    wire.start(x_xc)
    for copy in (x_own_c, x_c, x_own_xc, x_xc):
        copy.wait_recv()
    own_x.wait()
    for r in range(2, n - 1):
        egs[r].third()

    if n > 2:
        ups.wave(n - 1)
        eg_chunk(n - 1)

    def lh_body(parity):
        rows = half_of(parity)

        def body(i):
            at = pl.ds(pl.multiple_of(parity * group + i * slope_rows, slope_rows), slope_rows)
            h = dot(x_all[at, :], up_full[...]).astype(BF16)
            lh[at, :] = h
            act_l[at, :] = squared(h)

        loop(group // slope_rows, body)
        return rows

    theirs = lh_body(1 - y)
    lh_y = [
        wire.remote(lh.at[theirs, strip(i)], lh_o.at[:, cols(i, y)], py) for i in range(n)
    ]
    for copy in lh_y:
        wire.start(copy)
    egs[n - 1].second()
    ours = lh_body(y)
    lh_mine = [wire.copy(lh.at[ours, strip(i)], lh_o.at[:, cols(i, y)]) for i in range(n)]
    for k in range(n):
        out_chunk(k)
        if k:
            outs[k - 1].second()
    outs[n - 1].second()
    for m in range(n - 3, -1, -1):
        gus.relay(m)
    egs[n - 1].third()
    for k in range(n):
        outs[k].third()

    gds.final(gd_fin, lambda i: i, hb // 4)
    gd_done = wire.copy(gd_fin, gd_o)
    per = up_rows // (chunk // 4)
    gus.final(gu_fin, lambda i: lax.rem(i + (1 - y) * per, 2 * per), chunk // 4)
    swap_out[...] = gu_fin[pl.ds(pl.multiple_of((1 - y) * up_rows, up_rows), up_rows), :].astype(BF16)
    swap = wire.remote(swap_out, swap_in, py)
    wire.start(swap)
    for k in range(n):
        egs[k].last(eg_fin, column_block(k))
    eg_done = wire.copy(eg_fin, eg_o)
    for k in range(n):
        outs[k].last(out_fin, pl.ds(k * chunk, chunk))
    out_done = wire.copy(out_fin, out_o)
    swap.wait_recv()
    for i in range(n):
        gu_out[:, cols(i, y)] = gu_fin[pl.ds(pl.multiple_of(y * up_rows, up_rows), up_rows), strip(i)]
        gu_out[:, cols(i, 1 - y)] = swap_in[:, strip(i)].astype(F32)
    gu_done = wire.copy(gu_out, gu_o)
    for copy in lh_y:
        copy.wait_recv()
    for copy in lh_mine + [gd_done, eg_done, out_done, gu_done]:
        copy.wait()
    wire.drain()


def fused(n, later_in, earlier_in, hidden, cot, up, down):
    group, width = earlier_in.shape
    block, hb, up_rows = later_in.shape[0], down.shape[0], up.shape[0]
    half, tokens, chunk = n * hb, 2 * group, 2 * up_rows
    any_space = pl.BlockSpec(memory_space=pl.ANY)
    shapes = (
        jax.ShapeDtypeStruct(later_in.shape, BF16),
        jax.ShapeDtypeStruct(hidden.shape, BF16),
        jax.ShapeDtypeStruct(later_in.shape, BF16),
        jax.ShapeDtypeStruct(up.shape, F32),
        jax.ShapeDtypeStruct(down.shape, F32),
    )
    vm = pltpu.VMEM
    scratch = [
        vm((tokens, width), BF16), vm((tokens, width), BF16), vm((tokens, width), BF16),
        vm((tokens, half), BF16), vm((half, tokens), BF16), vm((tokens, half), BF16),
        vm((width, half), BF16), vm((half, width), BF16),
        vm((half, width), BF16), vm((width, half), BF16),
        vm((2, n - 1, hb, width), BF16), vm((2, max(n - 2, 1), hb, width), BF16),
        vm((2, n - 1, chunk, half), BF16), vm((2, max(n - 2, 1), chunk, half), BF16),
        vm((up_rows, half), BF16), vm((up_rows, half), BF16),
        vm((tokens, half), BF16), vm((tokens, half), BF16),
        vm((2 * n, 2, 2, 2, block, chunk), BF16), vm((2 * n, 2, 2, block, chunk), BF16),
        vm((2 * n, 2, block, chunk), BF16), vm((2 * n, 2, block, chunk), BF16),
        vm((2 * n, block, chunk), BF16), vm((2 * n, block, chunk), BF16),
        vm((block, width), BF16), vm((block, width), BF16),
        vm((hb, width), F32), vm((chunk, half), F32), vm(up.shape, F32),
    ]
    remote_copies = 8 * (n - 1) + 15 + 3 * n + 6 * n + 1
    local_copies = 3 * n + 8
    return pl.pallas_call(
        functools.partial(layer, n),
        out_shape=shapes,
        in_specs=[any_space] * 6,
        out_specs=(any_space,) * 5,
        scratch_shapes=scratch + [
            pltpu.SemaphoreType.DMA((remote_copies,)),
            pltpu.SemaphoreType.DMA((remote_copies,)),
            pltpu.SemaphoreType.DMA((local_copies,)),
        ],
        compiler_params=pltpu.CompilerParams(
            collective_id=0, has_side_effects=True, vmem_limit_bytes=VMEM_BYTES
        ),
        name="layer",
    )(later_in, earlier_in, hidden, cot, up, down)


def portable(later_in, earlier_in, hidden, cot, up, down):
    def split_sum(partial, axis):
        return lax.psum_scatter(partial.astype(F32), axis, scatter_dimension=0, tiled=True)

    up_full = lax.all_gather(up, "fs", axis=0, tiled=True)
    down_full = lax.all_gather(down, "fs", axis=0, tiled=True)
    rows = lax.all_gather(later_in, "tp", axis=0, tiled=True)
    lifted = jnp.maximum(hidden.astype(F32), 0.0)
    gd = split_sum(dot(squared(hidden), cot, 0, 0), "fs")
    pre = (2.0 * dot(cot, down_full, 1, 1) * lifted).astype(BF16)
    gu = split_sum(dot(earlier_in, pre, 0, 0), "fs")
    eg = split_sum(dot(pre, up_full, 1, 1).astype(BF16), "tp").astype(BF16)
    later_hidden = dot(rows, up_full).astype(BF16)
    out = split_sum(dot(squared(later_hidden), down_full).astype(BF16), "tp").astype(BF16)
    return out, later_hidden, eg, gu, gd


def solution(mesh):
    n_fs, n_tp = mesh.shape["fs"], mesh.shape["tp"]

    def shards(
        later_input, earlier_input, earlier_hidden, cotangent, up_weight, down_weight, up_sum, down_sum
    ):
        scale = float(earlier_input.shape[0] * n_fs) ** (-0.5)
        args = (later_input, earlier_input, earlier_hidden, cotangent, up_weight, down_weight)
        planes = n_fs // 2
        fits = (
            n_tp == 4 and n_fs % 2 == 0 and 2 < planes <= 4
            and down_weight.shape[0] % LANES == 0 and up_weight.shape[0] % LANES == 0
            and later_input.shape[0] % LANES == 0
        )
        out, later_hidden, eg, gu, gd = fused(planes, *args) if fits else portable(*args)
        return out, later_hidden, eg, up_sum + scale * gu, down_sum + scale * gd

    in_specs = (
        P(("fs", "tp"), None), P("fs", None), P("fs", "tp"), P("fs", None),
        P("fs", "tp"), P(("tp", "fs"), None), P("fs", "tp"), P(("tp", "fs"), None),
    )
    out_specs = (
        P(("fs", "tp"), None), P("fs", "tp"), P(("fs", "tp"), None),
        P("fs", "tp"), P(("tp", "fs"), None),
    )
    return jax.shard_map(shards, mesh=mesh, in_specs=in_specs, out_specs=out_specs, check_vma=False)
```

```python
import functools

import jax
import jax.numpy as jnp
from jax import lax
from jax.experimental import pallas as pl
from jax.experimental.pallas import tpu as pltpu
from jax.sharding import PartitionSpec as P

F32, BF16 = jnp.float32, jnp.bfloat16
MESH = pl.DeviceIdType.MESH
LANES = 128
VMEM_BYTES = 67_043_328


def dot(a, b, ca=1, cb=0):
    return lax.dot_general(a, b, (((ca,), (cb,)), ((), ())), preferred_element_type=F32)


def loop(n, body):
    def step(i, carry):
        body(i)
        return carry

    lax.fori_loop(0, n, step, 0)


def squared(h):
    lifted = jnp.maximum(h.astype(F32), 0.0)
    return (lifted * lifted).astype(BF16)


def both(a, b):
    return jnp.logical_and(a, b)


class Wire:
    def __init__(self, send, recv, local):
        self.send, self.recv, self.local = send, recv, local
        self.n_remote = self.n_local = 0
        self.open = []

    def slot(self):
        self.n_remote += 1
        return self.n_remote - 1

    def remote(self, src, dst, device, slot=None):
        i = self.slot() if slot is None else slot
        return pltpu.make_async_remote_copy(
            src_ref=src, dst_ref=dst, send_sem=self.send.at[i], recv_sem=self.recv.at[i],
            device_id=device, device_id_type=MESH,
        )

    def start(self, copy, when=None):
        if when is None:
            copy.start()
        else:
            pl.when(when)(copy.start)
        self.open.append((copy, when))

    def copy(self, src, dst):
        i = self.n_local
        self.n_local += 1
        made = pltpu.make_async_copy(src, dst, self.local.at[i])
        made.start()
        return made

    def drain(self):
        for copy, when in self.open:
            if when is None:
                copy.wait_send()
            else:
                pl.when(when)(copy.wait_send)


class Line:
    def __init__(self, wire, full, rows, own, z, n, left, right):
        self.wire, self.z, self.n = wire, z, n
        self.right, self.left = {}, {}

        def block(i):
            return full.at[pl.ds(pl.multiple_of(lax.rem(i + n, n) * rows, rows), rows)]

        for r in range(1, n):
            src = own if r == 1 else block(z - r + 1)
            self.right[r] = wire.remote(src, block(z - r + 1), right)
            src = own if r == 1 else block(z + r - 1)
            self.left[r] = wire.remote(src, block(z + r - 1), left)

    def begin(self, right=True, left=True):
        self.wire.start(self.right[1], both(self.z < self.n - 1, right))
        self.wire.start(self.left[1], both(self.z > 0, left))

    def forward(self, r):
        z, n = self.z, self.n
        rightward, leftward = both(z >= r, z < n - 1), both(z <= n - 1 - r, z > 0)
        pl.when(rightward)(self.right[r].wait_recv)
        self.wire.start(self.right[r + 1], rightward)
        pl.when(leftward)(self.left[r].wait_recv)
        self.wire.start(self.left[r + 1], leftward)

    def ends(self, r):
        z, n = self.z, self.n
        pl.when(both(z >= r, z == n - 1))(self.right[r].wait_recv)
        pl.when(both(z <= n - 1 - r, z == 0))(self.left[r].wait_recv)


class Sums:
    def __init__(self, wire, part, inbox, relayed, rows, z, n, left, right):
        self.wire, self.part, self.inbox, self.relayed = wire, part, inbox, relayed
        self.rows, self.z, self.n = rows, z, n
        self.seed, self.pass_on = {}, {}
        for way, device in ((0, right), (1, left)):
            for m in range(n - 1):
                slot = wire.slot()
                dst = inbox.at[way, m]
                self.seed[way, m] = wire.remote(part.at[self.span(way, m)], dst, device, slot)
                if m < n - 2:
                    self.pass_on[way, m] = wire.remote(relayed.at[way, m], dst, device, slot)

    def span(self, way, m, lo=0, size=None):
        ahead = self.z + 1 + m if way == 0 else self.z - 1 - m
        base = lax.rem(ahead + 2 * self.n, self.n) * self.rows
        size = self.rows if size is None else size
        return pl.ds(pl.multiple_of(base + lo, size), size)

    def seeds(self, ms):
        for m in ms:
            self.wire.start(self.seed[0, m], self.z == 0)
            self.wire.start(self.seed[1, m], self.z == self.n - 1)

    def relay(self, m):
        z, n = self.z, self.n
        tile = self.rows // 4
        for way in (0, 1):
            if way == 0:
                when = both(z >= 1, z + 1 + m <= n - 1)
            else:
                when = both(z <= n - 2, z - 1 - m >= 0)

            def add(way=way):
                self.seed[way, m + 1].wait_recv()

                def body(i):
                    lo = pl.multiple_of(i * tile, tile)
                    mine = self.part[self.span(way, m, lo, tile), :].astype(F32)
                    came = self.inbox[way, m + 1, pl.ds(lo, tile), :].astype(F32)
                    self.relayed[way, m, pl.ds(lo, tile), :] = (mine + came).astype(BF16)

                loop(4, body)

            pl.when(when)(add)
            self.wire.start(self.pass_on[way, m], when)

    def final(self, out, order, tile):
        z, n = self.z, self.n
        pl.when(z >= 1)(self.seed[0, 0].wait_recv)
        pl.when(z <= n - 2)(self.seed[1, 0].wait_recv)
        up, down = (z >= 1).astype(F32), (z <= n - 2).astype(F32)
        base = z * self.rows

        def body(i):
            lo = pl.multiple_of(order(i) * tile, tile)
            rows = pl.ds(lo, tile)
            mine = self.part[pl.ds(pl.multiple_of(base + lo, tile), tile), :].astype(F32)
            first = jnp.where(z >= 1, self.inbox[0, 0, rows, :].astype(F32), 0.0)
            second = jnp.where(z <= n - 2, self.inbox[1, 0, rows, :].astype(F32), 0.0)
            out[rows, :] = mine + first + second

        loop(self.rows // tile, body)


class Plane:
    def __init__(self, wire, bufs, k, at, peers, x_first):
        self.part, self.in_a, self.to_b, self.in_b, self.to_c, self.in_c = (b.at[k] for b in bufs)
        self.wire, self.x_first = wire, x_first
        x, y, self.core = at
        self.one, self.two = (x, y) if x_first else (y, x)
        self.a = wire.remote(self.part.at[1 - self.core], self.in_a, peers[2])
        self.b = wire.remote(self.to_b, self.in_b, peers[0 if x_first else 1])
        self.c = wire.remote(self.to_c, self.in_c, peers[1 if x_first else 0])

    def pair(self, one, two):
        i, j = (one, two) if self.x_first else (two, one)
        return self.part[self.core, i, j].astype(F32) + self.in_a[i, j].astype(F32)

    def mine(self, two):
        return self.pair(self.one, two) + self.in_b[two].astype(F32)

    def begin(self):
        self.wire.start(self.a)

    def second(self):
        self.a.wait_recv()
        for two in (0, 1):
            self.to_b[two] = self.pair(1 - self.one, two).astype(BF16)
        self.wire.start(self.b)

    def third(self):
        self.b.wait_recv()
        self.to_c[...] = self.mine(1 - self.two).astype(BF16)
        self.wire.start(self.c)

    def last(self, out, columns):
        self.c.wait_recv()
        out[:, columns] = (self.mine(self.two) + self.in_c[...].astype(F32)).astype(BF16)


def layer(
    n, later_in, earlier_in, hidden, cot, up, down,
    out_o, lh_o, eg_o, gu_o, gd_o,
    c_all, e_all, x_all, h_all, act_t, pg, up_full, down_full, gd_part, gu_part,
    gd_in, gd_relay, gu_in, gu_relay, swap_out, swap_in, lh, act_l,
    part, in_a, to_b, in_b, to_c, in_c, eg_fin, out_fin, gd_fin, gu_fin, gu_out,
    send, recv, local,
):
    fs, tp = lax.axis_index("fs"), lax.axis_index("tp")
    z, y = fs // 2, fs % 2
    x, c = tp // 2, tp % 2
    py, px, pc = (fs + 1 - 2 * y, tp), (fs, tp + 2 - 4 * x), (fs, tp + 1 - 2 * c)
    left, right = (lax.rem(fs + 2 * n - 2, 2 * n), tp), (lax.rem(fs + 2, 2 * n), tp)

    group, width = earlier_in.shape
    block = later_in.shape[0]
    hb = down.shape[0]
    half = n * hb
    up_rows = up.shape[0]
    chunk = 2 * up_rows
    wire = Wire(send, recv, local)

    def cols(i, parity):
        return pl.ds(pl.multiple_of((2 * i + parity) * hb, hb), hb)

    def strip(i):
        return pl.ds(i * hb, hb)

    def rows_of(parity, q):
        return pl.ds(pl.multiple_of(parity * group + q * block, block), block)

    def half_of(parity):
        return pl.ds(pl.multiple_of(parity * group, group), group)

    barrier = pltpu.get_barrier_semaphore()

    def greet(device):
        pl.semaphore_signal(barrier, inc=1, device_id=device, device_id_type=MESH)

    for device in (py, px, pc):
        greet(device)
    pl.when(z > 0)(lambda: greet(left))
    pl.when(z < n - 1)(lambda: greet(right))

    own_h = [wire.copy(hidden.at[:, cols(i, y)], h_all.at[half_of(y), strip(i)]) for i in range(n)]
    my_rows = pl.ds(pl.multiple_of(fs * up_rows, up_rows), up_rows)
    own_up = [wire.copy(up.at[:, cols(i, y)], up_full.at[my_rows, strip(i)]) for i in range(n)]
    own_c = wire.copy(cot, c_all.at[half_of(y)])
    own_down = wire.copy(down, down_full.at[pl.ds(pl.multiple_of(z * hb, hb), hb)])
    own_e = wire.copy(earlier_in, e_all.at[half_of(y)])
    own_x = wire.copy(later_in, x_all.at[rows_of(y, tp)])

    pl.semaphore_wait(barrier, 3 + (z > 0).astype(jnp.int32) + (z < n - 1).astype(jnp.int32))

    def spread(whole, source, first, parts):
        size = block // parts

        def sub(parity, q, i):
            base = parity * group + q * block + i * size
            return whole.at[pl.ds(pl.multiple_of(base, size), size)]

        made = []
        for i in range(parts):
            there, came = sub(y, tp, i), sub(1 - y, tp, i)
            beside = sub(1 - y, tp + 2 - 4 * x, i)
            src = source.at[pl.ds(pl.multiple_of(first + i * size, size), size)]
            made.append((
                wire.remote(src, there, py), wire.remote(came, came, px),
                wire.remote(came, came, pc), wire.remote(beside, beside, pc),
            ))
        return zip(*made)

    downs = Line(wire, down_full, hb, down, z, n, left, right)
    up_block = up_full.at[pl.ds(pl.multiple_of(z * chunk, chunk), chunk)]
    ups = Line(wire, up_full, chunk, up_block, z, n, left, right)
    c_y, c_x, c_c, c_xc = spread(c_all, cot, tp * block, 2)
    e_y, e_x, e_c, e_xc = spread(e_all, earlier_in, tp * block, 2)
    x_y, x_x, x_c, x_xc = spread(x_all, later_in, 0, 2)
    mine_x = x_all.at[rows_of(y, tp)]
    beside_x = x_all.at[rows_of(y, tp + 2 - 4 * x)]
    x_own_x = wire.remote(later_in, mine_x, px)
    x_own_c = wire.remote(later_in, mine_x, pc)
    x_own_xc = wire.remote(beside_x, beside_x, pc)
    up_y = [
        wire.remote(up.at[:, cols(i, 1 - y)], up_full.at[my_rows, strip(i)], py) for i in range(n)
    ]
    h_y = [
        wire.remote(hidden.at[:, cols(i, 1 - y)], h_all.at[half_of(y), strip(i)], py)
        for i in range(n)
    ]

    gds = Sums(wire, gd_part, gd_in, gd_relay, hb, z, n, left, right)
    gus = Sums(wire, gu_part, gu_in, gu_relay, chunk, z, n, left, right)
    bufs = (part, in_a, to_b, in_b, to_c, in_c)
    planes = [Plane(wire, bufs, k, (x, y, c), (px, py, pc), k >= n) for k in range(2 * n)]
    egs, outs = planes[:n], planes[n:]
    tile = min(256, chunk)
    slope_rows = min(256, 2 * group)
    theirs, ours = half_of(1 - y), half_of(y)
    lh_y = [wire.remote(lh.at[theirs, strip(i)], lh_o.at[:, cols(i, y)], py) for i in range(n)]
    swap = wire.remote(swap_out, swap_in, py)
    stores = []

    def start(*copies):
        for copy in copies:
            wire.start(copy)

    def arrive(*copies):
        for copy in copies:
            copy.wait_recv()

    def activate(parity):
        def body(i):
            rows = rows_of(parity, i)
            act_t[:, rows] = squared(h_all[rows, :]).T

        loop(group // block, body)

    def column_block(k):
        where = 0
        for i in range(n):
            order = sorted(range(n), key=lambda b: (abs(b - i), b))
            where = where + jnp.where(z == i, order[k], 0)
        return pl.ds(pl.multiple_of(where * chunk, chunk), chunk)

    def store_part(k, parity, value):
        for q in range(4):
            part[k, q % 2, q // 2, parity] = value[q * block : (q + 1) * block].astype(BF16)

    def gd_dots():
        def body(i):
            columns = pl.ds(pl.multiple_of(i * tile, tile), tile)
            gd_part[:, columns] = dot(act_t[...], c_all[:, columns]).astype(BF16)

        loop(width // tile, body)

    def pg_dots():
        def body(i):
            rows = pl.ds(pl.multiple_of(i * slope_rows, slope_rows), slope_rows)
            lifted = jnp.maximum(h_all[rows, :].astype(F32), 0.0)
            pg[rows, :] = (2.0 * dot(c_all[rows, :], down_full[...], 1, 1) * lifted).astype(BF16)

        loop(2 * group // slope_rows, body)

    def gu_dots():
        def body(i):
            wide = pl.ds(pl.multiple_of(i * tile, tile), tile)
            gu_part[wide, :] = dot(e_all[:, wide], pg[...], 0, 0).astype(BF16)

        loop(width // tile, body)

    def eg_chunk(k):
        wide = column_block(k)

        def body(parity):
            store_part(k, parity, dot(pg[half_of(parity), :], up_full[wide, :], 1, 1))

        loop(2, body)
        egs[k].begin()

    def out_chunk(k):
        wide = pl.ds(k * chunk, chunk)

        def body(parity):
            store_part(n + k, parity, dot(act_l[half_of(parity), :], down_full[:, wide]))

        loop(2, body)
        outs[k].begin()

    def lh_dots(parity):
        def body(i):
            at = pl.ds(pl.multiple_of(parity * group + i * slope_rows, slope_rows), slope_rows)
            h = dot(x_all[at, :], up_full[...]).astype(BF16)
            lh[at, :] = h
            act_l[at, :] = squared(h)

        loop(group // slope_rows, body)

    def first_sends():
        downs.begin()
        start(*c_y, *up_y, *h_y, *e_y, *x_y, x_own_x, x_own_c)

    def ups_begin():
        for copy in own_up:
            copy.wait()
        arrive(*up_y)
        ups.begin(z < 2, z > n - 3)

    def own_act():
        for copy in own_h:
            copy.wait()
        activate(y)

    def all_c():
        arrive(*c_c, *c_xc)
        own_c.wait()

    def all_e():
        arrive(*e_c, *e_xc)
        own_e.wait()

    def all_x():
        arrive(x_own_c, x_own_xc, *x_c, *x_xc)
        own_x.wait()

    def pass_on(came, *onward):
        arrive(came)
        start(*onward)

    def lh_send():
        start(*lh_y)

    def lh_store():
        stores.extend(wire.copy(lh.at[ours, strip(i)], lh_o.at[:, cols(i, y)]) for i in range(n))

    def gd_final():
        gds.final(gd_fin, lambda i: i, hb // 4)
        stores.append(wire.copy(gd_fin, gd_o))

    def gu_final():
        per = up_rows // (chunk // 4)
        gus.final(gu_fin, lambda i: lax.rem(i + (1 - y) * per, 2 * per), chunk // 4)
        away = pl.ds(pl.multiple_of((1 - y) * up_rows, up_rows), up_rows)
        swap_out[...] = gu_fin[away, :].astype(BF16)
        start(swap)

    def gu_store():
        home = pl.ds(pl.multiple_of(y * up_rows, up_rows), up_rows)
        arrive(swap)
        for i in range(n):
            gu_out[:, cols(i, y)] = gu_fin[home, strip(i)]
            gu_out[:, cols(i, 1 - y)] = swap_in[:, strip(i)].astype(F32)
        stores.append(wire.copy(gu_out, gu_o))

    def eg_store():
        for k in range(n):
            egs[k].last(eg_fin, column_block(k))
        stores.append(wire.copy(eg_fin, eg_o))

    def out_store():
        for k in range(n):
            outs[k].last(out_fin, pl.ds(k * chunk, chunk))
        stores.append(wire.copy(out_fin, out_o))

    def close():
        arrive(*lh_y)
        for copy in stores:
            copy.wait()
        wire.drain()

    def do(name, act, *args):
        with jax.named_scope(name):
            act(*args)

    last = n - 1
    do("first", first_sends)
    do("own_act", own_act)
    do("c_y0", pass_on, c_y[0], c_x[0], c_c[0])
    do("down1", downs.forward, 1)
    do("c_y1", pass_on, c_y[1], c_x[1], c_c[1])
    do("x_own_x", pass_on, x_own_x, x_own_xc)
    do("up_y", ups_begin)
    for i in (0, 1):
        do("c_x", pass_on, c_x[i], c_xc[i])
    for r in range(2, last):
        do("down2", downs.forward, r)
    ups.begin(z >= 2, z <= n - 3)
    do("h_y", arrive, *h_y)
    do("act2", activate, 1 - y)
    do("c_all", all_c)
    do("gd_dots", gd_dots)
    do("gd_seed", gds.seeds, range(n - 2, 0, -1))
    do("e_y0", pass_on, e_y[0], e_x[0], e_c[0])
    do("ups1", ups.forward, 1)
    for r in range(1, n):
        do("down_end", downs.ends, r)
    own_down.wait()
    do("pg", pg_dots)
    do("e_y1", pass_on, e_y[1], e_x[1], e_c[1])
    do("eg0", eg_chunk, 0)
    do("e_x0", pass_on, e_x[0], e_xc[0])
    do("eg0_b", egs[0].second)
    for m in range(n - 3, 0, -1):
        do("gd_relay", gds.relay, m)
    do("x_y0", pass_on, x_y[0], x_x[0], x_c[0])
    do("e_x1", pass_on, e_x[1], e_xc[1])
    do("e_all", all_e)
    do("gu_dots", gu_dots)
    do("gu_seed", gus.seeds, range(n - 2, -1, -1))
    gds.seeds([0])
    do("x_y1", pass_on, x_y[1], x_x[1], x_c[1])
    do("up1_end", ups.ends, 1)
    do("eg1", eg_chunk, 1)
    for r in range(2, last):
        do("ups2", ups.forward, r)
    do("eg1_b", egs[1].second)
    do("eg0_c", egs[0].third)
    do("gd_relay0", gds.relay, 0)
    for r in range(2, last):
        do("up2_end", ups.ends, r)
        do("eg2", eg_chunk, r)
    do("eg1_c", egs[1].third)
    for r in range(2, last):
        do("eg2_b", egs[r].second)
    for i in (0, 1):
        do("x_x", pass_on, x_x[i], x_xc[i])
    do("x_all", all_x)
    do("up3_end", ups.ends, last)
    do("lh1", lh_dots, 1 - y)
    do("lh2", lh_dots, y)
    lh_store()
    do("out0", out_chunk, 0)
    do("eg3", eg_chunk, last)
    for r in range(2, last):
        do("eg2_c", egs[r].third)
    do("out1", out_chunk, 1)
    do("out0_b", outs[0].second)
    do("eg3_b", egs[last].second)
    do("lh_send", lh_send)
    for m in range(n - 3, 0, -1):
        do("gu_relay", gus.relay, m)
    for k in range(2, n):
        do("out", out_chunk, k)
        do("out_b", outs[k - 1].second)
    do("out_b", outs[last].second)
    do("out0_c", outs[0].third)
    do("gu_relay0", gus.relay, 0)
    do("eg3_c", egs[last].third)
    for k in range(1, n):
        do("out_c", outs[k].third)
    do("gu_fin", gu_final)
    do("eg_fin", eg_store)
    do("gd_fin", gd_final)
    do("out_fin", out_store)
    do("gu_sto", gu_store)
    do("close", close)


def fused(n, later_in, earlier_in, hidden, cot, up, down):
    group, width = earlier_in.shape
    block, hb, up_rows = later_in.shape[0], down.shape[0], up.shape[0]
    half, tokens, chunk = n * hb, 2 * group, 2 * up_rows
    any_space = pl.BlockSpec(memory_space=pl.ANY)
    shapes = (
        jax.ShapeDtypeStruct(later_in.shape, BF16),
        jax.ShapeDtypeStruct(hidden.shape, BF16),
        jax.ShapeDtypeStruct(later_in.shape, BF16),
        jax.ShapeDtypeStruct(up.shape, F32),
        jax.ShapeDtypeStruct(down.shape, F32),
    )
    vm = pltpu.VMEM
    scratch = [
        vm((tokens, width), BF16), vm((tokens, width), BF16), vm((tokens, width), BF16),
        vm((tokens, half), BF16), vm((half, tokens), BF16), vm((tokens, half), BF16),
        vm((width, half), BF16), vm((half, width), BF16),
        vm((half, width), BF16), vm((width, half), BF16),
        vm((2, n - 1, hb, width), BF16), vm((2, max(n - 2, 1), hb, width), BF16),
        vm((2, n - 1, chunk, half), BF16), vm((2, max(n - 2, 1), chunk, half), BF16),
        vm((up_rows, half), BF16), vm((up_rows, half), BF16),
        vm((tokens, half), BF16), vm((tokens, half), BF16),
        vm((2 * n, 2, 2, 2, block, chunk), BF16), vm((2 * n, 2, 2, block, chunk), BF16),
        vm((2 * n, 2, block, chunk), BF16), vm((2 * n, 2, block, chunk), BF16),
        vm((2 * n, block, chunk), BF16), vm((2 * n, block, chunk), BF16),
        vm((block, width), BF16), vm((block, width), BF16),
        vm((hb, width), F32), vm((chunk, half), F32), vm(up.shape, F32),
    ]
    remote_copies = 24 * n + 40
    local_copies = 3 * n + 8
    return pl.pallas_call(
        functools.partial(layer, n),
        out_shape=shapes,
        in_specs=[any_space] * 6,
        out_specs=(any_space,) * 5,
        scratch_shapes=scratch + [
            pltpu.SemaphoreType.DMA((remote_copies,)),
            pltpu.SemaphoreType.DMA((remote_copies,)),
            pltpu.SemaphoreType.DMA((local_copies,)),
        ],
        compiler_params=pltpu.CompilerParams(
            collective_id=0, has_side_effects=True, vmem_limit_bytes=VMEM_BYTES
        ),
        name="layer",
    )(later_in, earlier_in, hidden, cot, up, down)


def portable(later_in, earlier_in, hidden, cot, up, down):
    def split_sum(partial, axis):
        return lax.psum_scatter(partial.astype(F32), axis, scatter_dimension=0, tiled=True)

    up_full = lax.all_gather(up, "fs", axis=0, tiled=True)
    down_full = lax.all_gather(down, "fs", axis=0, tiled=True)
    rows = lax.all_gather(later_in, "tp", axis=0, tiled=True)
    lifted = jnp.maximum(hidden.astype(F32), 0.0)
    gd = split_sum(dot(squared(hidden), cot, 0, 0), "fs")
    pre = (2.0 * dot(cot, down_full, 1, 1) * lifted).astype(BF16)
    gu = split_sum(dot(earlier_in, pre, 0, 0), "fs")
    eg = split_sum(dot(pre, up_full, 1, 1).astype(BF16), "tp").astype(BF16)
    later_hidden = dot(rows, up_full).astype(BF16)
    out = split_sum(dot(squared(later_hidden), down_full).astype(BF16), "tp").astype(BF16)
    return out, later_hidden, eg, gu, gd


def solution(mesh):
    n_fs, n_tp = mesh.shape["fs"], mesh.shape["tp"]

    def shards(
        later_input, earlier_input, earlier_hidden, cotangent, up_weight, down_weight, up_sum, down_sum
    ):
        scale = float(earlier_input.shape[0] * n_fs) ** (-0.5)
        args = (later_input, earlier_input, earlier_hidden, cotangent, up_weight, down_weight)
        planes = n_fs // 2
        fits = (
            n_tp == 4 and n_fs % 2 == 0 and 2 < planes <= 4
            and down_weight.shape[0] % LANES == 0 and up_weight.shape[0] % LANES == 0
            and later_input.shape[0] % LANES == 0
        )
        out, later_hidden, eg, gu, gd = fused(planes, *args) if fits else portable(*args)
        return out, later_hidden, eg, up_sum + scale * gu, down_sum + scale * gd

    in_specs = (
        P(("fs", "tp"), None), P("fs", None), P("fs", "tp"), P("fs", None),
        P("fs", "tp"), P(("tp", "fs"), None), P("fs", "tp"), P(("tp", "fs"), None),
    )
    out_specs = (
        P(("fs", "tp"), None), P("fs", "tp"), P(("fs", "tp"), None),
        P("fs", "tp"), P(("tp", "fs"), None),
    )
    return jax.shard_map(shards, mesh=mesh, in_specs=in_specs, out_specs=out_specs, check_vma=False)
```

```python
import functools

import jax
import jax.numpy as jnp
from jax import lax
from jax.experimental import pallas as pl
from jax.experimental.pallas import tpu as pltpu
from jax.sharding import PartitionSpec as P

F32, BF16 = jnp.float32, jnp.bfloat16
MESH = pl.DeviceIdType.MESH
LANES = 128
VMEM_BYTES = 67_043_328


def dot(a, b, ca=1, cb=0):
    return lax.dot_general(a, b, (((ca,), (cb,)), ((), ())), preferred_element_type=F32)


def loop(n, body):
    def step(i, carry):
        body(i)
        return carry

    lax.fori_loop(0, n, step, 0)


def squared(h):
    lifted = jnp.maximum(h.astype(F32), 0.0)
    return (lifted * lifted).astype(BF16)


def both(a, b):
    return jnp.logical_and(a, b)


class Wire:
    def __init__(self, send, recv, local):
        self.send, self.recv, self.local = send, recv, local
        self.n_remote = self.n_local = 0
        self.open = []

    def slot(self):
        self.n_remote += 1
        return self.n_remote - 1

    def remote(self, src, dst, device, slot=None):
        i = self.slot() if slot is None else slot
        return pltpu.make_async_remote_copy(
            src_ref=src, dst_ref=dst, send_sem=self.send.at[i], recv_sem=self.recv.at[i],
            device_id=device, device_id_type=MESH,
        )

    def start(self, copy, when=None):
        if when is None:
            copy.start()
        else:
            pl.when(when)(copy.start)
        self.open.append((copy, when))

    def copy(self, src, dst):
        i = self.n_local
        self.n_local += 1
        made = pltpu.make_async_copy(src, dst, self.local.at[i])
        made.start()
        return made

    def drain(self):
        for copy, when in self.open:
            if when is None:
                copy.wait_send()
            else:
                pl.when(when)(copy.wait_send)


class Line:
    def __init__(self, wire, full, rows, own, swap, z, n, left, right):
        self.wire, self.z, self.n = wire, z, n
        self.right, self.left = {}, {}
        size = rows // 2

        def half(i, p):
            base = lax.rem(i + n, n) * rows + lax.rem(swap + p, 2) * size
            return full.at[pl.ds(pl.multiple_of(base, size), size)]

        for p in (0, 1):
            first = half(z, p)
            if own is not None:
                first = own.at[pl.ds(pl.multiple_of(lax.rem(swap + p, 2) * size, size), size)]
            for r in range(1, n):
                src = first if r == 1 else half(z - r + 1, p)
                self.right[r, p] = wire.remote(src, half(z - r + 1, p), right)
                src = first if r == 1 else half(z + r - 1, p)
                self.left[r, p] = wire.remote(src, half(z + r - 1, p), left)

    def begin(self, p, right=True, left=True):
        self.wire.start(self.right[1, p], both(self.z < self.n - 1, right))
        self.wire.start(self.left[1, p], both(self.z > 0, left))

    def begin_at(self, stage, p):
        self.begin(p, self.z == stage, self.z == self.n - 1 - stage)

    def forward(self, r, p, outer=None):
        z, n = self.z, self.n
        rightward, leftward = both(z >= r, z < n - 1), both(z <= n - 1 - r, z > 0)
        if outer is not None:
            rightward = both(rightward, (z == r) == outer)
            leftward = both(leftward, (z == n - 1 - r) == outer)
        pl.when(rightward)(self.right[r, p].wait_recv)
        self.wire.start(self.right[r + 1, p], rightward)
        pl.when(leftward)(self.left[r, p].wait_recv)
        self.wire.start(self.left[r + 1, p], leftward)

    def ends(self, r):
        z, n = self.z, self.n
        for p in (0, 1):
            pl.when(both(z >= r, z == n - 1))(self.right[r, p].wait_recv)
            pl.when(both(z <= n - 1 - r, z == 0))(self.left[r, p].wait_recv)


class Sums:
    def __init__(self, wire, part, inbox, relayed, rows, swap, z, n, left, right):
        self.wire, self.part, self.inbox, self.relayed = wire, part, inbox, relayed
        self.rows, self.size, self.swap, self.z, self.n = rows, rows // 2, swap, z, n
        self.seed, self.pass_on = {}, {}
        for way, device in ((0, right), (1, left)):
            for m in range(n - 1):
                for p in (0, 1):
                    slot = wire.slot()
                    at = pl.ds(p * self.size, self.size)
                    dst = inbox.at[way, m, at]
                    src = part.at[self.span(way, m, p)]
                    self.seed[way, m, p] = wire.remote(src, dst, device, slot)
                    if m < n - 2:
                        src = relayed.at[way, m, at]
                        self.pass_on[way, m, p] = wire.remote(src, dst, device, slot)

    def half(self, p):
        return lax.rem(self.swap + p, 2) * self.size

    def span(self, way, m, p):
        ahead = self.z + 1 + m if way == 0 else self.z - 1 - m
        base = lax.rem(ahead + 2 * self.n, self.n) * self.rows + self.half(p)
        return pl.ds(pl.multiple_of(base, self.size), self.size)

    def seeds(self, ms):
        for m in ms:
            for p in (0, 1):
                self.wire.start(self.seed[0, m, p], self.z == 0)
                self.wire.start(self.seed[1, m, p], self.z == self.n - 1)

    def relay(self, m, p):
        z, n = self.z, self.n
        at = pl.ds(p * self.size, self.size)
        for way in (0, 1):
            if way == 0:
                when = both(z >= 1, z + 1 + m <= n - 1)
            else:
                when = both(z <= n - 2, z - 1 - m >= 0)

            def add(way=way):
                self.seed[way, m + 1, p].wait_recv()
                mine = self.part[self.span(way, m, p), :].astype(F32)
                came = self.inbox[way, m + 1, at, :].astype(F32)
                self.relayed[way, m, at, :] = (mine + came).astype(BF16)

            pl.when(when)(add)
            self.wire.start(self.pass_on[way, m, p], when)

    def total(self, p):
        z, n = self.z, self.n
        pl.when(z >= 1)(self.seed[0, 0, p].wait_recv)
        pl.when(z <= n - 2)(self.seed[1, 0, p].wait_recv)
        at = pl.ds(p * self.size, self.size)
        base = z * self.rows + self.half(p)
        mine = self.part[pl.ds(pl.multiple_of(base, self.size), self.size), :].astype(F32)
        first = jnp.where(z >= 1, self.inbox[0, 0, at, :].astype(F32), 0.0)
        second = jnp.where(z <= n - 2, self.inbox[1, 0, at, :].astype(F32), 0.0)
        return mine + first + second


class Plane:
    def __init__(self, wire, bufs, k, at, peers, x_first):
        self.part, self.in_a, self.to_b, self.in_b, self.to_c, self.in_c = (b.at[k] for b in bufs)
        self.wire, self.x_first = wire, x_first
        x, y, self.core = at
        self.one, self.two = (x, y) if x_first else (y, x)
        self.a = wire.remote(self.part.at[1 - self.core], self.in_a, peers[2])
        self.b = wire.remote(self.to_b, self.in_b, peers[0 if x_first else 1])
        self.c = wire.remote(self.to_c, self.in_c, peers[1 if x_first else 0])

    def pair(self, one, two):
        i, j = (one, two) if self.x_first else (two, one)
        return self.part[self.core, i, j].astype(F32) + self.in_a[i, j].astype(F32)

    def mine(self, two):
        return self.pair(self.one, two) + self.in_b[two].astype(F32)

    def begin(self):
        self.wire.start(self.a)

    def second(self):
        self.a.wait_recv()
        for two in (0, 1):
            self.to_b[two] = self.pair(1 - self.one, two).astype(BF16)
        self.wire.start(self.b)

    def third(self):
        self.b.wait_recv()
        self.to_c[...] = self.mine(1 - self.two).astype(BF16)
        self.wire.start(self.c)

    def last(self, out, columns):
        self.c.wait_recv()
        out[:, columns] = (self.mine(self.two) + self.in_c[...].astype(F32)).astype(BF16)


def layer(
    n, later_in, earlier_in, hidden, cot, up, down, up_sum, down_sum,
    out_o, lh_o, eg_o, gu_o, gd_o,
    c_all, e_all, x_all, h_all, act_t, pg, up_full, down_full, gd_part, gu_part,
    gd_in, gd_relay, gu_in, gu_relay, swap_out, swap_in, lh, act_l, lh_sum,
    *rest,
):
    eg_bufs, out_bufs = rest[:6], rest[6:12]
    eg_fin, out_fin, gd_fin, gu_fin, send, recv, local = rest[12:]
    fs, tp = lax.axis_index("fs"), lax.axis_index("tp")
    z, y = fs // 2, fs % 2
    x, c = tp // 2, tp % 2
    py, px, pc = (fs + 1 - 2 * y, tp), (fs, tp + 2 - 4 * x), (fs, tp + 1 - 2 * c)
    left, right = (lax.rem(fs + 2 * n - 2, 2 * n), tp), (lax.rem(fs + 2, 2 * n), tp)

    group, width = earlier_in.shape
    block = later_in.shape[0]
    hb = down.shape[0]
    half = n * hb
    up_rows = up.shape[0]
    chunk = 2 * up_rows
    wire = Wire(send, recv, local)

    def cols(i, parity):
        return pl.ds(pl.multiple_of((2 * i + parity) * hb, hb), hb)

    def strip(i):
        return pl.ds(i * hb, hb)

    def rows_of(parity, q):
        return pl.ds(pl.multiple_of(parity * group + q * block, block), block)

    def half_of(parity):
        return pl.ds(pl.multiple_of(parity * group, group), group)

    barrier = pltpu.get_barrier_semaphore()

    def greet(device):
        pl.semaphore_signal(barrier, inc=1, device_id=device, device_id_type=MESH)

    for device in (py, px, pc):
        greet(device)
    pl.when(z > 0)(lambda: greet(left))
    pl.when(z < n - 1)(lambda: greet(right))

    own_h = [wire.copy(hidden.at[:, cols(i, y)], h_all.at[half_of(y), strip(i)]) for i in range(n)]
    my_rows = pl.ds(pl.multiple_of(fs * up_rows, up_rows), up_rows)
    own_up = [wire.copy(up.at[:, cols(i, y)], up_full.at[my_rows, strip(i)]) for i in range(n)]
    own_c = wire.copy(cot, c_all.at[half_of(y)])
    own_down = wire.copy(down, down_full.at[pl.ds(pl.multiple_of(z * hb, hb), hb)])
    own_e = wire.copy(earlier_in, e_all.at[half_of(y)])
    own_x = wire.copy(later_in, x_all.at[rows_of(y, tp)])
    own_up_sum = wire.copy(up_sum, gu_fin)
    own_down_sum = wire.copy(down_sum, gd_fin)
    scale = float(group * 2 * n) ** (-0.5)

    pl.semaphore_wait(barrier, 3 + (z > 0).astype(jnp.int32) + (z < n - 1).astype(jnp.int32))

    def spread(whole, source, first, parts):
        size = block // parts

        def sub(parity, q, i):
            base = parity * group + q * block + i * size
            return whole.at[pl.ds(pl.multiple_of(base, size), size)]

        made = []
        for i in range(parts):
            there, came = sub(y, tp, i), sub(1 - y, tp, i)
            beside = sub(1 - y, tp + 2 - 4 * x, i)
            src = source.at[pl.ds(pl.multiple_of(first + i * size, size), size)]
            made.append((
                wire.remote(src, there, py), wire.remote(came, came, px),
                wire.remote(came, came, pc), wire.remote(beside, beside, pc),
            ))
        return zip(*made)

    downs = Line(wire, down_full, hb, down, y, z, n, left, right)
    ups = Line(wire, up_full, chunk, None, y, z, n, left, right)
    c_y, c_x, c_c, c_xc = spread(c_all, cot, tp * block, 2)
    e_y, e_x, e_c, e_xc = spread(e_all, earlier_in, tp * block, 2)
    x_y, x_x, x_c, x_xc = spread(x_all, later_in, 0, 2)
    mine_x = x_all.at[rows_of(y, tp)]
    beside_x = x_all.at[rows_of(y, tp + 2 - 4 * x)]
    x_own_x = wire.remote(later_in, mine_x, px)
    x_own_c = wire.remote(later_in, mine_x, pc)
    x_own_xc = wire.remote(beside_x, beside_x, pc)
    up_y = [
        wire.remote(up.at[:, cols(i, 1 - y)], up_full.at[my_rows, strip(i)], py) for i in range(n)
    ]
    h_y = [
        wire.remote(hidden.at[:, cols(i, 1 - y)], h_all.at[half_of(y), strip(i)], py)
        for i in range(n)
    ]

    gds = Sums(wire, gd_part, gd_in, gd_relay, hb, 1 - y, z, n, left, right)
    gus = Sums(wire, gu_part, gu_in, gu_relay, chunk, 1 - y, z, n, left, right)
    at, peers = (x, y, c), (px, py, pc)
    egs = [Plane(wire, eg_bufs, k, at, peers, k >= n - 1) for k in range(n)]
    outs = [Plane(wire, out_bufs, k, at, peers, True) for k in range(2 * n)]
    tile = min(256, chunk)
    slope_rows = min(256, 2 * group)
    theirs, ours = half_of(1 - y), half_of(y)
    lh_y = [wire.remote(lh.at[theirs, strip(i)], lh_o.at[:, cols(i, y)], py) for i in range(n)]
    swap = wire.remote(swap_out, swap_in, py)
    stores = []

    def start(*copies):
        for copy in copies:
            wire.start(copy)

    def arrive(*copies):
        for copy in copies:
            copy.wait_recv()

    def activate(parity):
        def body(i):
            rows = rows_of(parity, i)
            act_t[:, rows] = squared(h_all[rows, :]).T

        loop(group // block, body)

    def column_block(k):
        where = 0
        for i in range(n):
            order = sorted(range(n), key=lambda b: (abs(b - i), b))
            where = where + jnp.where(z == i, order[k], 0)
        return pl.ds(pl.multiple_of(where * chunk, chunk), chunk)

    def store_part(plane, parity, value):
        for q in range(4):
            plane.part[q % 2, q // 2, parity] = value[q * block : (q + 1) * block].astype(BF16)

    far = jnp.where(z < n // 2, n - 1, 0)

    def gd_dots(row, size):
        rows = pl.ds(pl.multiple_of(row, hb), size)

        def body(i):
            columns = pl.ds(pl.multiple_of(i * tile, tile), tile)
            gd_part[rows, columns] = dot(act_t[rows, :], c_all[:, columns]).astype(BF16)

        loop(width // tile, body)

    def pg_dots():
        def body(i):
            rows = pl.ds(pl.multiple_of(i * slope_rows, slope_rows), slope_rows)
            lifted = jnp.maximum(h_all[rows, :].astype(F32), 0.0)
            pg[rows, :] = (2.0 * dot(c_all[rows, :], down_full[...], 1, 1) * lifted).astype(BF16)

        loop(2 * group // slope_rows, body)

    def gu_dots():
        def body(i):
            wide = pl.ds(pl.multiple_of(i * tile, tile), tile)
            gu_part[wide, :] = dot(e_all[:, wide], pg[...], 0, 0).astype(BF16)

        loop(width // tile, body)

    def eg_chunk(k):
        wide = column_block(k)

        def body(parity):
            store_part(egs[k], parity, dot(pg[half_of(parity), :], up_full[wide, :], 1, 1))

        loop(2, body)
        egs[k].begin()

    def out_columns(k):
        return pl.ds(k * (chunk // 2), chunk // 2)

    def out_chunk(k):
        wide = out_columns(k)

        def body(parity):
            store_part(outs[k], parity, dot(act_l[half_of(parity), :], down_full[:, wide]))

        loop(2, body)
        outs[k].begin()

    def lh_early():
        blocks = [column_block(k) for k in range(n - 1)]

        def body(i):
            at = pl.ds(pl.multiple_of(i * slope_rows, slope_rows), slope_rows)
            total = dot(x_all[at, blocks[0]], up_full[blocks[0], :])
            for wide in blocks[1:]:
                total = total + dot(x_all[at, wide], up_full[wide, :])
            lh_sum[at, :] = total

        loop(2 * group // slope_rows, body)

    def lh_late(parity):
        wide = column_block(n - 1)

        def body(i):
            at = pl.ds(pl.multiple_of(parity * group + i * slope_rows, slope_rows), slope_rows)
            h = (lh_sum[at, :] + dot(x_all[at, wide], up_full[wide, :])).astype(BF16)
            lh[at, :] = h
            act_l[at, :] = squared(h)

        loop(group // slope_rows, body)

    def first_sends():
        for p in (0, 1):
            downs.begin(p)
        start(*c_y, *up_y, *h_y, *e_y, *x_y, x_own_x, x_own_c)
        for copy in own_up:
            copy.wait()
        ups.begin_at(0, 0)

    def relay(sums, m):
        for p in (0, 1):
            sums.relay(m, p)

    def own_act():
        for copy in own_h:
            copy.wait()
        activate(y)

    def all_c():
        arrive(*c_c, *c_xc)
        own_c.wait()

    def all_e():
        arrive(*e_c, *e_xc)
        own_e.wait()

    def all_x():
        arrive(x_own_c, x_own_xc, *x_c, *x_xc)
        own_x.wait()

    def pass_on(came, *onward):
        arrive(came)
        start(*onward)

    def lh_send():
        start(*lh_y)

    def lh_store():
        stores.extend(wire.copy(lh.at[ours, strip(i)], lh_o.at[:, cols(i, y)]) for i in range(n))

    def gd_final():
        own_down_sum.wait()
        for p in (0, 1):
            rows = pl.ds(pl.multiple_of(gds.half(p), hb // 2), hb // 2)
            gd_fin[rows, :] = gd_fin[rows, :] + scale * gds.total(p)
        stores.append(wire.copy(gd_fin, gd_o))

    def gu_away():
        swap_out[...] = gus.total(0).astype(BF16)
        start(swap)

    def gu_home():
        own_up_sum.wait()
        total = gus.total(1)
        for i in range(n):
            kept = total[:, i * hb : (i + 1) * hb]
            gu_fin[:, cols(i, y)] = gu_fin[:, cols(i, y)] + scale * kept

    def gu_store():
        arrive(swap)
        for i in range(n):
            came = swap_in[:, strip(i)].astype(F32)
            gu_fin[:, cols(i, 1 - y)] = gu_fin[:, cols(i, 1 - y)] + scale * came
        stores.append(wire.copy(gu_fin, gu_o))

    def eg_store():
        for k in range(n):
            egs[k].last(eg_fin, column_block(k))
        stores.append(wire.copy(eg_fin, eg_o))

    def out_last(k):
        outs[k].last(out_fin, out_columns(k))

    def out_store():
        stores.append(wire.copy(out_fin, out_o))

    def close():
        arrive(*lh_y)
        for copy in stores:
            copy.wait()
        wire.drain()

    def do(name, act, *args):
        with jax.named_scope(name):
            act(*args)

    last = n - 1
    do("first", first_sends)
    do("own_act", own_act)
    do("c_y0", pass_on, c_y[0], c_x[0], c_c[0])
    do("down10", downs.forward, 1, 0)
    do("c_y1", pass_on, c_y[1], c_x[1], c_c[1])
    do("down11", downs.forward, 1, 1)
    ups.begin_at(1, 0)
    do("x_own_x", pass_on, x_own_x, x_own_xc)
    do("up_y", arrive, *up_y)
    for stage in (0, 1):
        ups.begin_at(stage, 1)
    for r in range(2, last):
        do("down20", downs.forward, r, 0)
    for i in (0, 1):
        do("c_x", pass_on, c_x[i], c_xc[i])
    for r in range(2, last):
        do("down21", downs.forward, r, 1)
        for p in (0, 1):
            ups.begin_at(r, p)
    do("h_y", arrive, *h_y)
    do("act2", activate, 1 - y)
    for p in (0, 1):
        do("ups1e", ups.forward, 1, p, True)
    do("c_all", all_c)
    do("gd_far", gd_dots, far * hb, hb)
    gds.seeds([n - 2])
    do("gd_dots", gd_dots, jnp.where(far == 0, hb, 0), half - hb)
    do("gd_seed", gds.seeds, range(n - 3, 0, -1))
    do("e_y0", pass_on, e_y[0], e_x[0], e_c[0])
    for p in (0, 1):
        do("ups1", ups.forward, 1, p, False)
    for r in range(1, n):
        do("down_end", downs.ends, r)
    own_down.wait()
    do("pg", pg_dots)
    do("e_y1", pass_on, e_y[1], e_x[1], e_c[1])
    do("eg0", eg_chunk, 0)
    do("e_x0", pass_on, e_x[0], e_xc[0])
    do("eg0_b", egs[0].second)
    for m in range(n - 3, 0, -1):
        do("gd_relay", relay, gds, m)
    do("x_y0", pass_on, x_y[0], x_x[0], x_c[0])
    do("e_x1", pass_on, e_x[1], e_xc[1])
    do("e_all", all_e)
    do("gu_dots", gu_dots)
    do("gu_seed", gus.seeds, range(n - 2, -1, -1))
    gds.seeds([0])
    do("x_y1", pass_on, x_y[1], x_x[1], x_c[1])
    do("up1_end", ups.ends, 1)
    do("eg1", eg_chunk, 1)
    for r in range(2, last):
        for p in (0, 1):
            do("ups2", ups.forward, r, p)
    do("eg1_b", egs[1].second)
    do("eg0_c", egs[0].third)
    do("gd_relay0", relay, gds, 0)
    for r in range(2, last):
        do("up2_end", ups.ends, r)
        do("eg2", eg_chunk, r)
    for r in range(2, last):
        do("eg2_b", egs[r].second)
    do("eg1_c", egs[1].third)
    for i in (0, 1):
        do("x_x", pass_on, x_x[i], x_xc[i])
    do("x_all", all_x)
    do("lh_early", lh_early)
    for r in range(2, last):
        do("eg2_c", egs[r].third)
    do("up3_end", ups.ends, last)
    do("eg3", eg_chunk, last)
    do("lh_late1", lh_late, 1 - y)
    do("lh_send", lh_send)
    do("lh_late2", lh_late, y)
    do("eg3_b", egs[last].second)
    lh_store()
    do("out0", out_chunk, 0)
    for m in range(n - 3, 0, -1):
        do("gu_relay", relay, gus, m)
    pieces = 2 * n
    for k in range(1, pieces):
        do("out", out_chunk, k)
        do("out_b", outs[k - 1].second)
    do("out_b", outs[pieces - 1].second)
    do("eg3_c", egs[last].third)
    do("out_c", outs[0].third)
    do("gu_relay0", relay, gus, 0)
    for k in range(1, n):
        do("out_c", outs[k].third)
    do("gu_away", gu_away)
    do("eg_fin", eg_store)
    do("gu_home", gu_home)
    for k in range(n, pieces):
        do("out_c", outs[k].third)
        do("out_last", out_last, k - n)
    do("gu_sto", gu_store)
    do("gd_fin", gd_final)
    for k in range(pieces - n, pieces):
        do("out_last", out_last, k)
    do("out_fin", out_store)
    do("close", close)


def fused(n, later_in, earlier_in, hidden, cot, up, down, up_sum, down_sum):
    group, width = earlier_in.shape
    block, hb, up_rows = later_in.shape[0], down.shape[0], up.shape[0]
    half, tokens, chunk = n * hb, 2 * group, 2 * up_rows
    any_space = pl.BlockSpec(memory_space=pl.ANY)
    shapes = (
        jax.ShapeDtypeStruct(later_in.shape, BF16),
        jax.ShapeDtypeStruct(hidden.shape, BF16),
        jax.ShapeDtypeStruct(later_in.shape, BF16),
        jax.ShapeDtypeStruct(up.shape, F32),
        jax.ShapeDtypeStruct(down.shape, F32),
    )
    vm = pltpu.VMEM

    def plane(count, columns):
        leading = (2, 2, 2), (2, 2), (2,), (2,), (), ()
        return [vm((count, *lead, block, columns), BF16) for lead in leading]

    scratch = [
        vm((tokens, width), BF16), vm((tokens, width), BF16), vm((tokens, width), BF16),
        vm((tokens, half), BF16), vm((half, tokens), BF16), vm((tokens, half), BF16),
        vm((width, half), BF16), vm((half, width), BF16),
        vm((half, width), BF16), vm((width, half), BF16),
        vm((2, n - 1, hb, width), BF16), vm((2, max(n - 2, 1), hb, width), BF16),
        vm((2, n - 1, chunk, half), BF16), vm((2, max(n - 2, 1), chunk, half), BF16),
        vm((up_rows, half), BF16), vm((up_rows, half), BF16),
        vm((tokens, half), BF16), vm((tokens, half), BF16), vm((tokens, half), F32),
        *plane(n, chunk), *plane(2 * n, chunk // 2),
        vm((block, width), BF16), vm((block, width), BF16),
        vm((hb, width), F32), vm(up.shape, F32),
    ]
    remote_copies = 36 * n + 40
    local_copies = 3 * n + 10
    return pl.pallas_call(
        functools.partial(layer, n),
        out_shape=shapes,
        in_specs=[any_space] * 8,
        out_specs=(any_space,) * 5,
        scratch_shapes=scratch + [
            pltpu.SemaphoreType.DMA((remote_copies,)),
            pltpu.SemaphoreType.DMA((remote_copies,)),
            pltpu.SemaphoreType.DMA((local_copies,)),
        ],
        compiler_params=pltpu.CompilerParams(
            collective_id=0, has_side_effects=True, vmem_limit_bytes=VMEM_BYTES
        ),
        name="layer",
    )(later_in, earlier_in, hidden, cot, up, down, up_sum, down_sum)


def hand_on(*refs):
    count = (len(refs) - 2) // 3
    came, gone = refs[-2:]
    sources, results, held = refs[:count], refs[count : 2 * count], refs[2 * count : 3 * count]
    pieces = []
    for source, result, hold in zip(sources, results, held):
        parts = 2 if source.dtype == F32 or source.shape[0] > LANES * 2 else 1
        size = source.shape[0] // parts
        for p in range(parts):
            at, i = pl.ds(p * size, size), len(pieces)
            read = pltpu.make_async_copy(source.at[at], hold.at[at], came.at[i])
            write = pltpu.make_async_copy(hold.at[at], result.at[at], gone.at[i])
            read.start()
            pieces.append((read, write))
    for read, write in pieces:
        read.wait()
        write.start()
    for _, write in pieces:
        write.wait()


def handed_on(arrays):
    any_space = pl.BlockSpec(memory_space=pl.ANY)
    return pl.pallas_call(
        hand_on,
        out_shape=tuple(jax.ShapeDtypeStruct(a.shape, a.dtype) for a in arrays),
        in_specs=[any_space] * len(arrays),
        out_specs=(any_space,) * len(arrays),
        scratch_shapes=[pltpu.VMEM(a.shape, a.dtype) for a in arrays]
        + [pltpu.SemaphoreType.DMA((2 * len(arrays),))] * 2,
        name="hand_on",
    )(*arrays)


def portable(n_fs, later_in, earlier_in, hidden, cot, up, down, up_sum, down_sum):
    def split_sum(partial, axis):
        return lax.psum_scatter(partial.astype(F32), axis, scatter_dimension=0, tiled=True)

    up_full = lax.all_gather(up, "fs", axis=0, tiled=True)
    down_full = lax.all_gather(down, "fs", axis=0, tiled=True)
    rows = lax.all_gather(later_in, "tp", axis=0, tiled=True)
    lifted = jnp.maximum(hidden.astype(F32), 0.0)
    gd = split_sum(dot(squared(hidden), cot, 0, 0), "fs")
    pre = (2.0 * dot(cot, down_full, 1, 1) * lifted).astype(BF16)
    gu = split_sum(dot(earlier_in, pre, 0, 0), "fs")
    eg = split_sum(dot(pre, up_full, 1, 1).astype(BF16), "tp").astype(BF16)
    later_hidden = dot(rows, up_full).astype(BF16)
    out = split_sum(dot(squared(later_hidden), down_full).astype(BF16), "tp").astype(BF16)
    scale = float(earlier_in.shape[0] * n_fs) ** (-0.5)
    return out, later_hidden, eg, up_sum + scale * gu, down_sum + scale * gd


def solution(mesh):
    n_fs, n_tp = mesh.shape["fs"], mesh.shape["tp"]

    def shards(*args):
        later_input, up_weight, down_weight = args[0], args[4], args[5]
        planes = n_fs // 2
        fits = (
            n_tp == 4 and n_fs % 2 == 0 and 2 < planes <= 4
            and down_weight.shape[0] % LANES == 0 and up_weight.shape[0] % LANES == 0
            and later_input.shape[0] % LANES == 0
        )
        return handed_on(fused(planes, *args)) if fits else portable(n_fs, *args)

    in_specs = (
        P(("fs", "tp"), None), P("fs", None), P("fs", "tp"), P("fs", None),
        P("fs", "tp"), P(("tp", "fs"), None), P("fs", "tp"), P(("tp", "fs"), None),
    )
    out_specs = (
        P(("fs", "tp"), None), P("fs", "tp"), P(("fs", "tp"), None),
        P("fs", "tp"), P(("tp", "fs"), None),
    )
    return jax.shard_map(shards, mesh=mesh, in_specs=in_specs, out_specs=out_specs, check_vma=False)
```

```python
import functools

import jax
import jax.numpy as jnp
from jax import lax
from jax.experimental import pallas as pl
from jax.experimental.pallas import tpu as pltpu
from jax.sharding import PartitionSpec as P

F32, BF16 = jnp.float32, jnp.bfloat16
MESH = pl.DeviceIdType.MESH
LANES = 128
VMEM_BYTES = 62_000_000


def dot(a, b, ca=1, cb=0):
    return lax.dot_general(a, b, (((ca,), (cb,)), ((), ())), preferred_element_type=F32)


def loop(n, body):
    def step(i, carry):
        body(i)
        return carry

    lax.fori_loop(0, n, step, 0)


def squared(h):
    lifted = jnp.maximum(h.astype(F32), 0.0)
    return (lifted * lifted).astype(BF16)


def both(a, b):
    return jnp.logical_and(a, b)


class Wire:
    def __init__(self, send, recv, local):
        self.send, self.recv, self.local = send, recv, local
        self.n_remote = self.n_local = 0
        self.open = []

    def slot(self):
        self.n_remote += 1
        return self.n_remote - 1

    def remote(self, src, dst, device, slot=None):
        i = self.slot() if slot is None else slot
        return pltpu.make_async_remote_copy(
            src_ref=src, dst_ref=dst, send_sem=self.send.at[i], recv_sem=self.recv.at[i],
            device_id=device, device_id_type=MESH,
        )

    def start(self, copy, when=None):
        if when is None:
            copy.start()
        else:
            pl.when(when)(copy.start)
        self.open.append((copy, when))

    def copy(self, src, dst):
        i = self.n_local
        self.n_local += 1
        made = pltpu.make_async_copy(src, dst, self.local.at[i])
        made.start()
        return made

    def drain(self):
        for copy, when in self.open:
            if when is None:
                copy.wait_send()
            else:
                pl.when(when)(copy.wait_send)


class Line:
    def __init__(self, wire, full, rows, own, swap, z, n, left, right):
        self.wire, self.z, self.n = wire, z, n
        self.right, self.left = {}, {}
        size = rows // 2

        def half(i, p):
            base = lax.rem(i + n, n) * rows + lax.rem(swap + p, 2) * size
            return full.at[pl.ds(pl.multiple_of(base, size), size)]

        for p in (0, 1):
            first = half(z, p)
            if own is not None:
                first = own.at[pl.ds(pl.multiple_of(lax.rem(swap + p, 2) * size, size), size)]
            for r in range(1, n):
                src = first if r == 1 else half(z - r + 1, p)
                self.right[r, p] = wire.remote(src, half(z - r + 1, p), right)
                src = first if r == 1 else half(z + r - 1, p)
                self.left[r, p] = wire.remote(src, half(z + r - 1, p), left)

    def begin(self, p, right=True, left=True):
        self.wire.start(self.right[1, p], both(self.z < self.n - 1, right))
        self.wire.start(self.left[1, p], both(self.z > 0, left))

    def begin_at(self, stage, p):
        self.begin(p, self.z == stage, self.z == self.n - 1 - stage)

    def forward(self, r, p, outer=None):
        z, n = self.z, self.n
        rightward, leftward = both(z >= r, z < n - 1), both(z <= n - 1 - r, z > 0)
        if outer is not None:
            rightward = both(rightward, (z == r) == outer)
            leftward = both(leftward, (z == n - 1 - r) == outer)
        pl.when(rightward)(self.right[r, p].wait_recv)
        self.wire.start(self.right[r + 1, p], rightward)
        pl.when(leftward)(self.left[r, p].wait_recv)
        self.wire.start(self.left[r + 1, p], leftward)

    def ends(self, r, halves=(0, 1)):
        z, n = self.z, self.n
        for p in halves:
            pl.when(both(z >= r, z == n - 1))(self.right[r, p].wait_recv)
            pl.when(both(z <= n - 1 - r, z == 0))(self.left[r, p].wait_recv)


class Sums:
    def __init__(self, wire, part, inbox, relayed, rows, swap, z, n, left, right):
        self.wire, self.part, self.inbox, self.relayed = wire, part, inbox, relayed
        self.rows, self.size, self.swap, self.z, self.n = rows, rows // 2, swap, z, n
        self.seed, self.pass_on = {}, {}
        for way, device in ((0, right), (1, left)):
            for m in range(n - 1):
                for p in (0, 1):
                    slot = wire.slot()
                    at = pl.ds(p * self.size, self.size)
                    dst = inbox.at[way, m, at]
                    src = part.at[self.span(way, m, p)]
                    self.seed[way, m, p] = wire.remote(src, dst, device, slot)
                    if m < n - 2:
                        src = relayed.at[way, m, at]
                        self.pass_on[way, m, p] = wire.remote(src, dst, device, slot)

    def half(self, p):
        return lax.rem(self.swap + p, 2) * self.size

    def span(self, way, m, p):
        ahead = self.z + 1 + m if way == 0 else self.z - 1 - m
        base = lax.rem(ahead + 2 * self.n, self.n) * self.rows + self.half(p)
        return pl.ds(pl.multiple_of(base, self.size), self.size)

    def seeds(self, ms):
        for m in ms:
            for p in (0, 1):
                self.wire.start(self.seed[0, m, p], self.z == 0)
                self.wire.start(self.seed[1, m, p], self.z == self.n - 1)

    def relay(self, m, p):
        z, n = self.z, self.n
        at = pl.ds(p * self.size, self.size)
        for way in (0, 1):
            if way == 0:
                when = both(z >= 1, z + 1 + m <= n - 1)
            else:
                when = both(z <= n - 2, z - 1 - m >= 0)

            def add(way=way):
                self.seed[way, m + 1, p].wait_recv()
                mine = self.part[self.span(way, m, p), :].astype(F32)
                came = self.inbox[way, m + 1, at, :].astype(F32)
                self.relayed[way, m, at, :] = (mine + came).astype(BF16)

            pl.when(when)(add)
            self.wire.start(self.pass_on[way, m, p], when)

    def total(self, p):
        z, n = self.z, self.n
        pl.when(z >= 1)(self.seed[0, 0, p].wait_recv)
        pl.when(z <= n - 2)(self.seed[1, 0, p].wait_recv)
        at = pl.ds(p * self.size, self.size)
        base = z * self.rows + self.half(p)
        mine = self.part[pl.ds(pl.multiple_of(base, self.size), self.size), :].astype(F32)
        first = jnp.where(z >= 1, self.inbox[0, 0, at, :].astype(F32), 0.0)
        second = jnp.where(z <= n - 2, self.inbox[1, 0, at, :].astype(F32), 0.0)
        return mine + first + second


class Plane:
    def __init__(self, wire, bufs, k, at, peers, x_first, slots=None):
        self.part, self.in_a, self.to_b, self.in_b, self.to_c, self.in_c = (b.at[k] for b in bufs)
        self.wire, self.x_first = wire, x_first
        x, y, self.core = at
        self.one, self.two = (x, y) if x_first else (y, x)
        if slots is None:
            slot = [None] * 3
        else:
            slot = [slots[0] + 3 * k + i for i in range(3)]
        self.a = wire.remote(self.part.at[1 - self.core], self.in_a, peers[2], slot[0])
        self.b = wire.remote(self.to_b, self.in_b, peers[0 if x_first else 1], slot[1])
        self.c = wire.remote(self.to_c, self.in_c, peers[1 if x_first else 0], slot[2])

    def pair(self, one, two):
        i, j = (one, two) if self.x_first else (two, one)
        return self.part[self.core, i, j].astype(F32) + self.in_a[i, j].astype(F32)

    def mine(self, two):
        return self.pair(self.one, two) + self.in_b[two].astype(F32)

    def begin(self):
        self.wire.start(self.a)

    def second(self):
        self.a.wait_recv()
        for two in (0, 1):
            self.to_b[two] = self.pair(1 - self.one, two).astype(BF16)
        self.wire.start(self.b)

    def third(self):
        self.b.wait_recv()
        self.to_c[...] = self.mine(1 - self.two).astype(BF16)
        self.wire.start(self.c)

    def last(self, out, columns):
        self.c.wait_recv()
        out[:, columns] = (self.mine(self.two) + self.in_c[...].astype(F32)).astype(BF16)


def layer(
    n, later_in, earlier_in, hidden, cot, up, down, up_sum, down_sum,
    out_o, lh_o, eg_o, gu_o, gd_o,
    c_all, e_all, x_all, h_all, act_t, pg, up_full, down_full, gd_part, gu_part,
    gd_in, gd_relay, gu_in, gu_relay, swap_out, swap_in, lh, act_l, lh_sum,
    *rest,
):
    eg_bufs, tail_bufs, out_bufs = rest[:6], rest[6:12], rest[12:18]
    send, recv, local = rest[18:]
    fs, tp = lax.axis_index("fs"), lax.axis_index("tp")
    z, y = fs // 2, fs % 2
    x, c = tp // 2, tp % 2
    py, px, pc = (fs + 1 - 2 * y, tp), (fs, tp + 2 - 4 * x), (fs, tp + 1 - 2 * c)
    left, right = (lax.rem(fs + 2 * n - 2, 2 * n), tp), (lax.rem(fs + 2, 2 * n), tp)

    group, width = earlier_in.shape
    block = later_in.shape[0]
    hb = down.shape[0]
    half = n * hb
    up_rows = up.shape[0]
    chunk = 2 * up_rows
    wire = Wire(send, recv, local)

    def cols(i, parity):
        return pl.ds(pl.multiple_of((2 * i + parity) * hb, hb), hb)

    def strip(i):
        return pl.ds(i * hb, hb)

    def rows_of(parity, q):
        return pl.ds(pl.multiple_of(parity * group + q * block, block), block)

    def half_of(parity):
        return pl.ds(pl.multiple_of(parity * group, group), group)

    barrier = pltpu.get_barrier_semaphore()

    def greet(device):
        pl.semaphore_signal(barrier, inc=1, device_id=device, device_id_type=MESH)

    for device in (py, px, pc):
        greet(device)
    pl.when(z > 0)(lambda: greet(left))
    pl.when(z < n - 1)(lambda: greet(right))

    own_h = [wire.copy(hidden.at[:, cols(i, y)], h_all.at[half_of(y), strip(i)]) for i in range(n)]
    my_rows = pl.ds(pl.multiple_of(fs * up_rows, up_rows), up_rows)
    own_up = [wire.copy(up.at[:, cols(i, y)], up_full.at[my_rows, strip(i)]) for i in range(n)]
    own_c = wire.copy(cot, c_all.at[half_of(y)])
    own_down = wire.copy(down, down_full.at[pl.ds(pl.multiple_of(z * hb, hb), hb)])
    own_e = wire.copy(earlier_in, e_all.at[half_of(y)])
    own_x = wire.copy(later_in, x_all.at[rows_of(y, tp)])
    own_up_sum = wire.copy(up_sum, gu_o)
    own_down_sum = wire.copy(down_sum, gd_o)
    scale = float(group * 2 * n) ** (-0.5)

    pl.semaphore_wait(barrier, 3 + (z > 0).astype(jnp.int32) + (z < n - 1).astype(jnp.int32))

    def spread(whole, source, first, parts):
        size = block // parts

        def sub(parity, q, i):
            base = parity * group + q * block + i * size
            return whole.at[pl.ds(pl.multiple_of(base, size), size)]

        made = []
        for i in range(parts):
            there, came = sub(y, tp, i), sub(1 - y, tp, i)
            beside = sub(1 - y, tp + 2 - 4 * x, i)
            src = source.at[pl.ds(pl.multiple_of(first + i * size, size), size)]
            made.append((
                wire.remote(src, there, py), wire.remote(came, came, px),
                wire.remote(came, came, pc), wire.remote(beside, beside, pc),
            ))
        return zip(*made)

    downs = Line(wire, down_full, hb, down, y, z, n, left, right)
    ups = Line(wire, up_full, chunk, None, y, z, n, left, right)
    c_y, c_x, c_c, c_xc = spread(c_all, cot, tp * block, 2)
    e_y, e_x, e_c, e_xc = spread(e_all, earlier_in, tp * block, 2)
    x_y, x_x, x_c, x_xc = spread(x_all, later_in, 0, 2)
    mine_x = x_all.at[rows_of(y, tp)]
    beside_x = x_all.at[rows_of(y, tp + 2 - 4 * x)]
    x_own_x = wire.remote(later_in, mine_x, px)
    x_own_c = wire.remote(later_in, mine_x, pc)
    x_own_xc = wire.remote(beside_x, beside_x, pc)
    up_y = [
        wire.remote(up.at[:, cols(i, 1 - y)], up_full.at[my_rows, strip(i)], py) for i in range(n)
    ]
    far = jnp.where(z < n // 2, n - 1, 0)
    strips = [lax.rem(far + i, n) for i in range(n)]

    def strip_at(i):
        return pl.ds(pl.multiple_of(strips[i] * hb, hb), hb)

    h_y = [
        wire.remote(hidden.at[:, cols(strips[i], 1 - y)], h_all.at[half_of(y), strip_at(i)], py)
        for i in range(n)
    ]

    gds = Sums(wire, gd_part, gd_in, gd_relay, hb, 1 - y, z, n, left, right)
    gus = Sums(wire, gu_part, gu_in, gu_relay, chunk, 1 - y, z, n, left, right)
    at, peers = (x, y, c), (px, py, pc)
    egs = [Plane(wire, eg_bufs, k, at, peers, False) for k in range(n - 1)]
    slots = [wire.slot() for _ in range(6)]
    tails = [
        Plane(wire, tail_bufs, lax.rem(y + p, 2), at, peers, True, slots) for p in (0, 1)
    ]
    outs = [Plane(wire, out_bufs, k, at, peers, True) for k in range(2 * n)]
    tile = min(256, chunk)
    slope_rows = min(256, 2 * group)
    lh_y = [wire.remote(lh.at[:, strip(i)], lh_o.at[:, cols(i, y)], py) for i in range(n)]
    swap = wire.remote(swap_out, swap_in, py)

    def start(*copies):
        for copy in copies:
            wire.start(copy)

    def arrive(*copies):
        for copy in copies:
            copy.wait_recv()

    def activate(parity, i):
        def body(j):
            rows = rows_of(parity, j)
            act_t[strip_at(i), rows] = squared(h_all[rows, strip_at(i)]).T

        loop(group // block, body)

    def column_block(k):
        where = 0
        for i in range(n):
            order = sorted(range(n), key=lambda b: (abs(b - i), b))
            where = where + jnp.where(z == i, order[k], 0)
        return pl.ds(pl.multiple_of(where * chunk, chunk), chunk)

    def store_part(plane, parity, value):
        for q in range(4):
            plane.part[q % 2, q // 2, parity] = value[q * block : (q + 1) * block].astype(BF16)

    def gd_dots(row, size):
        rows = pl.ds(pl.multiple_of(row, hb), size)

        def body(i):
            columns = pl.ds(pl.multiple_of(i * tile, tile), tile)
            gd_part[rows, columns] = dot(act_t[rows, :], c_all[:, columns]).astype(BF16)

        loop(width // tile, body)

    def pg_dots():
        def body(i):
            rows = pl.ds(pl.multiple_of(i * slope_rows, slope_rows), slope_rows)
            lifted = jnp.maximum(h_all[rows, :].astype(F32), 0.0)
            pg[rows, :] = (2.0 * dot(c_all[rows, :], down_full[...], 1, 1) * lifted).astype(BF16)

        loop(2 * group // slope_rows, body)

    def gu_dots():
        def body(i):
            wide = pl.ds(pl.multiple_of(i * tile, tile), tile)
            gu_part[wide, :] = dot(e_all[:, wide], pg[...], 0, 0).astype(BF16)

        loop(width // tile, body)

    def tail_columns(p):
        base = column_block(n - 1).start + lax.rem(y + p, 2) * up_rows
        return pl.ds(pl.multiple_of(base, up_rows), up_rows)

    def tail_chunk(p):
        wide = tail_columns(p)

        def body(parity):
            store_part(tails[p], parity, dot(pg[half_of(parity), :], up_full[wide, :], 1, 1))

        loop(2, body)
        tails[p].begin()

    def eg_chunk(k):
        wide = column_block(k)

        def body(parity):
            store_part(egs[k], parity, dot(pg[half_of(parity), :], up_full[wide, :], 1, 1))

        loop(2, body)
        egs[k].begin()

    def out_columns(k):
        return pl.ds(k * (chunk // 2), chunk // 2)

    def out_chunk(k):
        wide = out_columns(k)

        def body(parity):
            store_part(outs[k], parity, dot(act_l[half_of(parity), :], down_full[:, wide]))

        loop(2, body)
        outs[k].begin()

    def lh_early():
        blocks = [column_block(k) for k in range(n - 1)] + [tail_columns(0)]

        def body(i):
            at = pl.ds(pl.multiple_of(i * slope_rows, slope_rows), slope_rows)
            total = dot(x_all[at, blocks[0]], up_full[blocks[0], :])
            for wide in blocks[1:]:
                total = total + dot(x_all[at, wide], up_full[wide, :])
            lh_sum[at, :] = total

        loop(2 * group // slope_rows, body)

    def lh_late(parity):
        wide = tail_columns(1)

        def body(i):
            base = pl.multiple_of(i * slope_rows, slope_rows)
            at = pl.ds(pl.multiple_of(parity * group + base, slope_rows), slope_rows)
            h = (lh_sum[at, :] + dot(x_all[at, wide], up_full[wide, :])).astype(BF16)
            act_l[at, :] = squared(h)
            return base, at, h

        def away(i):
            _, at, h = body(i)
            lh[pl.ds(pl.multiple_of(i * slope_rows, slope_rows), slope_rows), :] = h

        def home(i):
            base, _, h = body(i)
            for j in range(n):
                lh_o[pl.ds(base, slope_rows), cols(j, y)] = h[:, j * hb : (j + 1) * hb]

        return away, home

    def lh_away():
        loop(group // slope_rows, lh_late(1 - y)[0])

    def lh_home():
        loop(group // slope_rows, lh_late(y)[1])

    def first_sends():
        for p in (0, 1):
            downs.begin(p)
        start(*c_y, h_y[0], *up_y, *h_y[1:], *e_y, *x_y, x_own_x, x_own_c)
        for copy in own_up:
            copy.wait()
        ups.begin_at(0, 0)

    def relay(sums, m):
        for p in (0, 1):
            sums.relay(m, p)

    def own_act():
        for copy in own_h:
            copy.wait()
        for i in range(n):
            activate(y, i)

    def all_c():
        arrive(*c_c, *c_xc)
        own_c.wait()

    def all_e():
        arrive(*e_c, *e_xc)
        own_e.wait()

    def all_x():
        arrive(x_own_c, x_own_xc, *x_c, *x_xc)
        own_x.wait()

    def pass_on(came, *onward):
        arrive(came)
        start(*onward)

    def lh_send():
        start(*lh_y)

    def gd_oal():
        own_down_sum.wait()
        for p in (0, 1):
            rows = pl.ds(pl.multiple_of(gds.half(p), hb // 2), hb // 2)
            gd_o[rows, :] = gd_o[rows, :] + scale * gds.total(p)

    def gu_away():
        swap_out[...] = gus.total(0).astype(BF16)
        start(swap)

    def gu_home():
        own_up_sum.wait()
        total = gus.total(1)
        for i in range(n):
            kept = total[:, i * hb : (i + 1) * hb]
            gu_o[:, cols(i, y)] = gu_o[:, cols(i, y)] + scale * kept

    def gu_store():
        arrive(swap)
        for i in range(n):
            came = swap_in[:, strip(i)].astype(F32)
            gu_o[:, cols(i, 1 - y)] = gu_o[:, cols(i, 1 - y)] + scale * came

    def eg_store():
        for k in range(n - 1):
            egs[k].last(eg_o, column_block(k))
        for p in (0, 1):
            tails[p].last(eg_o, tail_columns(p))

    def out_last(k):
        outs[k].last(out_o, out_columns(k))

    def close():
        arrive(*lh_y)
        wire.drain()

    def do(name, act, *args):
        with jax.named_scope(name):
            act(*args)

    last = n - 1
    do("first", first_sends)
    do("own_act", own_act)
    do("c_y0", pass_on, c_y[0], c_x[0], c_c[0])
    do("down10", downs.forward, 1, 0)
    do("c_y1", pass_on, c_y[1], c_x[1], c_c[1])
    do("down11", downs.forward, 1, 1)
    ups.begin_at(1, 0)
    do("x_own_x", pass_on, x_own_x, x_own_xc)
    do("up_y", arrive, *up_y)
    for stage in (0, 1):
        ups.begin_at(stage, 1)
    for r in range(2, last):
        do("down20", downs.forward, r, 0)
    for i in (0, 1):
        do("c_x", pass_on, c_x[i], c_xc[i])
    for r in range(2, last):
        do("down21", downs.forward, r, 1)
        for p in (0, 1):
            ups.begin_at(r, p)
    do("h_y0", arrive, h_y[0])
    do("act2", activate, 1 - y, 0)
    do("c_all", all_c)
    do("gd_far", gd_dots, far * hb, hb)
    gds.seeds([n - 2])
    do("h_y", arrive, *h_y[1:])
    for i in range(1, n):
        do("act2", activate, 1 - y, i)
    for p in (0, 1):
        do("ups1e", ups.forward, 1, p, True)
    do("gd_dots", gd_dots, jnp.where(far == 0, hb, 0), half - hb)
    do("gd_seed", gds.seeds, range(n - 3, 0, -1))
    do("e_y0", pass_on, e_y[0], e_x[0], e_c[0])
    for p in (0, 1):
        do("ups1", ups.forward, 1, p, False)
    for r in range(1, n):
        do("down_end", downs.ends, r)
    own_down.wait()
    do("pg", pg_dots)
    do("e_y1", pass_on, e_y[1], e_x[1], e_c[1])
    do("eg0", eg_chunk, 0)
    do("e_x0", pass_on, e_x[0], e_xc[0])
    do("eg0_b", egs[0].second)
    for m in range(n - 3, 0, -1):
        do("gd_relay", relay, gds, m)
    do("x_y0", pass_on, x_y[0], x_x[0], x_c[0])
    do("e_x1", pass_on, e_x[1], e_xc[1])
    do("e_all", all_e)
    do("gu_dots", gu_dots)
    do("gu_seed", gus.seeds, range(n - 2, -1, -1))
    do("x_y1", pass_on, x_y[1], x_x[1], x_c[1])
    do("up1_end", ups.ends, 1)
    do("eg1", eg_chunk, 1)
    for r in range(2, last):
        for p in (0, 1):
            do("ups2", ups.forward, r, p)
    do("eg1_b", egs[1].second)
    do("eg0_c", egs[0].third)
    do("gd_relay0", relay, gds, 0)
    for r in range(2, last):
        do("up2_end", ups.ends, r)
        do("eg2", eg_chunk, r)
    for r in range(2, last):
        do("eg2_b", egs[r].second)
    do("eg1_c", egs[1].third)
    for i in (0, 1):
        do("x_x", pass_on, x_x[i], x_xc[i])
    for m in range(n - 3, 0, -1):
        do("gu_relay_0", gus.relay, m, 0)
    do("up3_0", ups.ends, last, (0,))
    do("eg3_0", tail_chunk, 0)
    do("x_all", all_x)
    do("eg3_0b", tails[0].second)
    do("lh_early", lh_early)
    for m in range(n - 3, 0, -1):
        do("gu_relay_1", gus.relay, m, 1)
    for r in range(2, last):
        do("eg2_c", egs[r].third)
    do("up3_1", ups.ends, last, (1,))
    do("eg3_1", tail_chunk, 1)
    do("lh_away", lh_away)
    do("lh_send", lh_send)
    do("lh_home", lh_home)
    do("eg3_1b", tails[1].second)
    do("out0", out_chunk, 0)
    pieces = 2 * n
    for k in range(1, pieces):
        do("out", out_chunk, k)
        do("out_b", outs[k - 1].second)
    do("out_b", outs[pieces - 1].second)
    gds.seeds([0])
    for p in (0, 1):
        do("eg3_c", tails[p].third)
    do("out_c", outs[0].third)
    do("gu_relay0", relay, gus, 0)
    for k in range(1, n - 1):
        do("out_c", outs[k].third)
    do("gu_away", gu_away)
    do("eg_fin", eg_store)
    for k in range(n - 1, n + 2):
        do("out_c", outs[k].third)
    do("gu_home", gu_home)
    for k in range(n + 2, pieces):
        do("out_c", outs[k].third)
        do("out_last", out_last, k - n - 2)
    for k in range(pieces - n - 2, n):
        do("out_last", out_last, k)
    do("gu_sto", gu_store)
    do("gd_o", gd_oal)
    for k in range(pieces - n, pieces):
        do("out_last", out_last, k)
    do("close", close)


def fused(n, later_in, earlier_in, hidden, cot, up, down, up_sum, down_sum):
    group, width = earlier_in.shape
    block, hb, up_rows = later_in.shape[0], down.shape[0], up.shape[0]
    half, tokens, chunk = n * hb, 2 * group, 2 * up_rows
    any_space = pl.BlockSpec(memory_space=pl.ANY)
    vm = pltpu.VMEM
    results = (
        vm(later_in.shape, BF16), vm(hidden.shape, BF16), vm(later_in.shape, BF16),
        vm(up.shape, F32), vm(down.shape, F32),
    )

    def plane(count, columns):
        leading = (2, 2, 2), (2, 2), (2,), (2,), (), ()
        return [vm((count, *lead, block, columns), BF16) for lead in leading]

    scratch = [
        vm((tokens, width), BF16), vm((tokens, width), BF16), vm((tokens, width), BF16),
        vm((tokens, half), BF16), vm((half, tokens), BF16), vm((tokens, half), BF16),
        vm((width, half), BF16), vm((half, width), BF16),
        vm((half, width), BF16), vm((width, half), BF16),
        vm((2, n - 1, hb, width), BF16), vm((2, max(n - 2, 1), hb, width), BF16),
        vm((2, n - 1, chunk, half), BF16), vm((2, max(n - 2, 1), chunk, half), BF16),
        vm((up_rows, half), BF16), vm((up_rows, half), BF16),
        vm((group, half), BF16), vm((tokens, half), BF16), vm((tokens, half), F32),
        *plane(n - 1, chunk), *plane(2, chunk // 2), *plane(2 * n, chunk // 2),
    ]
    remote_copies = 36 * n + 40
    local_copies = 3 * n + 10
    return pl.pallas_call(
        functools.partial(layer, n),
        out_shape=results,
        in_specs=[any_space] * 8,
        out_specs=(pl.BlockSpec(memory_space=vm),) * 5,
        scratch_shapes=scratch + [
            pltpu.SemaphoreType.DMA((remote_copies,)),
            pltpu.SemaphoreType.DMA((remote_copies,)),
            pltpu.SemaphoreType.DMA((local_copies,)),
        ],
        compiler_params=pltpu.CompilerParams(
            collective_id=0, has_side_effects=True, vmem_limit_bytes=VMEM_BYTES
        ),
        name="layer",
    )(later_in, earlier_in, hidden, cot, up, down, up_sum, down_sum)


def hand_on(*refs):
    count = (len(refs) - 1) // 2
    sources, results, gone = refs[:count], refs[count : 2 * count], refs[-1]
    copies = [
        pltpu.make_async_copy(source, result, gone.at[i])
        for i, (source, result) in enumerate(zip(sources, results))
    ]
    for copy in copies:
        copy.start()
    for copy in copies:
        copy.wait()


def handed_on(arrays):
    count = len(arrays)
    held = [pltpu.with_memory_space_constraint(a, pltpu.VMEM) for a in arrays]
    return pl.pallas_call(
        hand_on,
        out_shape=tuple(pltpu.HBM(a.shape, a.dtype) for a in arrays),
        in_specs=[pl.BlockSpec(memory_space=pltpu.VMEM)] * count,
        out_specs=(pl.BlockSpec(memory_space=pltpu.HBM),) * count,
        scratch_shapes=[pltpu.SemaphoreType.DMA((count,))],
        compiler_params=pltpu.CompilerParams(vmem_limit_bytes=1 << 20),
        name="hand_on",
    )(*held)


def portable(n_fs, later_in, earlier_in, hidden, cot, up, down, up_sum, down_sum):
    def split_sum(partial, axis):
        return lax.psum_scatter(partial.astype(F32), axis, scatter_dimension=0, tiled=True)

    up_full = lax.all_gather(up, "fs", axis=0, tiled=True)
    down_full = lax.all_gather(down, "fs", axis=0, tiled=True)
    rows = lax.all_gather(later_in, "tp", axis=0, tiled=True)
    lifted = jnp.maximum(hidden.astype(F32), 0.0)
    gd = split_sum(dot(squared(hidden), cot, 0, 0), "fs")
    pre = (2.0 * dot(cot, down_full, 1, 1) * lifted).astype(BF16)
    gu = split_sum(dot(earlier_in, pre, 0, 0), "fs")
    eg = split_sum(dot(pre, up_full, 1, 1).astype(BF16), "tp").astype(BF16)
    later_hidden = dot(rows, up_full).astype(BF16)
    out = split_sum(dot(squared(later_hidden), down_full).astype(BF16), "tp").astype(BF16)
    scale = float(earlier_in.shape[0] * n_fs) ** (-0.5)
    return out, later_hidden, eg, up_sum + scale * gu, down_sum + scale * gd


def solution(mesh):
    n_fs, n_tp = mesh.shape["fs"], mesh.shape["tp"]

    def shards(*args):
        later_input, up_weight, down_weight = args[0], args[4], args[5]
        planes = n_fs // 2
        fits = (
            n_tp == 4 and n_fs % 2 == 0 and 2 < planes <= 4
            and down_weight.shape[0] % LANES == 0 and up_weight.shape[0] % LANES == 0
            and later_input.shape[0] % LANES == 0
        )
        return handed_on(fused(planes, *args)) if fits else portable(n_fs, *args)

    in_specs = (
        P(("fs", "tp"), None), P("fs", None), P("fs", "tp"), P("fs", None),
        P("fs", "tp"), P(("tp", "fs"), None), P("fs", "tp"), P(("tp", "fs"), None),
    )
    out_specs = (
        P(("fs", "tp"), None), P("fs", "tp"), P(("fs", "tp"), None),
        P("fs", "tp"), P(("tp", "fs"), None),
    )
    return jax.shard_map(shards, mesh=mesh, in_specs=in_specs, out_specs=out_specs, check_vma=False)
```

```python
import functools

import jax
import jax.numpy as jnp
from jax import lax
from jax.experimental import pallas as pl
from jax.experimental.pallas import tpu as pltpu
from jax.sharding import PartitionSpec as P

F32, BF16 = jnp.float32, jnp.bfloat16
MESH = pl.DeviceIdType.MESH
LANES = 128
VMEM_BYTES = 62_000_000
SENDS = 84


def dot(a, b, ca=1, cb=0):
    return lax.dot_general(a, b, (((ca,), (cb,)), ((), ())), preferred_element_type=F32)


def loop(n, body):
    def step(i, carry):
        body(i)
        return carry

    lax.fori_loop(0, n, step, 0)


def squared(h):
    lifted = jnp.maximum(h.astype(F32), 0.0)
    return (lifted * lifted).astype(BF16)


def both(a, b):
    return jnp.logical_and(a, b)


class Hop:
    def __init__(self, wire, src, dst, device, slot):
        self.wire, self.src, self.dst, self.device, self.slot = wire, src, dst, device, slot

    def made(self, place):
        return pltpu.make_async_remote_copy(
            src_ref=self.src, dst_ref=self.dst, send_sem=self.wire.send.at[place],
            recv_sem=self.wire.recv.at[self.slot], device_id=self.device, device_id_type=MESH,
        )

    def wait_recv(self):
        self.made(0).wait_recv()


class Wire:
    def __init__(self, send, recv, local):
        self.send, self.recv, self.local = send, recv, local
        self.n_remote = self.n_local = 0
        self.busy = [None] * send.shape[0]

    def slot(self):
        self.n_remote += 1
        return self.n_remote - 1

    def remote(self, src, dst, device, slot=None):
        return Hop(self, src, dst, device, self.slot() if slot is None else slot)

    def free(self, place):
        copy, when, _ = self.busy[place]
        if when is None:
            copy.wait_send()
        else:
            pl.when(when)(copy.wait_send)
        self.busy[place] = None

    def settle(self, hops):
        for place, held in enumerate(self.busy):
            if held is not None and held[2] in hops:
                self.free(place)

    def start(self, hop, when=None):
        place = self.busy.index(None)
        copy = hop.made(place)
        if when is None:
            copy.start()
        else:
            pl.when(when)(copy.start)
        self.busy[place] = (copy, when, hop)

    def copy(self, src, dst):
        i = self.n_local
        self.n_local += 1
        made = pltpu.make_async_copy(src, dst, self.local.at[i])
        made.start()
        return made

    def drain(self):
        for place, held in enumerate(self.busy):
            if held is not None:
                self.free(place)


class Line:
    def __init__(self, wire, full, rows, own, swap, z, n, left, right):
        self.wire, self.z, self.n = wire, z, n
        self.right, self.left = {}, {}
        size = rows // 2

        def half(i, p):
            base = lax.rem(i + n, n) * rows + lax.rem(swap + p, 2) * size
            return full.at[pl.ds(pl.multiple_of(base, size), size)]

        for p in (0, 1):
            first = half(z, p)
            if own is not None:
                first = own.at[pl.ds(pl.multiple_of(lax.rem(swap + p, 2) * size, size), size)]
            for r in range(1, n):
                src = first if r == 1 else half(z - r + 1, p)
                self.right[r, p] = wire.remote(src, half(z - r + 1, p), right)
                src = first if r == 1 else half(z + r - 1, p)
                self.left[r, p] = wire.remote(src, half(z + r - 1, p), left)

    def begin(self, p, right=True, left=True):
        self.wire.start(self.right[1, p], both(self.z < self.n - 1, right))
        self.wire.start(self.left[1, p], both(self.z > 0, left))

    def begin_at(self, stage, p):
        self.begin(p, self.z == stage, self.z == self.n - 1 - stage)

    def forward(self, r, p, outer=None):
        z, n = self.z, self.n
        rightward, leftward = both(z >= r, z < n - 1), both(z <= n - 1 - r, z > 0)
        if outer is not None:
            rightward = both(rightward, (z == r) == outer)
            leftward = both(leftward, (z == n - 1 - r) == outer)
        pl.when(rightward)(self.right[r, p].wait_recv)
        self.wire.start(self.right[r + 1, p], rightward)
        pl.when(leftward)(self.left[r, p].wait_recv)
        self.wire.start(self.left[r + 1, p], leftward)

    def ends(self, r, halves=(0, 1)):
        z, n = self.z, self.n
        for p in halves:
            pl.when(both(z >= r, z == n - 1))(self.right[r, p].wait_recv)
            pl.when(both(z <= n - 1 - r, z == 0))(self.left[r, p].wait_recv)


class Sums:
    def __init__(self, wire, part, inbox, relayed, rows, swap, z, n, left, right):
        self.wire, self.part, self.inbox, self.relayed = wire, part, inbox, relayed
        self.rows, self.size, self.swap, self.z, self.n = rows, rows // 2, swap, z, n
        self.seed, self.pass_on = {}, {}
        for way, device in ((0, right), (1, left)):
            for m in range(n - 1):
                for p in (0, 1):
                    slot = wire.slot()
                    at = pl.ds(p * self.size, self.size)
                    dst = inbox.at[way, m, at]
                    src = part.at[self.span(way, m, p)]
                    self.seed[way, m, p] = wire.remote(src, dst, device, slot)
                    if m < n - 2:
                        src = relayed.at[way, m, at]
                        self.pass_on[way, m, p] = wire.remote(src, dst, device, slot)

    def half(self, p):
        return lax.rem(self.swap + p, 2) * self.size

    def span(self, way, m, p):
        ahead = self.z + 1 + m if way == 0 else self.z - 1 - m
        base = lax.rem(ahead + 2 * self.n, self.n) * self.rows + self.half(p)
        return pl.ds(pl.multiple_of(base, self.size), self.size)

    def seeds(self, ms):
        for m in ms:
            for p in (0, 1):
                self.wire.start(self.seed[0, m, p], self.z == 0)
                self.wire.start(self.seed[1, m, p], self.z == self.n - 1)

    def relay(self, m, p):
        z, n = self.z, self.n
        at = pl.ds(p * self.size, self.size)
        for way in (0, 1):
            if way == 0:
                when = both(z >= 1, z + 1 + m <= n - 1)
            else:
                when = both(z <= n - 2, z - 1 - m >= 0)

            def add(way=way):
                self.seed[way, m + 1, p].wait_recv()
                mine = self.part[self.span(way, m, p), :].astype(F32)
                came = self.inbox[way, m + 1, at, :].astype(F32)
                self.relayed[way, m, at, :] = (mine + came).astype(BF16)

            pl.when(when)(add)
            self.wire.start(self.pass_on[way, m, p], when)

    def total(self, p):
        z, n = self.z, self.n
        pl.when(z >= 1)(self.seed[0, 0, p].wait_recv)
        pl.when(z <= n - 2)(self.seed[1, 0, p].wait_recv)
        at = pl.ds(p * self.size, self.size)
        base = z * self.rows + self.half(p)
        mine = self.part[pl.ds(pl.multiple_of(base, self.size), self.size), :].astype(F32)
        first = jnp.where(z >= 1, self.inbox[0, 0, at, :].astype(F32), 0.0)
        second = jnp.where(z <= n - 2, self.inbox[1, 0, at, :].astype(F32), 0.0)
        return mine + first + second


class Plane:
    def __init__(self, wire, bufs, k, at, peers, x_first, slots=None):
        self.part, self.in_a, self.to_b, self.in_b, self.to_c, self.in_c = (b.at[k] for b in bufs)
        self.wire, self.x_first = wire, x_first
        x, y, self.core = at
        self.one, self.two = (x, y) if x_first else (y, x)
        if slots is None:
            slot = [None] * 3
        else:
            slot = [slots[0] + 3 * k + i for i in range(3)]
        self.a = wire.remote(self.part.at[1 - self.core], self.in_a, peers[2], slot[0])
        self.b = wire.remote(self.to_b, self.in_b, peers[0 if x_first else 1], slot[1])
        self.c = wire.remote(self.to_c, self.in_c, peers[1 if x_first else 0], slot[2])

    def pair(self, one, two):
        i, j = (one, two) if self.x_first else (two, one)
        return self.part[self.core, i, j].astype(F32) + self.in_a[i, j].astype(F32)

    def mine(self, two):
        return self.pair(self.one, two) + self.in_b[two].astype(F32)

    def begin(self):
        self.wire.start(self.a)

    def second(self):
        self.a.wait_recv()
        for two in (0, 1):
            self.to_b[two] = self.pair(1 - self.one, two).astype(BF16)
        self.wire.start(self.b)

    def third(self):
        self.b.wait_recv()
        self.to_c[...] = self.mine(1 - self.two).astype(BF16)
        self.wire.start(self.c)

    def last(self, out, columns):
        self.c.wait_recv()
        out[:, columns] = (self.mine(self.two) + self.in_c[...].astype(F32)).astype(BF16)


def layer(
    n, later_in, earlier_in, hidden, cot, up, down, up_sum, down_sum,
    out_o, lh_o, eg_o, gu_o, gd_o,
    c_all, e_all, x_all, h_all, act_t, pg, up_full, down_full, gd_part, gu_part,
    gd_in, gd_relay, gu_in, gu_relay, swap_out, swap_in, lh, act_l, lh_sum,
    *rest,
):
    eg_bufs, tail_bufs, out_bufs, end_bufs = (rest[i : i + 6] for i in range(0, 24, 6))
    send, recv, local = rest[24:]
    fs, tp = lax.axis_index("fs"), lax.axis_index("tp")
    z, y = fs // 2, fs % 2
    x, c = tp // 2, tp % 2
    py, px, pc = (fs + 1 - 2 * y, tp), (fs, tp + 2 - 4 * x), (fs, tp + 1 - 2 * c)
    left, right = (lax.rem(fs + 2 * n - 2, 2 * n), tp), (lax.rem(fs + 2, 2 * n), tp)

    group, width = earlier_in.shape
    block = later_in.shape[0]
    hb = down.shape[0]
    half = n * hb
    up_rows = up.shape[0]
    chunk = 2 * up_rows
    wire = Wire(send, recv, local)

    def cols(i, parity):
        return pl.ds(pl.multiple_of((2 * i + parity) * hb, hb), hb)

    def strip(i):
        return pl.ds(i * hb, hb)

    def rows_of(parity, q):
        return pl.ds(pl.multiple_of(parity * group + q * block, block), block)

    def half_of(parity):
        return pl.ds(pl.multiple_of(parity * group, group), group)

    barrier = pltpu.get_barrier_semaphore()

    def greet(device):
        pl.semaphore_signal(barrier, inc=1, device_id=device, device_id_type=MESH)

    for device in (py, px, pc):
        greet(device)
    pl.when(z > 0)(lambda: greet(left))
    pl.when(z < n - 1)(lambda: greet(right))

    own_h = [wire.copy(hidden.at[:, cols(i, y)], h_all.at[half_of(y), strip(i)]) for i in range(n)]
    my_rows = pl.ds(pl.multiple_of(fs * up_rows, up_rows), up_rows)
    own_up = [wire.copy(up.at[:, cols(i, y)], up_full.at[my_rows, strip(i)]) for i in range(n)]
    own_c = wire.copy(cot, c_all.at[half_of(y)])
    own_down = wire.copy(down, down_full.at[pl.ds(pl.multiple_of(z * hb, hb), hb)])
    own_e = wire.copy(earlier_in, e_all.at[half_of(y)])
    own_x = wire.copy(later_in, x_all.at[rows_of(y, tp)])
    own_up_sum = wire.copy(up_sum, gu_o)
    own_down_sum = wire.copy(down_sum, gd_o)
    scale = float(group * 2 * n) ** (-0.5)

    pl.semaphore_wait(barrier, 3 + (z > 0).astype(jnp.int32) + (z < n - 1).astype(jnp.int32))

    def spread(whole, source, first, parts):
        size = block // parts

        def sub(parity, q, i):
            base = parity * group + q * block + i * size
            return whole.at[pl.ds(pl.multiple_of(base, size), size)]

        made = []
        for i in range(parts):
            there, came = sub(y, tp, i), sub(1 - y, tp, i)
            beside = sub(1 - y, tp + 2 - 4 * x, i)
            src = source.at[pl.ds(pl.multiple_of(first + i * size, size), size)]
            made.append((
                wire.remote(src, there, py), wire.remote(came, came, px),
                wire.remote(came, came, pc), wire.remote(beside, beside, pc),
            ))
        return zip(*made)

    downs = Line(wire, down_full, hb, down, y, z, n, left, right)
    ups = Line(wire, up_full, chunk, None, y, z, n, left, right)
    c_y, c_x, c_c, c_xc = spread(c_all, cot, tp * block, 2)
    e_y, e_x, e_c, e_xc = spread(e_all, earlier_in, tp * block, 2)
    x_y, x_x, x_c, x_xc = spread(x_all, later_in, 0, 2)
    mine_x = x_all.at[rows_of(y, tp)]
    beside_x = x_all.at[rows_of(y, tp + 2 - 4 * x)]
    x_own_x = wire.remote(later_in, mine_x, px)
    x_own_c = wire.remote(later_in, mine_x, pc)
    x_own_xc = wire.remote(beside_x, beside_x, pc)
    up_y = [
        wire.remote(up.at[:, cols(i, 1 - y)], up_full.at[my_rows, strip(i)], py) for i in range(n)
    ]
    far = jnp.where(z < n // 2, n - 1, 0)
    strips = [lax.rem(far + i, n) for i in range(n)]

    def strip_at(i):
        return pl.ds(pl.multiple_of(strips[i] * hb, hb), hb)

    h_y = [
        wire.remote(hidden.at[:, cols(strips[i], 1 - y)], h_all.at[half_of(y), strip_at(i)], py)
        for i in range(n)
    ]

    gds = Sums(wire, gd_part, gd_in, gd_relay, hb, 1 - y, z, n, left, right)
    gus = Sums(wire, gu_part, gu_in, gu_relay, chunk, 1 - y, z, n, left, right)
    at, peers = (x, y, c), (px, py, pc)
    egs = [Plane(wire, eg_bufs, k, at, peers, False) for k in range(n - 1)]
    slots = [wire.slot() for _ in range(6)]
    tails = [
        Plane(wire, tail_bufs, lax.rem(y + p, 2), at, peers, True, slots) for p in (0, 1)
    ]
    outs = [Plane(wire, out_bufs, k, at, peers, True) for k in range(2 * n - 1)]
    outs += [Plane(wire, end_bufs, k, at, peers, True) for k in range(2)]
    tile = min(256, chunk)
    slope_rows = min(256, 2 * group)
    lh_y = [wire.remote(lh.at[:, strip(i)], lh_o.at[:, cols(i, y)], py) for i in range(n)]
    swap = wire.remote(swap_out, swap_in, py)

    def start(*copies):
        for copy in copies:
            wire.start(copy)

    def arrive(*copies):
        for copy in copies:
            copy.wait_recv()

    def activate(parity, i):
        def body(j):
            rows = rows_of(parity, j)
            act_t[strip_at(i), rows] = squared(h_all[rows, strip_at(i)]).T

        loop(group // block, body)

    def column_block(k):
        where = 0
        for i in range(n):
            order = sorted(range(n), key=lambda b: (abs(b - i), b))
            where = where + jnp.where(z == i, order[k], 0)
        return pl.ds(pl.multiple_of(where * chunk, chunk), chunk)

    def store_part(plane, parity, value):
        for q in range(4):
            plane.part[q % 2, q // 2, parity] = value[q * block : (q + 1) * block].astype(BF16)

    def gd_dots(row, size):
        rows = pl.ds(pl.multiple_of(row, hb), size)

        def body(i):
            columns = pl.ds(pl.multiple_of(i * tile, tile), tile)
            gd_part[rows, columns] = dot(act_t[rows, :], c_all[:, columns]).astype(BF16)

        loop(width // tile, body)

    def pg_dots():
        def body(i):
            rows = pl.ds(pl.multiple_of(i * slope_rows, slope_rows), slope_rows)
            lifted = jnp.maximum(h_all[rows, :].astype(F32), 0.0)
            pg[rows, :] = (2.0 * dot(c_all[rows, :], down_full[...], 1, 1) * lifted).astype(BF16)

        loop(2 * group // slope_rows, body)

    def gu_dots():
        def body(i):
            wide = pl.ds(pl.multiple_of(i * tile, tile), tile)
            gu_part[wide, :] = dot(e_all[:, wide], pg[...], 0, 0).astype(BF16)

        loop(width // tile, body)

    def tail_columns(p):
        base = column_block(n - 1).start + lax.rem(y + p, 2) * up_rows
        return pl.ds(pl.multiple_of(base, up_rows), up_rows)

    def tail_chunk(p):
        wide = tail_columns(p)

        def body(parity):
            store_part(tails[p], parity, dot(pg[half_of(parity), :], up_full[wide, :], 1, 1))

        loop(2, body)
        tails[p].begin()

    def eg_chunk(k):
        wide = column_block(k)

        def body(parity):
            store_part(egs[k], parity, dot(pg[half_of(parity), :], up_full[wide, :], 1, 1))

        loop(2, body)
        egs[k].begin()

    def out_columns(k):
        wide, narrow = chunk // 2, chunk // 4
        whole = min(k, 2 * n - 1)
        return pl.ds(whole * wide + (k - whole) * narrow, wide if whole == k < 2 * n - 1 else narrow)

    def out_chunk(k):
        wide = out_columns(k)

        def body(parity):
            store_part(outs[k], parity, dot(act_l[half_of(parity), :], down_full[:, wide]))

        loop(2, body)
        outs[k].begin()

    def lh_early():
        blocks = [column_block(k) for k in range(n - 1)] + [tail_columns(0)]

        def body(i):
            at = pl.ds(pl.multiple_of(i * slope_rows, slope_rows), slope_rows)
            total = dot(x_all[at, blocks[0]], up_full[blocks[0], :])
            for wide in blocks[1:]:
                total = total + dot(x_all[at, wide], up_full[wide, :])
            lh_sum[at, :] = total

        loop(2 * group // slope_rows, body)

    def lh_late(parity):
        wide = tail_columns(1)

        def body(i):
            base = pl.multiple_of(i * slope_rows, slope_rows)
            at = pl.ds(pl.multiple_of(parity * group + base, slope_rows), slope_rows)
            h = (lh_sum[at, :] + dot(x_all[at, wide], up_full[wide, :])).astype(BF16)
            act_l[at, :] = squared(h)
            return base, at, h

        def away(i):
            _, at, h = body(i)
            lh[pl.ds(pl.multiple_of(i * slope_rows, slope_rows), slope_rows), :] = h

        def home(i):
            base, _, h = body(i)
            for j in range(n):
                lh_o[pl.ds(base, slope_rows), cols(j, y)] = h[:, j * hb : (j + 1) * hb]

        return away, home

    def lh_away():
        loop(group // slope_rows, lh_late(1 - y)[0])

    def lh_home():
        loop(group // slope_rows, lh_late(y)[1])

    def first_sends():
        for p in (0, 1):
            downs.begin(p)
        start(*c_y, h_y[0], *up_y, *h_y[1:], *e_y, *x_y, x_own_x, x_own_c)
        for copy in own_up:
            copy.wait()
        ups.begin_at(0, 0)

    def relay(sums, m):
        for p in (0, 1):
            sums.relay(m, p)

    def own_act():
        for copy in own_h:
            copy.wait()
        for i in range(n):
            activate(y, i)

    def all_c():
        arrive(*c_c, *c_xc)
        own_c.wait()

    def all_e():
        arrive(*e_c, *e_xc)
        own_e.wait()

    def all_x():
        arrive(x_own_c, x_own_xc, *x_c, *x_xc)
        own_x.wait()

    def pass_on(came, *onward):
        arrive(came)
        start(*onward)

    def lh_send():
        start(*lh_y)

    def gd_oal():
        own_down_sum.wait()
        for p in (0, 1):
            rows = pl.ds(pl.multiple_of(gds.half(p), hb // 2), hb // 2)
            gd_o[rows, :] = gd_o[rows, :] + scale * gds.total(p)

    def gu_away():
        swap_out[...] = gus.total(0).astype(BF16)
        start(swap)

    def gu_home():
        own_up_sum.wait()
        total = gus.total(1)
        for i in range(n):
            kept = total[:, i * hb : (i + 1) * hb]
            gu_o[:, cols(i, y)] = gu_o[:, cols(i, y)] + scale * kept

    def gu_store():
        arrive(swap)
        for i in range(n):
            came = swap_in[:, strip(i)].astype(F32)
            gu_o[:, cols(i, 1 - y)] = gu_o[:, cols(i, 1 - y)] + scale * came

    def eg_store():
        for k in range(n - 1):
            egs[k].last(eg_o, column_block(k))
        for p in (0, 1):
            tails[p].last(eg_o, tail_columns(p))

    def out_last(k):
        outs[k].last(out_o, out_columns(k))

    def close():
        arrive(*lh_y)
        wire.drain()
        assert wire.n_remote == recv.shape[0] and wire.n_local == local.shape[0]

    def do(name, act, *args):
        with jax.named_scope(name):
            act(*args)

    last = n - 1
    do("first", first_sends)
    do("own_act", own_act)
    do("c_y0", pass_on, c_y[0], c_x[0], c_c[0])
    do("down10", downs.forward, 1, 0)
    do("c_y1", pass_on, c_y[1], c_x[1], c_c[1])
    do("down11", downs.forward, 1, 1)
    ups.begin_at(1, 0)
    do("x_own_x", pass_on, x_own_x, x_own_xc)
    do("up_y", arrive, *up_y)
    for stage in (0, 1):
        ups.begin_at(stage, 1)
    for r in range(2, last):
        do("down20", downs.forward, r, 0)
    for i in (0, 1):
        do("c_x", pass_on, c_x[i], c_xc[i])
    for r in range(2, last):
        do("down21", downs.forward, r, 1)
        for p in (0, 1):
            ups.begin_at(r, p)
    do("h_y0", arrive, h_y[0])
    do("act2", activate, 1 - y, 0)
    do("c_all", all_c)
    do("gd_far", gd_dots, far * hb, hb)
    gds.seeds([n - 2])
    do("h_y", arrive, *h_y[1:])
    for i in range(1, n):
        do("act2", activate, 1 - y, i)
    for p in (0, 1):
        do("ups1e", ups.forward, 1, p, True)
    do("gd_dots", gd_dots, jnp.where(far == 0, hb, 0), half - hb)
    do("gd_seed", gds.seeds, range(n - 3, 0, -1))
    do("e_y0", pass_on, e_y[0], e_x[0], e_c[0])
    for p in (0, 1):
        do("ups1", ups.forward, 1, p, False)
    for r in range(1, n):
        do("down_end", downs.ends, r)
    own_down.wait()
    do("pg", pg_dots)
    wire.settle([*downs.right.values(), *downs.left.values(), *up_y, *h_y, x_own_x, x_own_c, x_own_xc])
    wire.settle([*c_y, *c_x, *c_c, *c_xc])
    do("e_y1", pass_on, e_y[1], e_x[1], e_c[1])
    do("eg0", eg_chunk, 0)
    do("e_x0", pass_on, e_x[0], e_xc[0])
    do("eg0_b", egs[0].second)
    for m in range(n - 3, 0, -1):
        do("gd_relay", relay, gds, m)
    do("x_y0", pass_on, x_y[0], x_x[0], x_c[0])
    do("e_x1", pass_on, e_x[1], e_xc[1])
    do("e_all", all_e)
    do("gu_dots", gu_dots)
    do("gu_seed", gus.seeds, range(n - 2, -1, -1))
    do("x_y1", pass_on, x_y[1], x_x[1], x_c[1])
    do("up1_end", ups.ends, 1)
    do("eg1", eg_chunk, 1)
    for r in range(2, last):
        for p in (0, 1):
            do("ups2", ups.forward, r, p)
    do("eg1_b", egs[1].second)
    do("eg0_c", egs[0].third)
    do("gd_relay0", relay, gds, 0)
    for r in range(2, last):
        do("up2_end", ups.ends, r)
        do("eg2", eg_chunk, r)
    for r in range(2, last):
        do("eg2_b", egs[r].second)
    do("eg1_c", egs[1].third)
    for i in (0, 1):
        do("x_x", pass_on, x_x[i], x_xc[i])
    for m in range(n - 3, 0, -1):
        do("gu_relay_0", gus.relay, m, 0)
    do("up3_0", ups.ends, last, (0,))
    do("eg3_0", tail_chunk, 0)
    do("x_all", all_x)
    do("eg3_0b", tails[0].second)
    do("lh_early", lh_early)
    wire.settle([*e_y, *e_x, *e_c, *e_xc, *x_y, *x_x, *x_c, *x_xc, *gds.seed.values()])
    wire.settle([h for r in range(1, last) for p in (0, 1) for h in (ups.right[r, p], ups.left[r, p])])
    wire.settle([h for plane in egs[:last - 1] for h in (plane.a, plane.b)])
    for m in range(n - 3, 0, -1):
        do("gu_relay_1", gus.relay, m, 1)
    for r in range(2, last):
        do("eg2_c", egs[r].third)
    do("up3_1", ups.ends, last, (1,))
    do("lh_away", lh_away)
    do("lh_send", lh_send)
    do("eg3_1", tail_chunk, 1)
    do("lh_home", lh_home)
    do("eg3_1b", tails[1].second)
    do("out0", out_chunk, 0)
    pieces = len(outs)
    for k in range(1, pieces):
        do("out", out_chunk, k)
        do("out_b", outs[k - 1].second)
    do("out_b", outs[pieces - 1].second)
    gds.seeds([0])
    for p in (0, 1):
        do("eg3_c", tails[p].third)
    do("out_c", outs[0].third)
    do("gu_relay0", relay, gus, 0)
    for k in range(1, n - 1):
        do("out_c", outs[k].third)
    do("gu_away", gu_away)
    do("eg_fin", eg_store)
    for k in range(n - 1, n + 2):
        do("out_c", outs[k].third)
    do("gu_home", gu_home)
    for k in range(n + 2, pieces):
        do("out_c", outs[k].third)
        do("out_last", out_last, k - n - 2)
    for k in range(pieces - n - 2, n):
        do("out_last", out_last, k)
    do("gu_sto", gu_store)
    do("gd_o", gd_oal)
    for k in range(n, pieces):
        do("out_last", out_last, k)
    do("close", close)


def fused(n, later_in, earlier_in, hidden, cot, up, down, up_sum, down_sum):
    group, width = earlier_in.shape
    block, hb, up_rows = later_in.shape[0], down.shape[0], up.shape[0]
    half, tokens, chunk = n * hb, 2 * group, 2 * up_rows
    any_space = pl.BlockSpec(memory_space=pl.ANY)
    vm = pltpu.VMEM
    results = (
        vm(later_in.shape, BF16), vm(hidden.shape, BF16), vm(later_in.shape, BF16),
        vm(up.shape, F32), vm(down.shape, F32),
    )

    def plane(count, columns):
        leading = (2, 2, 2), (2, 2), (2,), (2,), (), ()
        return [vm((count, *lead, block, columns), BF16) for lead in leading]

    scratch = [
        vm((tokens, width), BF16), vm((tokens, width), BF16), vm((tokens, width), BF16),
        vm((tokens, half), BF16), vm((half, tokens), BF16), vm((tokens, half), BF16),
        vm((width, half), BF16), vm((half, width), BF16),
        vm((half, width), BF16), vm((width, half), BF16),
        vm((2, n - 1, hb, width), BF16), vm((2, max(n - 2, 1), hb, width), BF16),
        vm((2, n - 1, chunk, half), BF16), vm((2, max(n - 2, 1), chunk, half), BF16),
        vm((up_rows, half), BF16), vm((up_rows, half), BF16),
        vm((group, half), BF16), vm((tokens, half), BF16), vm((tokens, half), F32),
        *plane(n - 1, chunk), *plane(2, chunk // 2), *plane(2 * n - 1, chunk // 2),
        *plane(2, chunk // 4),
    ]
    remote_copies = 16 * (n - 1) + 3 * (n - 1) + 9 * n + 37
    local_copies = 2 * n + 6
    return pl.pallas_call(
        functools.partial(layer, n),
        out_shape=results,
        in_specs=[any_space] * 8,
        out_specs=(pl.BlockSpec(memory_space=vm),) * 5,
        scratch_shapes=scratch + [
            pltpu.SemaphoreType.DMA((SENDS,)),
            pltpu.SemaphoreType.DMA((remote_copies,)),
            pltpu.SemaphoreType.DMA((local_copies,)),
        ],
        compiler_params=pltpu.CompilerParams(
            collective_id=0, has_side_effects=True, vmem_limit_bytes=VMEM_BYTES
        ),
        name="layer",
    )(later_in, earlier_in, hidden, cot, up, down, up_sum, down_sum)


def hand_on(*refs):
    count = (len(refs) - 1) // 2
    sources, results, gone = refs[:count], refs[count : 2 * count], refs[-1]
    copies = [
        pltpu.make_async_copy(source, result, gone.at[i])
        for i, (source, result) in enumerate(zip(sources, results))
    ]
    for copy in copies:
        copy.start()
    for copy in copies:
        copy.wait()


def handed_on(arrays):
    count = len(arrays)
    held = [pltpu.with_memory_space_constraint(a, pltpu.VMEM) for a in arrays]
    return pl.pallas_call(
        hand_on,
        out_shape=tuple(pltpu.HBM(a.shape, a.dtype) for a in arrays),
        in_specs=[pl.BlockSpec(memory_space=pltpu.VMEM)] * count,
        out_specs=(pl.BlockSpec(memory_space=pltpu.HBM),) * count,
        scratch_shapes=[pltpu.SemaphoreType.DMA((count,))],
        compiler_params=pltpu.CompilerParams(vmem_limit_bytes=1 << 20),
        name="hand_on",
    )(*held)


def portable(n_fs, later_in, earlier_in, hidden, cot, up, down, up_sum, down_sum):
    def split_sum(partial, axis):
        return lax.psum_scatter(partial.astype(F32), axis, scatter_dimension=0, tiled=True)

    up_full = lax.all_gather(up, "fs", axis=0, tiled=True)
    down_full = lax.all_gather(down, "fs", axis=0, tiled=True)
    rows = lax.all_gather(later_in, "tp", axis=0, tiled=True)
    lifted = jnp.maximum(hidden.astype(F32), 0.0)
    gd = split_sum(dot(squared(hidden), cot, 0, 0), "fs")
    pre = (2.0 * dot(cot, down_full, 1, 1) * lifted).astype(BF16)
    gu = split_sum(dot(earlier_in, pre, 0, 0), "fs")
    eg = split_sum(dot(pre, up_full, 1, 1).astype(BF16), "tp").astype(BF16)
    later_hidden = dot(rows, up_full).astype(BF16)
    out = split_sum(dot(squared(later_hidden), down_full).astype(BF16), "tp").astype(BF16)
    scale = float(earlier_in.shape[0] * n_fs) ** (-0.5)
    return out, later_hidden, eg, up_sum + scale * gu, down_sum + scale * gd


def solution(mesh):
    n_fs, n_tp = mesh.shape["fs"], mesh.shape["tp"]

    def shards(*args):
        later_input, up_weight, down_weight = args[0], args[4], args[5]
        planes = n_fs // 2
        fits = (
            n_tp == 4 and n_fs % 2 == 0 and 2 < planes <= 4
            and down_weight.shape[0] % LANES == 0 and up_weight.shape[0] % LANES == 0
            and later_input.shape[0] % LANES == 0
        )
        return handed_on(fused(planes, *args)) if fits else portable(n_fs, *args)

    in_specs = (
        P(("fs", "tp"), None), P("fs", None), P("fs", "tp"), P("fs", None),
        P("fs", "tp"), P(("tp", "fs"), None), P("fs", "tp"), P(("tp", "fs"), None),
    )
    out_specs = (
        P(("fs", "tp"), None), P("fs", "tp"), P(("fs", "tp"), None),
        P("fs", "tp"), P(("tp", "fs"), None),
    )
    return jax.shard_map(shards, mesh=mesh, in_specs=in_specs, out_specs=out_specs, check_vma=False)
```

```python
import functools

import jax
import jax.numpy as jnp
from jax import lax
from jax.experimental import pallas as pl
from jax.experimental.pallas import tpu as pltpu
from jax.sharding import PartitionSpec as P

F32, BF16 = jnp.float32, jnp.bfloat16
MESH = pl.DeviceIdType.MESH
LANES = 128
VMEM_BYTES = 62_000_000
SENDS = 63


def dot(a, b, ca=1, cb=0):
    return lax.dot_general(a, b, (((ca,), (cb,)), ((), ())), preferred_element_type=F32)


def loop(n, body):
    def step(i, carry):
        body(i)
        return carry

    lax.fori_loop(0, n, step, 0)


def squared(h):
    lifted = jnp.maximum(h.astype(F32), 0.0)
    return (lifted * lifted).astype(BF16)


def both(a, b):
    return jnp.logical_and(a, b)


class Hop:
    def __init__(self, wire, src, dst, device, slot):
        self.wire, self.src, self.dst, self.device, self.slot = wire, src, dst, device, slot

    def made(self, place):
        return pltpu.make_async_remote_copy(
            src_ref=self.src, dst_ref=self.dst, send_sem=self.wire.send.at[place],
            recv_sem=self.wire.recv.at[self.slot], device_id=self.device, device_id_type=MESH,
        )

    def wait_recv(self):
        self.made(0).wait_recv()


class Wire:
    def __init__(self, send, recv, local):
        self.send, self.recv, self.local = send, recv, local
        self.n_remote = self.n_local = 0
        self.busy = [None] * send.shape[0]

    def slot(self):
        self.n_remote += 1
        return self.n_remote - 1

    def remote(self, src, dst, device, slot=None):
        return Hop(self, src, dst, device, self.slot() if slot is None else slot)

    def free(self, place):
        copy, when, _ = self.busy[place]
        if when is None:
            copy.wait_send()
        else:
            pl.when(when)(copy.wait_send)
        self.busy[place] = None

    def settle(self, hops):
        for place, held in enumerate(self.busy):
            if held is not None and held[2] in hops:
                self.free(place)

    def start(self, hop, when=None):
        place = self.busy.index(None)
        copy = hop.made(place)
        if when is None:
            copy.start()
        else:
            pl.when(when)(copy.start)
        self.busy[place] = (copy, when, hop)

    def copy(self, src, dst):
        i = self.n_local
        self.n_local += 1
        made = pltpu.make_async_copy(src, dst, self.local.at[i])
        made.start()
        return made

    def drain(self):
        for place, held in enumerate(self.busy):
            if held is not None:
                self.free(place)


class Line:
    def __init__(self, wire, full, rows, own, swap, z, n, left, right):
        self.wire, self.z, self.n = wire, z, n
        self.right, self.left = {}, {}
        size = rows // 2

        def half(i, p):
            base = lax.rem(i + n, n) * rows + lax.rem(swap + p, 2) * size
            return full.at[pl.ds(pl.multiple_of(base, size), size)]

        for p in (0, 1):
            first = half(z, p)
            if own is not None:
                first = own.at[pl.ds(pl.multiple_of(lax.rem(swap + p, 2) * size, size), size)]
            for r in range(1, n):
                src = first if r == 1 else half(z - r + 1, p)
                self.right[r, p] = wire.remote(src, half(z - r + 1, p), right)
                src = first if r == 1 else half(z + r - 1, p)
                self.left[r, p] = wire.remote(src, half(z + r - 1, p), left)

    def begin(self, p, right=True, left=True):
        self.wire.start(self.right[1, p], both(self.z < self.n - 1, right))
        self.wire.start(self.left[1, p], both(self.z > 0, left))

    def begin_at(self, stage, p):
        self.begin(p, self.z == stage, self.z == self.n - 1 - stage)

    def forward(self, r, p, outer=None):
        z, n = self.z, self.n
        rightward, leftward = both(z >= r, z < n - 1), both(z <= n - 1 - r, z > 0)
        if outer is not None:
            rightward = both(rightward, (z == r) == outer)
            leftward = both(leftward, (z == n - 1 - r) == outer)
        pl.when(rightward)(self.right[r, p].wait_recv)
        self.wire.start(self.right[r + 1, p], rightward)
        pl.when(leftward)(self.left[r, p].wait_recv)
        self.wire.start(self.left[r + 1, p], leftward)

    def ends(self, r, halves=(0, 1)):
        z, n = self.z, self.n
        for p in halves:
            pl.when(both(z >= r, z == n - 1))(self.right[r, p].wait_recv)
            pl.when(both(z <= n - 1 - r, z == 0))(self.left[r, p].wait_recv)


class Sums:
    def __init__(self, wire, part, inbox, relayed, rows, swap, z, n, left, right):
        self.wire, self.part, self.inbox, self.relayed = wire, part, inbox, relayed
        self.rows, self.size, self.swap, self.z, self.n = rows, rows // 2, swap, z, n
        self.seed, self.pass_on = {}, {}
        for way, device in ((0, right), (1, left)):
            for m in range(n - 1):
                for p in (0, 1):
                    slot = wire.slot()
                    at = pl.ds(p * self.size, self.size)
                    dst = inbox.at[way, m, at]
                    src = part.at[self.span(way, m, p)]
                    self.seed[way, m, p] = wire.remote(src, dst, device, slot)
                    if m < n - 2:
                        src = relayed.at[way, m, at]
                        self.pass_on[way, m, p] = wire.remote(src, dst, device, slot)

    def half(self, p):
        return lax.rem(self.swap + p, 2) * self.size

    def span(self, way, m, p):
        ahead = self.z + 1 + m if way == 0 else self.z - 1 - m
        base = lax.rem(ahead + 2 * self.n, self.n) * self.rows + self.half(p)
        return pl.ds(pl.multiple_of(base, self.size), self.size)

    def seeds(self, ms):
        for m in ms:
            for p in (0, 1):
                self.wire.start(self.seed[0, m, p], self.z == 0)
                self.wire.start(self.seed[1, m, p], self.z == self.n - 1)

    def relay(self, m, p):
        z, n = self.z, self.n
        at = pl.ds(p * self.size, self.size)
        for way in (0, 1):
            if way == 0:
                when = both(z >= 1, z + 1 + m <= n - 1)
            else:
                when = both(z <= n - 2, z - 1 - m >= 0)

            def add(way=way):
                self.seed[way, m + 1, p].wait_recv()
                mine = self.part[self.span(way, m, p), :].astype(F32)
                came = self.inbox[way, m + 1, at, :].astype(F32)
                self.relayed[way, m, at, :] = (mine + came).astype(BF16)

            pl.when(when)(add)
            self.wire.start(self.pass_on[way, m, p], when)

    def total(self, p):
        z, n = self.z, self.n
        pl.when(z >= 1)(self.seed[0, 0, p].wait_recv)
        pl.when(z <= n - 2)(self.seed[1, 0, p].wait_recv)
        at = pl.ds(p * self.size, self.size)
        base = z * self.rows + self.half(p)
        mine = self.part[pl.ds(pl.multiple_of(base, self.size), self.size), :].astype(F32)
        first = jnp.where(z >= 1, self.inbox[0, 0, at, :].astype(F32), 0.0)
        second = jnp.where(z <= n - 2, self.inbox[1, 0, at, :].astype(F32), 0.0)
        return mine + first + second


class Plane:
    def __init__(self, wire, bufs, k, at, peers, x_first, slots=None):
        self.part, self.in_a, self.to_b, self.in_b, self.to_c, self.in_c = (b.at[k] for b in bufs)
        self.wire, self.x_first = wire, x_first
        x, y, self.core = at
        self.one, self.two = (x, y) if x_first else (y, x)
        if slots is None:
            slot = [None] * 3
        else:
            slot = [slots[0] + 3 * k + i for i in range(3)]
        self.a = wire.remote(self.part.at[1 - self.core], self.in_a, peers[2], slot[0])
        self.b = wire.remote(self.to_b, self.in_b, peers[0 if x_first else 1], slot[1])
        self.c = wire.remote(self.to_c, self.in_c, peers[1 if x_first else 0], slot[2])

    def pair(self, one, two):
        i, j = (one, two) if self.x_first else (two, one)
        return self.part[self.core, i, j].astype(F32) + self.in_a[i, j].astype(F32)

    def mine(self, two):
        return self.pair(self.one, two) + self.in_b[two].astype(F32)

    def begin(self):
        self.wire.start(self.a)

    def second(self):
        self.a.wait_recv()
        for two in (0, 1):
            self.to_b[two] = self.pair(1 - self.one, two).astype(BF16)
        self.wire.start(self.b)

    def third(self):
        self.b.wait_recv()
        self.to_c[...] = self.mine(1 - self.two).astype(BF16)
        self.wire.start(self.c)

    def last(self, out, columns):
        self.c.wait_recv()
        out[:, columns] = (self.mine(self.two) + self.in_c[...].astype(F32)).astype(BF16)


def layer(
    n, later_in, earlier_in, hidden, cot, up, down, up_sum, down_sum,
    out_o, lh_o, eg_o, gu_o, gd_o,
    c_all, e_all, x_all, h_all, act_t, pg, up_full, down_full, gd_part, gu_part,
    gd_in, gd_relay, gu_in, gu_relay, swap_out, swap_in, lh, act_l, lh_sum,
    *rest,
):
    eg_bufs, tail_bufs, out_bufs, end_bufs = (rest[i : i + 6] for i in range(0, 24, 6))
    send, recv, local = rest[24:]
    fs, tp = lax.axis_index("fs"), lax.axis_index("tp")
    z, y = fs // 2, fs % 2
    x, c = tp // 2, tp % 2
    py, px, pc = (fs + 1 - 2 * y, tp), (fs, tp + 2 - 4 * x), (fs, tp + 1 - 2 * c)
    left, right = (lax.rem(fs + 2 * n - 2, 2 * n), tp), (lax.rem(fs + 2, 2 * n), tp)

    group, width = earlier_in.shape
    block = later_in.shape[0]
    hb = down.shape[0]
    half = n * hb
    up_rows = up.shape[0]
    chunk = 2 * up_rows
    wire = Wire(send, recv, local)

    def cols(i, parity):
        return pl.ds(pl.multiple_of((2 * i + parity) * hb, hb), hb)

    def strip(i):
        return pl.ds(i * hb, hb)

    def rows_of(parity, q):
        return pl.ds(pl.multiple_of(parity * group + q * block, block), block)

    def half_of(parity):
        return pl.ds(pl.multiple_of(parity * group, group), group)

    barrier = pltpu.get_barrier_semaphore()

    def greet(device):
        pl.semaphore_signal(barrier, inc=1, device_id=device, device_id_type=MESH)

    for device in (py, px, pc):
        greet(device)
    pl.when(z > 0)(lambda: greet(left))
    pl.when(z < n - 1)(lambda: greet(right))

    own_h = [wire.copy(hidden.at[:, cols(i, y)], h_all.at[half_of(y), strip(i)]) for i in range(n)]
    my_rows = pl.ds(pl.multiple_of(fs * up_rows, up_rows), up_rows)
    own_up = [wire.copy(up.at[:, cols(i, y)], up_full.at[my_rows, strip(i)]) for i in range(n)]
    own_c = wire.copy(cot, c_all.at[half_of(y)])
    own_down = wire.copy(down, down_full.at[pl.ds(pl.multiple_of(z * hb, hb), hb)])
    own_e = wire.copy(earlier_in, e_all.at[half_of(y)])
    own_x = wire.copy(later_in, x_all.at[rows_of(y, tp)])
    own_up_sum = wire.copy(up_sum, gu_o)
    own_down_sum = wire.copy(down_sum, gd_o)
    scale = float(group * 2 * n) ** (-0.5)

    pl.semaphore_wait(barrier, 3 + (z > 0).astype(jnp.int32) + (z < n - 1).astype(jnp.int32))

    def together(ref, slot):
        Hop(wire, ref, ref, pc, slot).wait_recv()

    def spread(whole, source, first, parts, shared):
        size = block // parts

        def sub(parity, q, i):
            base = parity * group + q * block + i * size
            return whole.at[pl.ds(pl.multiple_of(base, size), size)]

        made = []
        for i in range(parts):
            there, came = sub(y, tp, i), sub(1 - y, tp, i)
            beside = sub(1 - y, tp + 2 - 4 * x, i)
            src = source.at[pl.ds(pl.multiple_of(first + i * size, size), size)]
            made.append((
                wire.remote(src, there, py), wire.remote(came, came, px),
                wire.remote(came, came, pc, shared), wire.remote(beside, beside, pc, shared),
            ))
        return zip(*made)

    downs = Line(wire, down_full, hb, down, y, z, n, left, right)
    ups = Line(wire, up_full, chunk, None, y, z, n, left, right)
    c_slot, e_slot, x_slot, up_slot, h_slot, lh_slot = (wire.slot() for _ in range(6))
    c_y, c_x, c_c, c_xc = spread(c_all, cot, tp * block, 2, c_slot)
    e_y, e_x, e_c, e_xc = spread(e_all, earlier_in, tp * block, 2, e_slot)
    x_y, x_x, x_c, x_xc = spread(x_all, later_in, 0, 2, x_slot)
    mine_x = x_all.at[rows_of(y, tp)]
    beside_x = x_all.at[rows_of(y, tp + 2 - 4 * x)]
    x_own_x = wire.remote(later_in, mine_x, px)
    x_own_c = wire.remote(later_in, mine_x, pc, x_slot)
    x_own_xc = wire.remote(beside_x, beside_x, pc, x_slot)
    up_y = [
        wire.remote(up.at[:, cols(i, 1 - y)], up_full.at[my_rows, strip(i)], py, up_slot)
        for i in range(n)
    ]
    far = jnp.where(z < n // 2, n - 1, 0)
    strips = [lax.rem(far + i, n) for i in range(n)]

    def strip_at(i):
        return pl.ds(pl.multiple_of(strips[i] * hb, hb), hb)

    h_y = [
        wire.remote(
            hidden.at[:, cols(strips[i], 1 - y)], h_all.at[half_of(y), strip_at(i)], py,
            h_slot if i else None,
        )
        for i in range(n)
    ]

    gds = Sums(wire, gd_part, gd_in, gd_relay, hb, 1 - y, z, n, left, right)
    gus = Sums(wire, gu_part, gu_in, gu_relay, chunk, 1 - y, z, n, left, right)
    at, peers = (x, y, c), (px, py, pc)
    egs = [Plane(wire, eg_bufs, k, at, peers, False) for k in range(n - 1)]
    slots = [wire.slot() for _ in range(6)]
    tails = [
        Plane(wire, tail_bufs, lax.rem(y + p, 2), at, peers, True, slots) for p in (0, 1)
    ]
    outs = [Plane(wire, out_bufs, k, at, peers, True) for k in range(2 * n - 1)]
    outs += [Plane(wire, end_bufs, k, at, peers, True) for k in range(2)]
    tile = min(256, chunk)
    slope_rows = min(256, 2 * group)
    lh_y = [
        wire.remote(lh.at[:, strip(i)], lh_o.at[:, cols(i, y)], py, lh_slot) for i in range(n)
    ]
    swap = wire.remote(swap_out, swap_in, py)

    def start(*copies):
        for copy in copies:
            wire.start(copy)

    def arrive(*copies):
        for copy in copies:
            copy.wait_recv()

    def activate(parity, i):
        def body(j):
            rows = rows_of(parity, j)
            act_t[strip_at(i), rows] = squared(h_all[rows, strip_at(i)]).T

        loop(group // block, body)

    def column_block(k):
        where = 0
        for i in range(n):
            order = sorted(range(n), key=lambda b: (abs(b - i), b))
            where = where + jnp.where(z == i, order[k], 0)
        return pl.ds(pl.multiple_of(where * chunk, chunk), chunk)

    def store_part(plane, parity, value):
        for q in range(4):
            plane.part[q % 2, q // 2, parity] = value[q * block : (q + 1) * block].astype(BF16)

    def gd_dots(row, size):
        rows = pl.ds(pl.multiple_of(row, hb), size)

        def body(i):
            columns = pl.ds(pl.multiple_of(i * tile, tile), tile)
            gd_part[rows, columns] = dot(act_t[rows, :], c_all[:, columns]).astype(BF16)

        loop(width // tile, body)

    def pg_dots():
        def body(i):
            rows = pl.ds(pl.multiple_of(i * slope_rows, slope_rows), slope_rows)
            lifted = jnp.maximum(h_all[rows, :].astype(F32), 0.0)
            pg[rows, :] = (2.0 * dot(c_all[rows, :], down_full[...], 1, 1) * lifted).astype(BF16)

        loop(2 * group // slope_rows, body)

    def gu_dots():
        def body(i):
            wide = pl.ds(pl.multiple_of(i * tile, tile), tile)
            gu_part[wide, :] = dot(e_all[:, wide], pg[...], 0, 0).astype(BF16)

        loop(width // tile, body)

    def tail_columns(p):
        base = column_block(n - 1).start + lax.rem(y + p, 2) * up_rows
        return pl.ds(pl.multiple_of(base, up_rows), up_rows)

    def tail_chunk(p):
        wide = tail_columns(p)

        def body(parity):
            store_part(tails[p], parity, dot(pg[half_of(parity), :], up_full[wide, :], 1, 1))

        loop(2, body)
        tails[p].begin()

    def eg_chunk(k):
        wide = column_block(k)

        def body(parity):
            store_part(egs[k], parity, dot(pg[half_of(parity), :], up_full[wide, :], 1, 1))

        loop(2, body)
        egs[k].begin()

    def out_columns(k):
        wide, narrow = chunk // 2, chunk // 4
        whole = min(k, 2 * n - 1)
        return pl.ds(whole * wide + (k - whole) * narrow, wide if whole == k < 2 * n - 1 else narrow)

    def out_chunk(k):
        wide = out_columns(k)

        def body(parity):
            store_part(outs[k], parity, dot(act_l[half_of(parity), :], down_full[:, wide]))

        loop(2, body)
        outs[k].begin()

    def lh_early():
        blocks = [column_block(k) for k in range(n - 1)] + [tail_columns(0)]

        def body(i):
            at = pl.ds(pl.multiple_of(i * slope_rows, slope_rows), slope_rows)
            total = dot(x_all[at, blocks[0]], up_full[blocks[0], :])
            for wide in blocks[1:]:
                total = total + dot(x_all[at, wide], up_full[wide, :])
            lh_sum[at, :] = total

        loop(2 * group // slope_rows, body)

    def lh_late(parity):
        wide = tail_columns(1)

        def body(i):
            base = pl.multiple_of(i * slope_rows, slope_rows)
            at = pl.ds(pl.multiple_of(parity * group + base, slope_rows), slope_rows)
            h = (lh_sum[at, :] + dot(x_all[at, wide], up_full[wide, :])).astype(BF16)
            act_l[at, :] = squared(h)
            return base, at, h

        def away(i):
            _, at, h = body(i)
            lh[pl.ds(pl.multiple_of(i * slope_rows, slope_rows), slope_rows), :] = h

        def home(i):
            base, _, h = body(i)
            for j in range(n):
                lh_o[pl.ds(base, slope_rows), cols(j, y)] = h[:, j * hb : (j + 1) * hb]

        return away, home

    def lh_away():
        loop(group // slope_rows, lh_late(1 - y)[0])

    def lh_home():
        loop(group // slope_rows, lh_late(y)[1])

    def first_sends():
        for p in (0, 1):
            downs.begin(p)
        start(*c_y, h_y[0], *up_y, *h_y[1:], *e_y, *x_y, x_own_x, x_own_c)
        for copy in own_up:
            copy.wait()
        ups.begin_at(0, 0)

    def relay(sums, m):
        for p in (0, 1):
            sums.relay(m, p)

    def own_act():
        for copy in own_h:
            copy.wait()
        for i in range(n):
            activate(y, i)

    def all_c():
        together(c_all.at[pl.ds(0, 2 * block)], c_slot)
        own_c.wait()

    def all_e():
        together(e_all.at[pl.ds(0, 2 * block)], e_slot)
        own_e.wait()

    def all_x():
        together(x_all.at[pl.ds(0, 4 * block)], x_slot)
        own_x.wait()

    def pass_on(came, *onward):
        arrive(came)
        start(*onward)

    def lh_send():
        start(*lh_y)

    def gd_oal():
        own_down_sum.wait()
        for p in (0, 1):
            rows = pl.ds(pl.multiple_of(gds.half(p), hb // 2), hb // 2)
            gd_o[rows, :] = gd_o[rows, :] + scale * gds.total(p)

    def gu_away():
        swap_out[...] = gus.total(0).astype(BF16)
        start(swap)

    def gu_home():
        own_up_sum.wait()
        total = gus.total(1)
        for i in range(n):
            kept = total[:, i * hb : (i + 1) * hb]
            gu_o[:, cols(i, y)] = gu_o[:, cols(i, y)] + scale * kept

    def gu_store():
        arrive(swap)
        for i in range(n):
            came = swap_in[:, strip(i)].astype(F32)
            gu_o[:, cols(i, 1 - y)] = gu_o[:, cols(i, 1 - y)] + scale * came

    def eg_store():
        for k in range(n - 1):
            egs[k].last(eg_o, column_block(k))
        for p in (0, 1):
            tails[p].last(eg_o, tail_columns(p))

    def out_last(k):
        outs[k].last(out_o, out_columns(k))

    def close():
        together(lh_o.at[:, pl.ds(0, half)], lh_slot)
        wire.drain()
        assert wire.n_remote == recv.shape[0] and wire.n_local == local.shape[0]

    def do(name, act, *args):
        with jax.named_scope(name):
            act(*args)

    last = n - 1
    do("first", first_sends)
    do("own_act", own_act)
    do("c_y0", pass_on, c_y[0], c_x[0], c_c[0])
    do("down10", downs.forward, 1, 0)
    do("c_y1", pass_on, c_y[1], c_x[1], c_c[1])
    do("down11", downs.forward, 1, 1)
    ups.begin_at(1, 0)
    do("x_own_x", pass_on, x_own_x, x_own_xc)
    do("up_y", together, up_full.at[pl.ds(0, up_rows)], up_slot)
    for stage in (0, 1):
        ups.begin_at(stage, 1)
    for r in range(2, last):
        do("down20", downs.forward, r, 0)
    for i in (0, 1):
        do("c_x", pass_on, c_x[i], c_xc[i])
    for r in range(2, last):
        do("down21", downs.forward, r, 1)
        for p in (0, 1):
            ups.begin_at(r, p)
    do("h_y0", arrive, h_y[0])
    do("act2", activate, 1 - y, 0)
    do("c_all", all_c)
    do("gd_far", gd_dots, far * hb, hb)
    wire.settle([*c_y, *c_x, *c_c, *c_xc, *up_y, h_y[0], x_own_x, x_own_c, x_own_xc])
    wire.settle([hop for p in (0, 1) for hop in (downs.right[1, p], downs.left[1, p])])
    gds.seeds([n - 2])
    do("h_y", together, h_all.at[pl.ds(0, group), pl.ds(0, half - hb)], h_slot)
    for i in range(1, n):
        do("act2", activate, 1 - y, i)
    for p in (0, 1):
        do("ups1e", ups.forward, 1, p, True)
    do("gd_dots", gd_dots, jnp.where(far == 0, hb, 0), half - hb)
    do("gd_seed", gds.seeds, range(n - 3, 0, -1))
    do("e_y0", pass_on, e_y[0], e_x[0], e_c[0])
    for p in (0, 1):
        do("ups1", ups.forward, 1, p, False)
    for r in range(1, n):
        do("down_end", downs.ends, r)
    own_down.wait()
    do("pg", pg_dots)
    wire.settle([*downs.right.values(), *downs.left.values(), *h_y])
    do("e_y1", pass_on, e_y[1], e_x[1], e_c[1])
    do("eg0", eg_chunk, 0)
    do("e_x0", pass_on, e_x[0], e_xc[0])
    do("eg0_b", egs[0].second)
    for m in range(n - 3, 0, -1):
        do("gd_relay", relay, gds, m)
    do("x_y0", pass_on, x_y[0], x_x[0], x_c[0])
    do("e_x1", pass_on, e_x[1], e_xc[1])
    do("e_all", all_e)
    do("gu_dots", gu_dots)
    wire.settle([*e_y, *e_x, *e_c, *e_xc, egs[0].a])
    wire.settle([hop for p in (0, 1) for hop in (ups.right[1, p], ups.left[1, p])])
    do("gu_seed", gus.seeds, range(n - 2, -1, -1))
    do("x_y1", pass_on, x_y[1], x_x[1], x_c[1])
    do("up1_end", ups.ends, 1)
    do("eg1", eg_chunk, 1)
    for r in range(2, last):
        for p in (0, 1):
            do("ups2", ups.forward, r, p)
    do("eg1_b", egs[1].second)
    do("eg0_c", egs[0].third)
    do("gd_relay0", relay, gds, 0)
    for r in range(2, last):
        do("up2_end", ups.ends, r)
        do("eg2", eg_chunk, r)
    for r in range(2, last):
        do("eg2_b", egs[r].second)
    do("eg1_c", egs[1].third)
    for i in (0, 1):
        do("x_x", pass_on, x_x[i], x_xc[i])
    for m in range(n - 3, 0, -1):
        do("gu_relay_0", gus.relay, m, 0)
    do("up3_0", ups.ends, last, (0,))
    do("eg3_0", tail_chunk, 0)
    do("x_all", all_x)
    do("eg3_0b", tails[0].second)
    do("lh_early", lh_early)
    wire.settle([*e_y, *e_x, *e_c, *e_xc, *x_y, *x_x, *x_c, *x_xc, *gds.seed.values()])
    wire.settle([h for r in range(1, last) for p in (0, 1) for h in (ups.right[r, p], ups.left[r, p])])
    wire.settle([h for plane in egs[:last - 1] for h in (plane.a, plane.b)])
    for m in range(n - 3, 0, -1):
        do("gu_relay_1", gus.relay, m, 1)
    for r in range(2, last):
        do("eg2_c", egs[r].third)
    do("up3_1", ups.ends, last, (1,))
    do("lh_away", lh_away)
    do("lh_send", lh_send)
    do("eg3_1", tail_chunk, 1)
    do("lh_home", lh_home)
    do("eg3_1b", tails[1].second)
    do("out0", out_chunk, 0)
    pieces = len(outs)
    for k in range(1, pieces):
        do("out", out_chunk, k)
        do("out_b", outs[k - 1].second)
        wire.settle([tails[0].a, tails[1].a, *(plane.a for plane in outs[: k - 1])])
    do("out_b", outs[pieces - 1].second)
    gds.seeds([0])
    for p in (0, 1):
        do("eg3_c", tails[p].third)
    do("out_c", outs[0].third)
    do("gu_relay0", relay, gus, 0)
    for k in range(1, n - 1):
        do("out_c", outs[k].third)
    wire.settle([*ups.right.values(), *ups.left.values(), *(h for e in egs for h in (e.a, e.b, e.c))])
    wire.settle([gus.seed[w, m, p] for w in (0, 1) for m in range(1, n - 1) for p in (0, 1)])
    wire.settle([tails[0].b, tails[1].b, outs[0].b, outs[1].b, *gds.pass_on.values()])
    do("gu_away", gu_away)
    do("eg_fin", eg_store)
    for k in range(n - 1, n + 2):
        do("out_c", outs[k].third)
    do("gu_home", gu_home)
    for k in range(n + 2, pieces):
        do("out_c", outs[k].third)
        do("out_last", out_last, k - n - 2)
    for k in range(pieces - n - 2, n):
        do("out_last", out_last, k)
    do("gu_sto", gu_store)
    do("gd_o", gd_oal)
    for k in range(n, pieces):
        do("out_last", out_last, k)
    do("close", close)


def fused(n, later_in, earlier_in, hidden, cot, up, down, up_sum, down_sum):
    group, width = earlier_in.shape
    block, hb, up_rows = later_in.shape[0], down.shape[0], up.shape[0]
    half, tokens, chunk = n * hb, 2 * group, 2 * up_rows
    any_space = pl.BlockSpec(memory_space=pl.ANY)
    vm = pltpu.VMEM
    results = (
        vm(later_in.shape, BF16), vm(hidden.shape, BF16), vm(later_in.shape, BF16),
        vm(up.shape, F32), vm(down.shape, F32),
    )

    def plane(count, columns):
        leading = (2, 2, 2), (2, 2), (2,), (2,), (), ()
        return [vm((count, *lead, block, columns), BF16) for lead in leading]

    scratch = [
        vm((tokens, width), BF16), vm((tokens, width), BF16), vm((tokens, width), BF16),
        vm((tokens, half), BF16), vm((half, tokens), BF16), vm((tokens, half), BF16),
        vm((width, half), BF16), vm((half, width), BF16),
        vm((half, width), BF16), vm((width, half), BF16),
        vm((2, n - 1, hb, width), BF16), vm((2, max(n - 2, 1), hb, width), BF16),
        vm((2, n - 1, chunk, half), BF16), vm((2, max(n - 2, 1), chunk, half), BF16),
        vm((up_rows, half), BF16), vm((up_rows, half), BF16),
        vm((group, half), BF16), vm((tokens, half), BF16), vm((tokens, half), F32),
        *plane(n - 1, chunk), *plane(2, chunk // 2), *plane(2 * n - 1, chunk // 2),
        *plane(2, chunk // 4),
    ]
    remote_copies = 19 * (n - 1) + 6 * n + 30
    local_copies = 2 * n + 6
    return pl.pallas_call(
        functools.partial(layer, n),
        out_shape=results,
        in_specs=[any_space] * 8,
        out_specs=(pl.BlockSpec(memory_space=vm),) * 5,
        scratch_shapes=scratch + [
            pltpu.SemaphoreType.DMA((SENDS,)),
            pltpu.SemaphoreType.DMA((remote_copies,)),
            pltpu.SemaphoreType.DMA((local_copies,)),
        ],
        compiler_params=pltpu.CompilerParams(
            collective_id=0, has_side_effects=True, vmem_limit_bytes=VMEM_BYTES
        ),
        name="layer",
    )(later_in, earlier_in, hidden, cot, up, down, up_sum, down_sum)


def hand_on(*refs):
    count = (len(refs) - 1) // 2
    sources, results, gone = refs[:count], refs[count : 2 * count], refs[-1]
    copies = [
        pltpu.make_async_copy(source, result, gone.at[i])
        for i, (source, result) in enumerate(zip(sources, results))
    ]
    for copy in copies:
        copy.start()
    for copy in copies:
        copy.wait()


def handed_on(arrays):
    count = len(arrays)
    held = [pltpu.with_memory_space_constraint(a, pltpu.VMEM) for a in arrays]
    return pl.pallas_call(
        hand_on,
        out_shape=tuple(pltpu.HBM(a.shape, a.dtype) for a in arrays),
        in_specs=[pl.BlockSpec(memory_space=pltpu.VMEM)] * count,
        out_specs=(pl.BlockSpec(memory_space=pltpu.HBM),) * count,
        scratch_shapes=[pltpu.SemaphoreType.DMA((count,))],
        compiler_params=pltpu.CompilerParams(vmem_limit_bytes=1 << 20),
        name="hand_on",
    )(*held)


def portable(n_fs, later_in, earlier_in, hidden, cot, up, down, up_sum, down_sum):
    def split_sum(partial, axis):
        return lax.psum_scatter(partial.astype(F32), axis, scatter_dimension=0, tiled=True)

    up_full = lax.all_gather(up, "fs", axis=0, tiled=True)
    down_full = lax.all_gather(down, "fs", axis=0, tiled=True)
    rows = lax.all_gather(later_in, "tp", axis=0, tiled=True)
    lifted = jnp.maximum(hidden.astype(F32), 0.0)
    gd = split_sum(dot(squared(hidden), cot, 0, 0), "fs")
    pre = (2.0 * dot(cot, down_full, 1, 1) * lifted).astype(BF16)
    gu = split_sum(dot(earlier_in, pre, 0, 0), "fs")
    eg = split_sum(dot(pre, up_full, 1, 1).astype(BF16), "tp").astype(BF16)
    later_hidden = dot(rows, up_full).astype(BF16)
    out = split_sum(dot(squared(later_hidden), down_full).astype(BF16), "tp").astype(BF16)
    scale = float(earlier_in.shape[0] * n_fs) ** (-0.5)
    return out, later_hidden, eg, up_sum + scale * gu, down_sum + scale * gd


def solution(mesh):
    n_fs, n_tp = mesh.shape["fs"], mesh.shape["tp"]

    def shards(*args):
        later_input, up_weight, down_weight = args[0], args[4], args[5]
        planes = n_fs // 2
        fits = (
            n_tp == 4 and n_fs % 2 == 0 and 2 < planes <= 4
            and down_weight.shape[0] % LANES == 0 and up_weight.shape[0] % LANES == 0
            and later_input.shape[0] % LANES == 0
        )
        return handed_on(fused(planes, *args)) if fits else portable(n_fs, *args)

    in_specs = (
        P(("fs", "tp"), None), P("fs", None), P("fs", "tp"), P("fs", None),
        P("fs", "tp"), P(("tp", "fs"), None), P("fs", "tp"), P(("tp", "fs"), None),
    )
    out_specs = (
        P(("fs", "tp"), None), P("fs", "tp"), P(("fs", "tp"), None),
        P("fs", "tp"), P(("tp", "fs"), None),
    )
    return jax.shard_map(shards, mesh=mesh, in_specs=in_specs, out_specs=out_specs, check_vma=False)
```

```python
import functools

import jax
import jax.numpy as jnp
from jax import lax
from jax.experimental import pallas as pl
from jax.experimental.pallas import tpu as pltpu
from jax.sharding import PartitionSpec as P

F32, BF16 = jnp.float32, jnp.bfloat16
MESH = pl.DeviceIdType.MESH
LANES = 128
VMEM_BYTES = 62_000_000
SENDS = 63


def dot(a, b, ca=1, cb=0):
    return lax.dot_general(a, b, (((ca,), (cb,)), ((), ())), preferred_element_type=F32)


def loop(n, body):
    def step(i, carry):
        body(i)
        return carry

    lax.fori_loop(0, n, step, 0)


def squared(h):
    lifted = jnp.maximum(h.astype(F32), 0.0)
    return (lifted * lifted).astype(BF16)


def both(a, b):
    return jnp.logical_and(a, b)


class Hop:
    def __init__(self, wire, src, dst, device, slot):
        self.wire, self.src, self.dst, self.device, self.slot = wire, src, dst, device, slot

    def made(self, place):
        return pltpu.make_async_remote_copy(
            src_ref=self.src, dst_ref=self.dst, send_sem=self.wire.send.at[place],
            recv_sem=self.wire.recv.at[self.slot], device_id=self.device, device_id_type=MESH,
        )

    def wait_recv(self):
        self.made(0).wait_recv()


class Wire:
    def __init__(self, send, recv, local):
        self.send, self.recv, self.local = send, recv, local
        self.n_remote = self.n_local = 0
        self.busy = [None] * send.shape[0]

    def slot(self):
        self.n_remote += 1
        return self.n_remote - 1

    def remote(self, src, dst, device, slot=None):
        return Hop(self, src, dst, device, self.slot() if slot is None else slot)

    def free(self, place):
        copy, when, _ = self.busy[place]
        if when is None:
            copy.wait_send()
        else:
            pl.when(when)(copy.wait_send)
        self.busy[place] = None

    def settle(self, hops):
        for place, held in enumerate(self.busy):
            if held is not None and held[2] in hops:
                self.free(place)

    def start(self, hop, when=None):
        place = self.busy.index(None)
        copy = hop.made(place)
        if when is None:
            copy.start()
        else:
            pl.when(when)(copy.start)
        self.busy[place] = (copy, when, hop)

    def copy(self, src, dst):
        i = self.n_local
        self.n_local += 1
        made = pltpu.make_async_copy(src, dst, self.local.at[i])
        made.start()
        return made

    def drain(self):
        for place, held in enumerate(self.busy):
            if held is not None:
                self.free(place)


class Line:
    def __init__(self, wire, full, rows, own, swap, z, n, left, right):
        self.wire, self.z, self.n = wire, z, n
        self.right, self.left = {}, {}
        size = rows // 2

        def half(i, p):
            base = lax.rem(i + n, n) * rows + lax.rem(swap + p, 2) * size
            return full.at[pl.ds(pl.multiple_of(base, size), size)]

        for p in (0, 1):
            first = half(z, p)
            if own is not None:
                first = own.at[pl.ds(pl.multiple_of(lax.rem(swap + p, 2) * size, size), size)]
            for r in range(1, n):
                src = first if r == 1 else half(z - r + 1, p)
                self.right[r, p] = wire.remote(src, half(z - r + 1, p), right)
                src = first if r == 1 else half(z + r - 1, p)
                self.left[r, p] = wire.remote(src, half(z + r - 1, p), left)

    def begin(self, p, right=True, left=True):
        self.wire.start(self.right[1, p], both(self.z < self.n - 1, right))
        self.wire.start(self.left[1, p], both(self.z > 0, left))

    def begin_at(self, stage, p):
        self.begin(p, self.z == stage, self.z == self.n - 1 - stage)

    def forward(self, r, p, outer=None):
        z, n = self.z, self.n
        rightward, leftward = both(z >= r, z < n - 1), both(z <= n - 1 - r, z > 0)
        if outer is not None:
            rightward = both(rightward, (z == r) == outer)
            leftward = both(leftward, (z == n - 1 - r) == outer)
        pl.when(rightward)(self.right[r, p].wait_recv)
        self.wire.start(self.right[r + 1, p], rightward)
        pl.when(leftward)(self.left[r, p].wait_recv)
        self.wire.start(self.left[r + 1, p], leftward)

    def ends(self, r, halves=(0, 1)):
        z, n = self.z, self.n
        for p in halves:
            pl.when(both(z >= r, z == n - 1))(self.right[r, p].wait_recv)
            pl.when(both(z <= n - 1 - r, z == 0))(self.left[r, p].wait_recv)


class Sums:
    def __init__(self, wire, part, inbox, relayed, rows, swap, z, n, left, right):
        self.wire, self.part, self.inbox, self.relayed = wire, part, inbox, relayed
        self.rows, self.size, self.swap, self.z, self.n = rows, rows // 2, swap, z, n
        self.seed, self.pass_on = {}, {}
        for way, device in ((0, right), (1, left)):
            for m in range(n - 1):
                for p in (0, 1):
                    slot = wire.slot()
                    at = pl.ds(p * self.size, self.size)
                    dst = inbox.at[way, m, at]
                    src = part.at[self.span(way, m, p)]
                    self.seed[way, m, p] = wire.remote(src, dst, device, slot)
                    if m < n - 2:
                        src = relayed.at[way, m, at]
                        self.pass_on[way, m, p] = wire.remote(src, dst, device, slot)

    def half(self, p):
        return lax.rem(self.swap + p, 2) * self.size

    def span(self, way, m, p):
        ahead = self.z + 1 + m if way == 0 else self.z - 1 - m
        base = lax.rem(ahead + 2 * self.n, self.n) * self.rows + self.half(p)
        return pl.ds(pl.multiple_of(base, self.size), self.size)

    def seeds(self, ms):
        for m in ms:
            for p in (0, 1):
                self.wire.start(self.seed[0, m, p], self.z == 0)
                self.wire.start(self.seed[1, m, p], self.z == self.n - 1)

    def relay(self, m, p):
        z, n = self.z, self.n
        at = pl.ds(p * self.size, self.size)
        for way in (0, 1):
            if way == 0:
                when = both(z >= 1, z + 1 + m <= n - 1)
            else:
                when = both(z <= n - 2, z - 1 - m >= 0)

            def add(way=way):
                self.seed[way, m + 1, p].wait_recv()
                mine = self.part[self.span(way, m, p), :].astype(F32)
                came = self.inbox[way, m + 1, at, :].astype(F32)
                self.relayed[way, m, at, :] = (mine + came).astype(BF16)

            pl.when(when)(add)
            self.wire.start(self.pass_on[way, m, p], when)

    def total(self, p):
        z, n = self.z, self.n
        pl.when(z >= 1)(self.seed[0, 0, p].wait_recv)
        pl.when(z <= n - 2)(self.seed[1, 0, p].wait_recv)
        at = pl.ds(p * self.size, self.size)
        base = z * self.rows + self.half(p)
        mine = self.part[pl.ds(pl.multiple_of(base, self.size), self.size), :].astype(F32)
        first = jnp.where(z >= 1, self.inbox[0, 0, at, :].astype(F32), 0.0)
        second = jnp.where(z <= n - 2, self.inbox[1, 0, at, :].astype(F32), 0.0)
        return mine + first + second


class Plane:
    def __init__(self, wire, bufs, k, at, peers, x_first, slots=None):
        self.part, self.in_a, self.to_b, self.in_b, self.to_c, self.in_c = (b.at[k] for b in bufs)
        self.wire, self.x_first = wire, x_first
        x, y, self.core = at
        self.one, self.two = (x, y) if x_first else (y, x)
        if slots is None:
            slot = [None] * 3
        else:
            slot = [slots[0] + 3 * k + i for i in range(3)]
        self.a = wire.remote(self.part.at[1 - self.core], self.in_a, peers[2], slot[0])
        self.b = wire.remote(self.to_b, self.in_b, peers[0 if x_first else 1], slot[1])
        self.c = wire.remote(self.to_c, self.in_c, peers[1 if x_first else 0], slot[2])

    def pair(self, one, two):
        i, j = (one, two) if self.x_first else (two, one)
        return self.part[self.core, i, j].astype(F32) + self.in_a[i, j].astype(F32)

    def mine(self, two):
        return self.pair(self.one, two) + self.in_b[two].astype(F32)

    def begin(self):
        self.wire.start(self.a)

    def second(self):
        self.a.wait_recv()
        for two in (0, 1):
            self.to_b[two] = self.pair(1 - self.one, two).astype(BF16)
        self.wire.start(self.b)

    def third(self):
        self.b.wait_recv()
        self.to_c[...] = self.mine(1 - self.two).astype(BF16)
        self.wire.start(self.c)

    def last(self, out, columns):
        self.c.wait_recv()
        out[:, columns] = (self.mine(self.two) + self.in_c[...].astype(F32)).astype(BF16)


def layer(
    n, later_in, earlier_in, hidden, cot, up, down, up_sum, down_sum,
    out_o, lh_o, eg_o, gu_o, gd_o,
    c_all, e_all, x_all, h_all, act_t, pg, up_full, down_full, gd_part, gu_part,
    gd_in, gd_relay, gu_in, gu_relay, swap_out, swap_in, lh, act_l, lh_sum,
    *rest,
):
    eg_bufs, tail_bufs, out_bufs, end_bufs = (rest[i : i + 6] for i in range(0, 24, 6))
    send, recv, local = rest[24:]
    fs, tp = lax.axis_index("fs"), lax.axis_index("tp")
    z, y = fs // 2, fs % 2
    x, c = tp // 2, tp % 2
    py, px, pc = (fs + 1 - 2 * y, tp), (fs, tp + 2 - 4 * x), (fs, tp + 1 - 2 * c)
    left, right = (lax.rem(fs + 2 * n - 2, 2 * n), tp), (lax.rem(fs + 2, 2 * n), tp)

    group, width = earlier_in.shape
    block = later_in.shape[0]
    hb = down.shape[0]
    half = n * hb
    up_rows = up.shape[0]
    chunk = 2 * up_rows
    wire = Wire(send, recv, local)

    def cols(i, parity):
        return pl.ds(pl.multiple_of((2 * i + parity) * hb, hb), hb)

    def strip(i):
        return pl.ds(i * hb, hb)

    def rows_of(parity, q):
        return pl.ds(pl.multiple_of(parity * group + q * block, block), block)

    def half_of(parity):
        return pl.ds(pl.multiple_of(parity * group, group), group)

    barrier = pltpu.get_barrier_semaphore()

    def greet(device):
        pl.semaphore_signal(barrier, inc=1, device_id=device, device_id_type=MESH)

    for device in (py, px, pc):
        greet(device)
    pl.when(z > 0)(lambda: greet(left))
    pl.when(z < n - 1)(lambda: greet(right))

    def own_quarter(i):
        q = lax.rem(tp + i, 4)
        src = cot.at[pl.ds(pl.multiple_of(q * block, block), block)]
        return wire.copy(src, c_all.at[rows_of(y, q)])

    own_c = [own_quarter(0)]
    own_down = wire.copy(down, down_full.at[pl.ds(pl.multiple_of(z * hb, hb), hb)])
    own_c += [own_quarter(i) for i in range(1, 4)]
    own_h = [wire.copy(hidden.at[:, cols(i, y)], h_all.at[half_of(y), strip(i)]) for i in range(n)]
    my_rows = pl.ds(pl.multiple_of(fs * up_rows, up_rows), up_rows)
    own_up = [wire.copy(up.at[:, cols(i, y)], up_full.at[my_rows, strip(i)]) for i in range(n)]
    own_e = wire.copy(earlier_in, e_all.at[half_of(y)])
    own_x = wire.copy(later_in, x_all.at[rows_of(y, tp)])
    own_up_sum = wire.copy(up_sum, gu_o)
    own_down_sum = wire.copy(down_sum, gd_o)
    scale = float(group * 2 * n) ** (-0.5)

    pl.semaphore_wait(barrier, 3 + (z > 0).astype(jnp.int32) + (z < n - 1).astype(jnp.int32))

    def together(ref, slot):
        Hop(wire, ref, ref, pc, slot).wait_recv()

    def spread(whole, source, first, parts, shared):
        size = block // parts

        def sub(parity, q, i):
            base = parity * group + q * block + i * size
            return whole.at[pl.ds(pl.multiple_of(base, size), size)]

        made = []
        for i in range(parts):
            there, came = sub(y, tp, i), sub(1 - y, tp, i)
            beside = sub(1 - y, tp + 2 - 4 * x, i)
            src = source.at[pl.ds(pl.multiple_of(first + i * size, size), size)]
            made.append((
                wire.remote(src, there, py), wire.remote(came, came, px),
                wire.remote(came, came, pc, shared), wire.remote(beside, beside, pc, shared),
            ))
        return zip(*made)

    downs = Line(wire, down_full, hb, None, y, z, n, left, right)
    ups = Line(wire, up_full, chunk, None, y, z, n, left, right)
    c_slot, e_slot, x_slot, up_slot, h_slot, lh_slot = (wire.slot() for _ in range(6))
    c_y, c_x, c_c, c_xc = spread(c_all, c_all, y * group + tp * block, 2, c_slot)
    e_y, e_x, e_c, e_xc = spread(e_all, earlier_in, tp * block, 2, e_slot)
    x_y, x_x, x_c, x_xc = spread(x_all, later_in, 0, 2, x_slot)
    mine_x = x_all.at[rows_of(y, tp)]
    beside_x = x_all.at[rows_of(y, tp + 2 - 4 * x)]
    x_own_x = wire.remote(later_in, mine_x, px)
    x_own_c = wire.remote(later_in, mine_x, pc, x_slot)
    x_own_xc = wire.remote(beside_x, beside_x, pc, x_slot)
    up_y = [
        wire.remote(up.at[:, cols(i, 1 - y)], up_full.at[my_rows, strip(i)], py, up_slot)
        for i in range(n)
    ]
    far = jnp.where(z < n // 2, n - 1, 0)
    strips = [lax.rem(far + i, n) for i in range(n)]

    def strip_at(i):
        return pl.ds(pl.multiple_of(strips[i] * hb, hb), hb)

    h_y = [
        wire.remote(
            hidden.at[:, cols(strips[i], 1 - y)], h_all.at[half_of(y), strip_at(i)], py,
            h_slot if i else None,
        )
        for i in range(n)
    ]

    gds = Sums(wire, gd_part, gd_in, gd_relay, hb, 1 - y, z, n, left, right)
    gus = Sums(wire, gu_part, gu_in, gu_relay, chunk, 1 - y, z, n, left, right)
    at, peers = (x, y, c), (px, py, pc)
    egs = [Plane(wire, eg_bufs, k, at, peers, False) for k in range(n - 1)]
    slots = [wire.slot() for _ in range(6)]
    tails = [
        Plane(wire, tail_bufs, lax.rem(y + p, 2), at, peers, True, slots) for p in (0, 1)
    ]
    outs = [Plane(wire, out_bufs, k, at, peers, True) for k in range(2 * n - 1)]
    outs += [Plane(wire, end_bufs, k, at, peers, True) for k in range(2)]
    tile = min(256, chunk)
    slope_rows = min(256, 2 * group)
    lh_y = [
        wire.remote(lh.at[:, strip(i)], lh_o.at[:, cols(i, y)], py, lh_slot) for i in range(n)
    ]
    swap = wire.remote(swap_out, swap_in, py)

    def start(*copies):
        for copy in copies:
            wire.start(copy)

    def arrive(*copies):
        for copy in copies:
            copy.wait_recv()

    def activate(parity, i):
        def body(j):
            rows = rows_of(parity, j)
            act_t[strip_at(i), rows] = squared(h_all[rows, strip_at(i)]).T

        loop(group // block, body)

    def column_block(k):
        where = 0
        for i in range(n):
            order = sorted(range(n), key=lambda b: (abs(b - i), b))
            where = where + jnp.where(z == i, order[k], 0)
        return pl.ds(pl.multiple_of(where * chunk, chunk), chunk)

    def store_part(plane, parity, value):
        for q in range(4):
            plane.part[q % 2, q // 2, parity] = value[q * block : (q + 1) * block].astype(BF16)

    def gd_dots(row, size):
        rows = pl.ds(pl.multiple_of(row, hb), size)

        def body(i):
            columns = pl.ds(pl.multiple_of(i * tile, tile), tile)
            gd_part[rows, columns] = dot(act_t[rows, :], c_all[:, columns]).astype(BF16)

        loop(width // tile, body)

    def pg_dots():
        def body(i):
            rows = pl.ds(pl.multiple_of(i * slope_rows, slope_rows), slope_rows)
            lifted = jnp.maximum(h_all[rows, :].astype(F32), 0.0)
            pg[rows, :] = (2.0 * dot(c_all[rows, :], down_full[...], 1, 1) * lifted).astype(BF16)

        loop(2 * group // slope_rows, body)

    def gu_dots():
        def body(i):
            wide = pl.ds(pl.multiple_of(i * tile, tile), tile)
            gu_part[wide, :] = dot(e_all[:, wide], pg[...], 0, 0).astype(BF16)

        loop(width // tile, body)

    def tail_columns(p):
        base = column_block(n - 1).start + lax.rem(y + p, 2) * up_rows
        return pl.ds(pl.multiple_of(base, up_rows), up_rows)

    def tail_chunk(p):
        wide = tail_columns(p)

        def body(parity):
            store_part(tails[p], parity, dot(pg[half_of(parity), :], up_full[wide, :], 1, 1))

        loop(2, body)
        tails[p].begin()

    def eg_chunk(k):
        wide = column_block(k)

        def body(parity):
            store_part(egs[k], parity, dot(pg[half_of(parity), :], up_full[wide, :], 1, 1))

        loop(2, body)
        egs[k].begin()

    def out_columns(k):
        wide, narrow = chunk // 2, chunk // 4
        whole = min(k, 2 * n - 1)
        return pl.ds(whole * wide + (k - whole) * narrow, wide if whole == k < 2 * n - 1 else narrow)

    def out_chunk(k):
        wide = out_columns(k)

        def body(parity):
            store_part(outs[k], parity, dot(act_l[half_of(parity), :], down_full[:, wide]))

        loop(2, body)
        outs[k].begin()

    def lh_early():
        blocks = [column_block(k) for k in range(n - 1)] + [tail_columns(0)]

        def body(i):
            at = pl.ds(pl.multiple_of(i * slope_rows, slope_rows), slope_rows)
            total = dot(x_all[at, blocks[0]], up_full[blocks[0], :])
            for wide in blocks[1:]:
                total = total + dot(x_all[at, wide], up_full[wide, :])
            lh_sum[at, :] = total

        loop(2 * group // slope_rows, body)

    def lh_late(parity):
        wide = tail_columns(1)

        def body(i):
            base = pl.multiple_of(i * slope_rows, slope_rows)
            at = pl.ds(pl.multiple_of(parity * group + base, slope_rows), slope_rows)
            h = (lh_sum[at, :] + dot(x_all[at, wide], up_full[wide, :])).astype(BF16)
            act_l[at, :] = squared(h)
            return base, at, h

        def away(i):
            _, at, h = body(i)
            lh[pl.ds(pl.multiple_of(i * slope_rows, slope_rows), slope_rows), :] = h

        def home(i):
            base, _, h = body(i)
            for j in range(n):
                lh_o[pl.ds(base, slope_rows), cols(j, y)] = h[:, j * hb : (j + 1) * hb]

        return away, home

    def lh_away():
        loop(group // slope_rows, lh_late(1 - y)[0])

    def lh_home():
        loop(group // slope_rows, lh_late(y)[1])

    def first_sends():
        own_c[0].wait()
        start(*c_y)
        own_down.wait()
        for p in (0, 1):
            downs.begin(p)
        start(h_y[0], *up_y, *h_y[1:], *e_y, *x_y, x_own_x, x_own_c)
        for copy in own_up:
            copy.wait()
        ups.begin_at(0, 0)

    def relay(sums, m):
        for p in (0, 1):
            sums.relay(m, p)

    def own_act():
        for copy in own_h:
            copy.wait()
        for i in range(n):
            activate(y, i)

    def all_c():
        together(c_all.at[pl.ds(0, 2 * block)], c_slot)
        for copy in own_c[1:]:
            copy.wait()

    def all_e():
        together(e_all.at[pl.ds(0, 2 * block)], e_slot)
        own_e.wait()

    def all_x():
        together(x_all.at[pl.ds(0, 4 * block)], x_slot)
        own_x.wait()

    def pass_on(came, *onward):
        arrive(came)
        start(*onward)

    def lh_send():
        start(*lh_y)

    def gd_oal():
        own_down_sum.wait()
        for p in (0, 1):
            rows = pl.ds(pl.multiple_of(gds.half(p), hb // 2), hb // 2)
            gd_o[rows, :] = gd_o[rows, :] + scale * gds.total(p)

    def gu_away():
        swap_out[...] = gus.total(0).astype(BF16)
        start(swap)

    def gu_home():
        own_up_sum.wait()
        total = gus.total(1)
        for i in range(n):
            kept = total[:, i * hb : (i + 1) * hb]
            gu_o[:, cols(i, y)] = gu_o[:, cols(i, y)] + scale * kept

    def gu_store():
        arrive(swap)
        for i in range(n):
            came = swap_in[:, strip(i)].astype(F32)
            gu_o[:, cols(i, 1 - y)] = gu_o[:, cols(i, 1 - y)] + scale * came

    def eg_store():
        for k in range(n - 1):
            egs[k].last(eg_o, column_block(k))
        for p in (0, 1):
            tails[p].last(eg_o, tail_columns(p))

    def out_last(k):
        outs[k].last(out_o, out_columns(k))

    def close():
        together(lh_o.at[:, pl.ds(0, half)], lh_slot)
        wire.drain()
        assert wire.n_remote == recv.shape[0] and wire.n_local == local.shape[0]

    def do(name, act, *args):
        with jax.named_scope(name):
            act(*args)

    last = n - 1
    do("first", first_sends)
    do("own_act", own_act)
    do("c_y0", pass_on, c_y[0], c_x[0], c_c[0])
    do("down10", downs.forward, 1, 0)
    do("c_y1", pass_on, c_y[1], c_x[1], c_c[1])
    do("down11", downs.forward, 1, 1)
    ups.begin_at(1, 0)
    do("x_own_x", pass_on, x_own_x, x_own_xc)
    do("up_y", together, up_full.at[pl.ds(0, up_rows)], up_slot)
    for stage in (0, 1):
        ups.begin_at(stage, 1)
    for r in range(2, last):
        do("down20", downs.forward, r, 0)
    for i in (0, 1):
        do("c_x", pass_on, c_x[i], c_xc[i])
    for r in range(2, last):
        do("down21", downs.forward, r, 1)
        for p in (0, 1):
            ups.begin_at(r, p)
    do("h_y0", arrive, h_y[0])
    do("act2", activate, 1 - y, 0)
    do("c_all", all_c)
    do("gd_far", gd_dots, far * hb, hb)
    wire.settle([*c_y, *c_x, *c_c, *c_xc, *up_y, h_y[0], x_own_x, x_own_c, x_own_xc])
    wire.settle([hop for p in (0, 1) for hop in (downs.right[1, p], downs.left[1, p])])
    gds.seeds([n - 2])
    do("h_y", together, h_all.at[pl.ds(0, group), pl.ds(0, half - hb)], h_slot)
    for i in range(1, n):
        do("act2", activate, 1 - y, i)
    for p in (0, 1):
        do("ups1e", ups.forward, 1, p, True)
    do("gd_dots", gd_dots, jnp.where(far == 0, hb, 0), half - hb)
    do("gd_seed", gds.seeds, range(n - 3, 0, -1))
    do("e_y0", pass_on, e_y[0], e_x[0], e_c[0])
    for p in (0, 1):
        do("ups1", ups.forward, 1, p, False)
    for r in range(1, n):
        do("down_end", downs.ends, r)
    do("pg", pg_dots)
    wire.settle([*downs.right.values(), *downs.left.values(), *h_y])
    do("e_y1", pass_on, e_y[1], e_x[1], e_c[1])
    do("eg0", eg_chunk, 0)
    do("e_x0", pass_on, e_x[0], e_xc[0])
    do("eg0_b", egs[0].second)
    for m in range(n - 3, 0, -1):
        do("gd_relay", relay, gds, m)
    do("x_y0", pass_on, x_y[0], x_x[0], x_c[0])
    do("e_x1", pass_on, e_x[1], e_xc[1])
    do("e_all", all_e)
    do("gu_dots", gu_dots)
    wire.settle([*e_y, *e_x, *e_c, *e_xc, egs[0].a])
    wire.settle([hop for p in (0, 1) for hop in (ups.right[1, p], ups.left[1, p])])
    do("gu_seed", gus.seeds, range(n - 2, -1, -1))
    do("x_y1", pass_on, x_y[1], x_x[1], x_c[1])
    do("up1_end", ups.ends, 1)
    do("eg1", eg_chunk, 1)
    for r in range(2, last):
        for p in (0, 1):
            do("ups2", ups.forward, r, p)
    do("eg1_b", egs[1].second)
    do("eg0_c", egs[0].third)
    do("gd_relay0", relay, gds, 0)
    for r in range(2, last):
        do("up2_end", ups.ends, r)
        do("eg2", eg_chunk, r)
    for r in range(2, last):
        do("eg2_b", egs[r].second)
    do("eg1_c", egs[1].third)
    for i in (0, 1):
        do("x_x", pass_on, x_x[i], x_xc[i])
    for m in range(n - 3, 0, -1):
        do("gu_relay_0", gus.relay, m, 0)
    do("up3_0", ups.ends, last, (0,))
    do("eg3_0", tail_chunk, 0)
    do("x_all", all_x)
    do("eg3_0b", tails[0].second)
    do("lh_early", lh_early)
    wire.settle([*e_y, *e_x, *e_c, *e_xc, *x_y, *x_x, *x_c, *x_xc, *gds.seed.values()])
    wire.settle([h for r in range(1, last) for p in (0, 1) for h in (ups.right[r, p], ups.left[r, p])])
    wire.settle([h for plane in egs[:last - 1] for h in (plane.a, plane.b)])
    for m in range(n - 3, 0, -1):
        do("gu_relay_1", gus.relay, m, 1)
    for r in range(2, last):
        do("eg2_c", egs[r].third)
    do("up3_1", ups.ends, last, (1,))
    do("lh_away", lh_away)
    do("lh_send", lh_send)
    do("eg3_1", tail_chunk, 1)
    do("lh_home", lh_home)
    do("eg3_1b", tails[1].second)
    do("out0", out_chunk, 0)
    pieces = len(outs)
    for k in range(1, pieces):
        do("out", out_chunk, k)
        do("out_b", outs[k - 1].second)
        wire.settle([tails[0].a, tails[1].a, *(plane.a for plane in outs[: k - 1])])
    do("out_b", outs[pieces - 1].second)
    gds.seeds([0])
    for p in (0, 1):
        do("eg3_c", tails[p].third)
    do("out_c", outs[0].third)
    do("gu_relay0", relay, gus, 0)
    for k in range(1, n - 1):
        do("out_c", outs[k].third)
    wire.settle([*ups.right.values(), *ups.left.values(), *(h for e in egs for h in (e.a, e.b, e.c))])
    wire.settle([gus.seed[w, m, p] for w in (0, 1) for m in range(1, n - 1) for p in (0, 1)])
    wire.settle([tails[0].b, tails[1].b, outs[0].b, outs[1].b, *gds.pass_on.values()])
    do("gu_away", gu_away)
    do("eg_fin", eg_store)
    for k in range(n - 1, n + 2):
        do("out_c", outs[k].third)
    do("gu_home", gu_home)
    for k in range(n + 2, pieces):
        do("out_c", outs[k].third)
        do("out_last", out_last, k - n - 2)
    for k in range(pieces - n - 2, n):
        do("out_last", out_last, k)
    do("gu_sto", gu_store)
    do("gd_o", gd_oal)
    for k in range(n, pieces):
        do("out_last", out_last, k)
    do("close", close)


def fused(n, later_in, earlier_in, hidden, cot, up, down, up_sum, down_sum):
    group, width = earlier_in.shape
    block, hb, up_rows = later_in.shape[0], down.shape[0], up.shape[0]
    half, tokens, chunk = n * hb, 2 * group, 2 * up_rows
    any_space = pl.BlockSpec(memory_space=pl.ANY)
    vm = pltpu.VMEM
    results = (
        vm(later_in.shape, BF16), vm(hidden.shape, BF16), vm(later_in.shape, BF16),
        vm(up.shape, F32), vm(down.shape, F32),
    )

    def plane(count, columns):
        leading = (2, 2, 2), (2, 2), (2,), (2,), (), ()
        return [vm((count, *lead, block, columns), BF16) for lead in leading]

    scratch = [
        vm((tokens, width), BF16), vm((tokens, width), BF16), vm((tokens, width), BF16),
        vm((tokens, half), BF16), vm((half, tokens), BF16), vm((tokens, half), BF16),
        vm((width, half), BF16), vm((half, width), BF16),
        vm((half, width), BF16), vm((width, half), BF16),
        vm((2, n - 1, hb, width), BF16), vm((2, max(n - 2, 1), hb, width), BF16),
        vm((2, n - 1, chunk, half), BF16), vm((2, max(n - 2, 1), chunk, half), BF16),
        vm((up_rows, half), BF16), vm((up_rows, half), BF16),
        vm((group, half), BF16), vm((tokens, half), BF16), vm((tokens, half), F32),
        *plane(n - 1, chunk), *plane(2, chunk // 2), *plane(2 * n - 1, chunk // 2),
        *plane(2, chunk // 4),
    ]
    remote_copies = 19 * (n - 1) + 6 * n + 30
    local_copies = 2 * n + 9
    return pl.pallas_call(
        functools.partial(layer, n),
        out_shape=results,
        in_specs=[any_space] * 8,
        out_specs=(pl.BlockSpec(memory_space=vm),) * 5,
        scratch_shapes=scratch + [
            pltpu.SemaphoreType.DMA((SENDS,)),
            pltpu.SemaphoreType.DMA((remote_copies,)),
            pltpu.SemaphoreType.DMA((local_copies,)),
        ],
        compiler_params=pltpu.CompilerParams(
            collective_id=0, has_side_effects=True, vmem_limit_bytes=VMEM_BYTES
        ),
        name="layer",
    )(later_in, earlier_in, hidden, cot, up, down, up_sum, down_sum)


def hand_on(*refs):
    count = (len(refs) - 1) // 2
    sources, results, gone = refs[:count], refs[count : 2 * count], refs[-1]
    copies = [
        pltpu.make_async_copy(source, result, gone.at[i])
        for i, (source, result) in enumerate(zip(sources, results))
    ]
    for copy in copies:
        copy.start()
    for copy in copies:
        copy.wait()


def handed_on(arrays):
    count = len(arrays)
    held = [pltpu.with_memory_space_constraint(a, pltpu.VMEM) for a in arrays]
    return pl.pallas_call(
        hand_on,
        out_shape=tuple(pltpu.HBM(a.shape, a.dtype) for a in arrays),
        in_specs=[pl.BlockSpec(memory_space=pltpu.VMEM)] * count,
        out_specs=(pl.BlockSpec(memory_space=pltpu.HBM),) * count,
        scratch_shapes=[pltpu.SemaphoreType.DMA((count,))],
        compiler_params=pltpu.CompilerParams(vmem_limit_bytes=1 << 20),
        name="hand_on",
    )(*held)


def portable(n_fs, later_in, earlier_in, hidden, cot, up, down, up_sum, down_sum):
    def split_sum(partial, axis):
        return lax.psum_scatter(partial.astype(F32), axis, scatter_dimension=0, tiled=True)

    up_full = lax.all_gather(up, "fs", axis=0, tiled=True)
    down_full = lax.all_gather(down, "fs", axis=0, tiled=True)
    rows = lax.all_gather(later_in, "tp", axis=0, tiled=True)
    lifted = jnp.maximum(hidden.astype(F32), 0.0)
    gd = split_sum(dot(squared(hidden), cot, 0, 0), "fs")
    pre = (2.0 * dot(cot, down_full, 1, 1) * lifted).astype(BF16)
    gu = split_sum(dot(earlier_in, pre, 0, 0), "fs")
    eg = split_sum(dot(pre, up_full, 1, 1).astype(BF16), "tp").astype(BF16)
    later_hidden = dot(rows, up_full).astype(BF16)
    out = split_sum(dot(squared(later_hidden), down_full).astype(BF16), "tp").astype(BF16)
    scale = float(earlier_in.shape[0] * n_fs) ** (-0.5)
    return out, later_hidden, eg, up_sum + scale * gu, down_sum + scale * gd


def solution(mesh):
    n_fs, n_tp = mesh.shape["fs"], mesh.shape["tp"]

    def shards(*args):
        later_input, up_weight, down_weight = args[0], args[4], args[5]
        planes = n_fs // 2
        fits = (
            n_tp == 4 and n_fs % 2 == 0 and 2 < planes <= 4
            and down_weight.shape[0] % LANES == 0 and up_weight.shape[0] % LANES == 0
            and later_input.shape[0] % LANES == 0
        )
        return handed_on(fused(planes, *args)) if fits else portable(n_fs, *args)

    in_specs = (
        P(("fs", "tp"), None), P("fs", None), P("fs", "tp"), P("fs", None),
        P("fs", "tp"), P(("tp", "fs"), None), P("fs", "tp"), P(("tp", "fs"), None),
    )
    out_specs = (
        P(("fs", "tp"), None), P("fs", "tp"), P(("fs", "tp"), None),
        P("fs", "tp"), P(("tp", "fs"), None),
    )
    return jax.shard_map(shards, mesh=mesh, in_specs=in_specs, out_specs=out_specs, check_vma=False)
```

```python
import functools

import jax
import jax.numpy as jnp
from jax import lax
from jax.experimental import pallas as pl
from jax.experimental.pallas import tpu as pltpu
from jax.sharding import PartitionSpec as P

F32, BF16 = jnp.float32, jnp.bfloat16
MESH = pl.DeviceIdType.MESH
LANES = 128
VMEM_BYTES = 62_000_000
SENDS = 63


def dot(a, b, ca=1, cb=0):
    return lax.dot_general(a, b, (((ca,), (cb,)), ((), ())), preferred_element_type=F32)


def loop(n, body):
    def step(i, carry):
        body(i)
        return carry

    lax.fori_loop(0, n, step, 0)


def squared(h):
    lifted = jnp.maximum(h.astype(F32), 0.0)
    return (lifted * lifted).astype(BF16)


def both(a, b):
    return jnp.logical_and(a, b)


class Hop:
    def __init__(self, wire, src, dst, device, slot):
        self.wire, self.src, self.dst, self.device, self.slot = wire, src, dst, device, slot

    def made(self, place):
        return pltpu.make_async_remote_copy(
            src_ref=self.src, dst_ref=self.dst, send_sem=self.wire.send.at[place],
            recv_sem=self.wire.recv.at[self.slot], device_id=self.device, device_id_type=MESH,
        )

    def wait_recv(self):
        self.made(0).wait_recv()


class Wire:
    def __init__(self, send, recv, local):
        self.send, self.recv, self.local = send, recv, local
        self.n_remote = self.n_local = 0
        self.busy = [None] * send.shape[0]

    def slot(self):
        self.n_remote += 1
        return self.n_remote - 1

    def remote(self, src, dst, device, slot=None):
        return Hop(self, src, dst, device, self.slot() if slot is None else slot)

    def free(self, place):
        copy, when, _ = self.busy[place]
        if when is None:
            copy.wait_send()
        else:
            pl.when(when)(copy.wait_send)
        self.busy[place] = None

    def settle(self, hops):
        for place, held in enumerate(self.busy):
            if held is not None and held[2] in hops:
                self.free(place)

    def start(self, hop, when=None):
        place = self.busy.index(None)
        copy = hop.made(place)
        if when is None:
            copy.start()
        else:
            pl.when(when)(copy.start)
        self.busy[place] = (copy, when, hop)

    def copy(self, src, dst):
        i = self.n_local
        self.n_local += 1
        made = pltpu.make_async_copy(src, dst, self.local.at[i])
        made.start()
        return made

    def drain(self):
        for place, held in enumerate(self.busy):
            if held is not None:
                self.free(place)


class Line:
    def __init__(self, wire, full, rows, own, swap, z, n, left, right):
        self.wire, self.z, self.n = wire, z, n
        self.right, self.left = {}, {}
        size = rows // 2

        def half(i, p):
            base = lax.rem(i + n, n) * rows + lax.rem(swap + p, 2) * size
            return full.at[pl.ds(pl.multiple_of(base, size), size)]

        for p in (0, 1):
            first = half(z, p)
            if own is not None:
                first = own.at[pl.ds(pl.multiple_of(lax.rem(swap + p, 2) * size, size), size)]
            for r in range(1, n):
                src = first if r == 1 else half(z - r + 1, p)
                self.right[r, p] = wire.remote(src, half(z - r + 1, p), right)
                src = first if r == 1 else half(z + r - 1, p)
                self.left[r, p] = wire.remote(src, half(z + r - 1, p), left)

    def begin(self, p, right=True, left=True):
        self.wire.start(self.right[1, p], both(self.z < self.n - 1, right))
        self.wire.start(self.left[1, p], both(self.z > 0, left))

    def begin_at(self, stage, p):
        self.begin(p, self.z == stage, self.z == self.n - 1 - stage)

    def forward(self, r, p, outer=None):
        z, n = self.z, self.n
        rightward, leftward = both(z >= r, z < n - 1), both(z <= n - 1 - r, z > 0)
        if outer is not None:
            rightward = both(rightward, (z == r) == outer)
            leftward = both(leftward, (z == n - 1 - r) == outer)
        pl.when(rightward)(self.right[r, p].wait_recv)
        self.wire.start(self.right[r + 1, p], rightward)
        pl.when(leftward)(self.left[r, p].wait_recv)
        self.wire.start(self.left[r + 1, p], leftward)

    def ends(self, r, halves=(0, 1)):
        z, n = self.z, self.n
        for p in halves:
            pl.when(both(z >= r, z == n - 1))(self.right[r, p].wait_recv)
            pl.when(both(z <= n - 1 - r, z == 0))(self.left[r, p].wait_recv)


class Sums:
    def __init__(self, wire, part, inbox, relayed, rows, swap, z, n, left, right):
        self.wire, self.part, self.inbox, self.relayed = wire, part, inbox, relayed
        self.rows, self.size, self.swap, self.z, self.n = rows, rows // 2, swap, z, n
        self.seed, self.pass_on = {}, {}
        for way, device in ((0, right), (1, left)):
            for m in range(n - 1):
                for p in (0, 1):
                    slot = wire.slot()
                    at = pl.ds(p * self.size, self.size)
                    dst = inbox.at[way, m, at]
                    src = part.at[self.span(way, m, p)]
                    self.seed[way, m, p] = wire.remote(src, dst, device, slot)
                    if m < n - 2:
                        src = relayed.at[way, m, at]
                        self.pass_on[way, m, p] = wire.remote(src, dst, device, slot)

    def half(self, p):
        return lax.rem(self.swap + p, 2) * self.size

    def span(self, way, m, p):
        ahead = self.z + 1 + m if way == 0 else self.z - 1 - m
        base = lax.rem(ahead + 2 * self.n, self.n) * self.rows + self.half(p)
        return pl.ds(pl.multiple_of(base, self.size), self.size)

    def seeds(self, ms):
        for m in ms:
            for p in (0, 1):
                self.wire.start(self.seed[0, m, p], self.z == 0)
                self.wire.start(self.seed[1, m, p], self.z == self.n - 1)

    def relay(self, m, p):
        z, n = self.z, self.n
        at = pl.ds(p * self.size, self.size)
        for way in (0, 1):
            if way == 0:
                when = both(z >= 1, z + 1 + m <= n - 1)
            else:
                when = both(z <= n - 2, z - 1 - m >= 0)

            def add(way=way):
                self.seed[way, m + 1, p].wait_recv()
                mine = self.part[self.span(way, m, p), :].astype(F32)
                came = self.inbox[way, m + 1, at, :].astype(F32)
                self.relayed[way, m, at, :] = (mine + came).astype(BF16)

            pl.when(when)(add)
            self.wire.start(self.pass_on[way, m, p], when)

    def total(self, p):
        z, n = self.z, self.n
        pl.when(z >= 1)(self.seed[0, 0, p].wait_recv)
        pl.when(z <= n - 2)(self.seed[1, 0, p].wait_recv)
        at = pl.ds(p * self.size, self.size)
        base = z * self.rows + self.half(p)
        mine = self.part[pl.ds(pl.multiple_of(base, self.size), self.size), :].astype(F32)
        first = jnp.where(z >= 1, self.inbox[0, 0, at, :].astype(F32), 0.0)
        second = jnp.where(z <= n - 2, self.inbox[1, 0, at, :].astype(F32), 0.0)
        return mine + first + second


class Plane:
    def __init__(self, wire, bufs, k, at, peers, x_first, slots=None):
        self.part, self.in_a, self.to_b, self.in_b, self.to_c, self.in_c = (b.at[k] for b in bufs)
        self.wire, self.x_first = wire, x_first
        x, y, self.core = at
        self.one, self.two = (x, y) if x_first else (y, x)
        if slots is None:
            slot = [None] * 3
        else:
            slot = [slots[0] + 3 * k + i for i in range(3)]
        self.a = wire.remote(self.part.at[1 - self.core], self.in_a, peers[2], slot[0])
        self.b = wire.remote(self.to_b, self.in_b, peers[0 if x_first else 1], slot[1])
        self.c = wire.remote(self.to_c, self.in_c, peers[1 if x_first else 0], slot[2])

    def pair(self, one, two):
        i, j = (one, two) if self.x_first else (two, one)
        return self.part[self.core, i, j].astype(F32) + self.in_a[i, j].astype(F32)

    def mine(self, two):
        return self.pair(self.one, two) + self.in_b[two].astype(F32)

    def begin(self):
        self.wire.start(self.a)

    def second(self):
        self.a.wait_recv()
        for two in (0, 1):
            self.to_b[two] = self.pair(1 - self.one, two).astype(BF16)
        self.wire.start(self.b)

    def third(self):
        self.b.wait_recv()
        self.to_c[...] = self.mine(1 - self.two).astype(BF16)
        self.wire.start(self.c)

    def last(self, out, columns):
        self.c.wait_recv()
        out[:, columns] = (self.mine(self.two) + self.in_c[...].astype(F32)).astype(BF16)


def layer(
    n, later_in, earlier_in, hidden, cot, up, down, up_sum, down_sum,
    out_o, lh_o, eg_o, gu_o, gd_o,
    c_all, e_all, x_all, h_all, act_t, pg, up_full, down_full, gd_part, gu_part,
    gd_in, gd_relay, gu_in, gu_relay, swap_out, swap_in, lh, act_l, lh_sum,
    *rest,
):
    eg_bufs, tail_bufs, out_bufs, end_bufs = (rest[i : i + 6] for i in range(0, 24, 6))
    send, recv, local = rest[24:]
    fs, tp = lax.axis_index("fs"), lax.axis_index("tp")
    z, y = fs // 2, fs % 2
    x, c = tp // 2, tp % 2
    py, px, pc = (fs + 1 - 2 * y, tp), (fs, tp + 2 - 4 * x), (fs, tp + 1 - 2 * c)
    left, right = (lax.rem(fs + 2 * n - 2, 2 * n), tp), (lax.rem(fs + 2, 2 * n), tp)

    group, width = earlier_in.shape
    block = later_in.shape[0]
    hb = down.shape[0]
    half = n * hb
    up_rows = up.shape[0]
    chunk = 2 * up_rows
    wire = Wire(send, recv, local)

    def cols(i, parity):
        return pl.ds(pl.multiple_of((2 * i + parity) * hb, hb), hb)

    def strip(i):
        return pl.ds(i * hb, hb)

    def rows_of(parity, q):
        return pl.ds(pl.multiple_of(parity * group + q * block, block), block)

    def half_of(parity):
        return pl.ds(pl.multiple_of(parity * group, group), group)

    barrier = pltpu.get_barrier_semaphore()

    def greet(device):
        pl.semaphore_signal(barrier, inc=1, device_id=device, device_id_type=MESH)

    for device in (py, px, pc):
        greet(device)
    pl.when(z > 0)(lambda: greet(left))
    pl.when(z < n - 1)(lambda: greet(right))

    def own_quarter(i):
        q = lax.rem(tp + i, 4)
        src = cot.at[pl.ds(pl.multiple_of(q * block, block), block)]
        return wire.copy(src, c_all.at[rows_of(y, q)])

    own_c = [own_quarter(0)]
    own_down = wire.copy(down, down_full.at[pl.ds(pl.multiple_of(z * hb, hb), hb)])
    own_c += [own_quarter(i) for i in range(1, 4)]
    own_h = [wire.copy(hidden.at[:, cols(i, y)], h_all.at[half_of(y), strip(i)]) for i in range(n)]
    my_rows = pl.ds(pl.multiple_of(fs * up_rows, up_rows), up_rows)
    own_up = [wire.copy(up.at[:, cols(i, y)], up_full.at[my_rows, strip(i)]) for i in range(n)]
    own_e = wire.copy(earlier_in, e_all.at[half_of(y)])
    own_x = wire.copy(later_in, x_all.at[rows_of(y, tp)])
    own_up_sum = wire.copy(up_sum, gu_o)
    own_down_sum = wire.copy(down_sum, gd_o)
    scale = float(group * 2 * n) ** (-0.5)

    pl.semaphore_wait(barrier, 3 + (z > 0).astype(jnp.int32) + (z < n - 1).astype(jnp.int32))

    def together(ref, slot):
        Hop(wire, ref, ref, pc, slot).wait_recv()

    def spread(whole, source, first, parts, shared):
        size = block // parts

        def sub(parity, q, i):
            base = parity * group + q * block + i * size
            return whole.at[pl.ds(pl.multiple_of(base, size), size)]

        made = []
        for i in range(parts):
            there, came = sub(y, tp, i), sub(1 - y, tp, i)
            beside = sub(1 - y, tp + 2 - 4 * x, i)
            src = source.at[pl.ds(pl.multiple_of(first + i * size, size), size)]
            made.append((
                wire.remote(src, there, py), wire.remote(came, came, px),
                wire.remote(came, came, pc, shared), wire.remote(beside, beside, pc, shared),
            ))
        return zip(*made)

    downs = Line(wire, down_full, hb, None, y, z, n, left, right)
    ups = Line(wire, up_full, chunk, None, y, z, n, left, right)
    c_slot, e_slot, x_slot, up_slot, h_slot, lh_slot = (wire.slot() for _ in range(6))
    c_y, c_x, c_c, c_xc = spread(c_all, c_all, y * group + tp * block, 2, c_slot)
    e_y, e_x, e_c, e_xc = spread(e_all, earlier_in, tp * block, 2, e_slot)
    x_y, x_x, x_c, x_xc = spread(x_all, later_in, 0, 2, x_slot)
    mine_x = x_all.at[rows_of(y, tp)]
    beside_x = x_all.at[rows_of(y, tp + 2 - 4 * x)]
    x_own_x = wire.remote(later_in, mine_x, px)
    x_own_c = wire.remote(later_in, mine_x, pc, x_slot)
    x_own_xc = wire.remote(beside_x, beside_x, pc, x_slot)
    up_y = [
        wire.remote(up.at[:, cols(i, 1 - y)], up_full.at[my_rows, strip(i)], py, up_slot)
        for i in range(n)
    ]
    far = jnp.where(z < n // 2, n - 1, 0)
    strips = [lax.rem(far + i, n) for i in range(n)]

    def strip_at(i):
        return pl.ds(pl.multiple_of(strips[i] * hb, hb), hb)

    h_y = [
        wire.remote(
            hidden.at[:, cols(strips[i], 1 - y)], h_all.at[half_of(y), strip_at(i)], py,
            h_slot if i else None,
        )
        for i in range(n)
    ]

    gds = Sums(wire, gd_part, gd_in, gd_relay, hb, 1 - y, z, n, left, right)
    gus = Sums(wire, gu_part, gu_in, gu_relay, chunk, 1 - y, z, n, left, right)
    at, peers = (x, y, c), (px, py, pc)
    egs = [Plane(wire, eg_bufs, k, at, peers, False) for k in range(n - 1)]
    slots = [wire.slot() for _ in range(6)]
    tails = [
        Plane(wire, tail_bufs, lax.rem(y + p, 2), at, peers, True, slots) for p in (0, 1)
    ]
    outs = [Plane(wire, out_bufs, k, at, peers, True) for k in range(2 * n - 1)]
    outs += [Plane(wire, end_bufs, k, at, peers, True) for k in range(2)]
    tile = min(256, chunk)
    slope_rows = min(256, 2 * group)
    lh_y = [
        wire.remote(lh.at[:, strip(i)], lh_o.at[:, cols(i, y)], py, lh_slot) for i in range(n)
    ]
    swap = wire.remote(swap_out, swap_in, py)

    def start(*copies):
        for copy in copies:
            wire.start(copy)

    def arrive(*copies):
        for copy in copies:
            copy.wait_recv()

    def activate(parity, i):
        def body(j):
            rows = rows_of(parity, j)
            act_t[strip_at(i), rows] = squared(h_all[rows, strip_at(i)]).T

        loop(group // block, body)

    def column_block(k):
        where = 0
        for i in range(n):
            order = sorted(range(n), key=lambda b: (abs(b - i), b))
            where = where + jnp.where(z == i, order[k], 0)
        return pl.ds(pl.multiple_of(where * chunk, chunk), chunk)

    def store_part(plane, parity, value):
        for q in range(4):
            plane.part[q % 2, q // 2, parity] = value[q * block : (q + 1) * block].astype(BF16)

    def gd_dots(row, size):
        rows = pl.ds(pl.multiple_of(row, hb), size)

        def body(i):
            columns = pl.ds(pl.multiple_of(i * tile, tile), tile)
            gd_part[rows, columns] = dot(act_t[rows, :], c_all[:, columns]).astype(BF16)

        loop(width // tile, body)

    def pg_dots():
        def body(i):
            rows = pl.ds(pl.multiple_of(i * slope_rows, slope_rows), slope_rows)
            lifted = jnp.maximum(h_all[rows, :].astype(F32), 0.0)
            pg[rows, :] = (2.0 * dot(c_all[rows, :], down_full[...], 1, 1) * lifted).astype(BF16)

        loop(2 * group // slope_rows, body)

    def gu_dots():
        def body(i):
            wide = pl.ds(pl.multiple_of(i * tile, tile), tile)
            gu_part[wide, :] = dot(e_all[:, wide], pg[...], 0, 0).astype(BF16)

        loop(width // tile, body)

    def tail_columns(p):
        base = column_block(n - 1).start + lax.rem(y + p, 2) * up_rows
        return pl.ds(pl.multiple_of(base, up_rows), up_rows)

    def tail_chunk(p):
        wide = tail_columns(p)

        def body(parity):
            store_part(tails[p], parity, dot(pg[half_of(parity), :], up_full[wide, :], 1, 1))

        loop(2, body)
        tails[p].begin()

    def eg_chunk(k):
        wide = column_block(k)

        def body(parity):
            store_part(egs[k], parity, dot(pg[half_of(parity), :], up_full[wide, :], 1, 1))

        loop(2, body)
        egs[k].begin()

    def out_columns(k):
        wide, narrow = chunk // 2, chunk // 4
        whole = min(k, 2 * n - 1)
        return pl.ds(whole * wide + (k - whole) * narrow, wide if whole == k < 2 * n - 1 else narrow)

    def out_chunk(k):
        wide = out_columns(k)

        def body(parity):
            store_part(outs[k], parity, dot(act_l[half_of(parity), :], down_full[:, wide]))

        loop(2, body)
        outs[k].begin()

    def lh_early():
        blocks = [column_block(k) for k in range(n - 1)] + [tail_columns(0)]

        def body(i):
            at = pl.ds(pl.multiple_of(i * slope_rows, slope_rows), slope_rows)
            total = dot(x_all[at, blocks[0]], up_full[blocks[0], :])
            for wide in blocks[1:]:
                total = total + dot(x_all[at, wide], up_full[wide, :])
            lh_sum[at, :] = total

        loop(2 * group // slope_rows, body)

    def lh_late(parity):
        wide = tail_columns(1)

        def body(i):
            base = pl.multiple_of(i * slope_rows, slope_rows)
            at = pl.ds(pl.multiple_of(parity * group + base, slope_rows), slope_rows)
            h = (lh_sum[at, :] + dot(x_all[at, wide], up_full[wide, :])).astype(BF16)
            act_l[at, :] = squared(h)
            return base, at, h

        def away(i):
            _, at, h = body(i)
            lh[pl.ds(pl.multiple_of(i * slope_rows, slope_rows), slope_rows), :] = h

        def home(i):
            base, _, h = body(i)
            for j in range(n):
                lh_o[pl.ds(base, slope_rows), cols(j, y)] = h[:, j * hb : (j + 1) * hb]

        return away, home

    def lh_away():
        loop(group // slope_rows, lh_late(1 - y)[0])

    def lh_home():
        loop(group // slope_rows, lh_late(y)[1])

    def first_sends():
        own_c[0].wait()
        start(*c_y)
        own_down.wait()
        for p in (0, 1):
            downs.begin(p)
        start(h_y[0], *up_y, *h_y[1:], *e_y, *x_y, x_own_x, x_own_c)
        for copy in own_up:
            copy.wait()
        ups.begin_at(0, 0)

    def relay(sums, m):
        for p in (0, 1):
            sums.relay(m, p)

    def own_act():
        for copy in own_h:
            copy.wait()
        for i in range(n):
            activate(y, i)

    def all_c():
        together(c_all.at[pl.ds(0, 2 * block)], c_slot)
        for copy in own_c[1:]:
            copy.wait()

    def all_e():
        together(e_all.at[pl.ds(0, 2 * block)], e_slot)
        own_e.wait()

    def all_x():
        together(x_all.at[pl.ds(0, 4 * block)], x_slot)
        own_x.wait()

    def pass_on(came, *onward):
        arrive(came)
        start(*onward)

    def lh_send():
        start(*lh_y)

    def gd_oal():
        own_down_sum.wait()
        for p in (0, 1):
            rows = pl.ds(pl.multiple_of(gds.half(p), hb // 2), hb // 2)
            gd_o[rows, :] = gd_o[rows, :] + scale * gds.total(p)

    def gu_away():
        swap_out[...] = gus.total(0).astype(BF16)
        start(swap)

    def gu_home():
        own_up_sum.wait()
        total = gus.total(1)
        for i in range(n):
            kept = total[:, i * hb : (i + 1) * hb]
            gu_o[:, cols(i, y)] = gu_o[:, cols(i, y)] + scale * kept

    def gu_store():
        arrive(swap)
        for i in range(n):
            came = swap_in[:, strip(i)].astype(F32)
            gu_o[:, cols(i, 1 - y)] = gu_o[:, cols(i, 1 - y)] + scale * came

    def eg_store():
        for k in range(n - 1):
            egs[k].last(eg_o, column_block(k))
        for p in (0, 1):
            tails[p].last(eg_o, tail_columns(p))

    def out_last(k):
        outs[k].last(out_o, out_columns(k))

    def close():
        together(lh_o.at[:, pl.ds(0, half)], lh_slot)
        wire.drain()
        assert wire.n_remote == recv.shape[0] and wire.n_local == local.shape[0]

    def do(name, act, *args):
        with jax.named_scope(name):
            act(*args)

    last = n - 1
    do("first", first_sends)
    do("own_act", own_act)
    do("c_y0", pass_on, c_y[0], c_x[0], c_c[0])
    do("down10", downs.forward, 1, 0)
    do("c_y1", pass_on, c_y[1], c_x[1], c_c[1])
    do("down11", downs.forward, 1, 1)
    ups.begin_at(1, 0)
    do("x_own_x", pass_on, x_own_x, x_own_xc)
    do("up_y", together, up_full.at[pl.ds(0, up_rows)], up_slot)
    for stage in (0, 1):
        ups.begin_at(stage, 1)
    for r in range(2, last):
        do("down20", downs.forward, r, 0)
    for i in (0, 1):
        do("c_x", pass_on, c_x[i], c_xc[i])
    for r in range(2, last):
        do("down21", downs.forward, r, 1)
        for p in (0, 1):
            ups.begin_at(r, p)
    do("h_y0", arrive, h_y[0])
    do("act2", activate, 1 - y, 0)
    do("c_all", all_c)
    do("gd_far", gd_dots, far * hb, hb)
    wire.settle([*c_y, *c_x, *c_c, *c_xc, *up_y, h_y[0], x_own_x, x_own_c, x_own_xc])
    wire.settle([hop for p in (0, 1) for hop in (downs.right[1, p], downs.left[1, p])])
    gds.seeds([n - 2])
    do("h_y", together, h_all.at[pl.ds(0, group), pl.ds(0, half - hb)], h_slot)
    for i in range(1, n):
        do("act2", activate, 1 - y, i)
    for p in (0, 1):
        do("ups1e", ups.forward, 1, p, True)
    do("gd_dots", gd_dots, jnp.where(far == 0, hb, 0), half - hb)
    do("gd_seed", gds.seeds, range(n - 3, 0, -1))
    do("e_y0", pass_on, e_y[0], e_x[0], e_c[0])
    for p in (0, 1):
        do("ups1", ups.forward, 1, p, False)
    for r in range(1, n):
        do("down_end", downs.ends, r)
    do("pg", pg_dots)
    wire.settle([*downs.right.values(), *downs.left.values(), *h_y])
    do("e_y1", pass_on, e_y[1], e_x[1], e_c[1])
    do("eg0", eg_chunk, 0)
    do("e_x0", pass_on, e_x[0], e_xc[0])
    do("eg0_b", egs[0].second)
    for m in range(n - 3, 0, -1):
        do("gd_relay", relay, gds, m)
    do("x_y0", pass_on, x_y[0], x_x[0], x_c[0])
    do("e_x1", pass_on, e_x[1], e_xc[1])
    do("e_all", all_e)
    do("gu_dots", gu_dots)
    wire.settle([*e_y, *e_x, *e_c, *e_xc, egs[0].a])
    wire.settle([hop for p in (0, 1) for hop in (ups.right[1, p], ups.left[1, p])])
    do("gu_seed", gus.seeds, range(n - 2, -1, -1))
    do("x_y1", pass_on, x_y[1], x_x[1], x_c[1])
    do("up1_end", ups.ends, 1)
    do("eg1", eg_chunk, 1)
    for r in range(2, last):
        for p in (0, 1):
            do("ups2", ups.forward, r, p)
    do("eg1_b", egs[1].second)
    do("eg0_c", egs[0].third)
    do("gd_relay0", relay, gds, 0)
    for r in range(2, last):
        do("up2_end", ups.ends, r)
        do("eg2", eg_chunk, r)
    for r in range(2, last):
        do("eg2_b", egs[r].second)
    do("eg1_c", egs[1].third)
    for i in (0, 1):
        do("x_x", pass_on, x_x[i], x_xc[i])
    for m in range(n - 3, 0, -1):
        do("gu_relay_0", gus.relay, m, 0)
    do("up3_0", ups.ends, last, (0,))
    do("eg3_0", tail_chunk, 0)
    do("x_all", all_x)
    do("eg3_0b", tails[0].second)
    do("lh_early", lh_early)
    wire.settle([*e_y, *e_x, *e_c, *e_xc, *x_y, *x_x, *x_c, *x_xc, *gds.seed.values()])
    wire.settle([h for r in range(1, last) for p in (0, 1) for h in (ups.right[r, p], ups.left[r, p])])
    wire.settle([h for plane in egs[:last - 1] for h in (plane.a, plane.b)])
    for m in range(n - 3, 0, -1):
        do("gu_relay_1", gus.relay, m, 1)
    do("up3_1", ups.ends, last, (1,))
    do("lh_away", lh_away)
    do("lh_send", lh_send)
    for r in range(2, last):
        do("eg2_c", egs[r].third)
    do("eg3_1", tail_chunk, 1)
    do("lh_home", lh_home)
    do("eg3_1b", tails[1].second)
    do("out0", out_chunk, 0)
    pieces = len(outs)
    for k in range(1, pieces):
        do("out", out_chunk, k)
        do("out_b", outs[k - 1].second)
        wire.settle([tails[0].a, tails[1].a, *(plane.a for plane in outs[: k - 1])])
    do("out_b", outs[pieces - 1].second)
    gds.seeds([0])
    for p in (0, 1):
        do("eg3_c", tails[p].third)
    do("out_c", outs[0].third)
    do("gu_relay0", relay, gus, 0)
    for k in range(1, n - 1):
        do("out_c", outs[k].third)
    wire.settle([*ups.right.values(), *ups.left.values(), *(h for e in egs for h in (e.a, e.b, e.c))])
    wire.settle([gus.seed[w, m, p] for w in (0, 1) for m in range(1, n - 1) for p in (0, 1)])
    wire.settle([tails[0].b, tails[1].b, outs[0].b, outs[1].b, *gds.pass_on.values()])
    do("gu_away", gu_away)
    do("eg_fin", eg_store)
    for k in range(n - 1, n + 2):
        do("out_c", outs[k].third)
    do("gu_home", gu_home)
    for k in range(n + 2, pieces):
        do("out_c", outs[k].third)
        do("out_last", out_last, k - n - 2)
    for k in range(pieces - n - 2, n):
        do("out_last", out_last, k)
    do("gu_sto", gu_store)
    do("gd_o", gd_oal)
    for k in range(n, pieces):
        do("out_last", out_last, k)
    do("close", close)


def fused(n, later_in, earlier_in, hidden, cot, up, down, up_sum, down_sum):
    group, width = earlier_in.shape
    block, hb, up_rows = later_in.shape[0], down.shape[0], up.shape[0]
    half, tokens, chunk = n * hb, 2 * group, 2 * up_rows
    any_space = pl.BlockSpec(memory_space=pl.ANY)
    vm = pltpu.VMEM
    results = (
        vm(later_in.shape, BF16), vm(hidden.shape, BF16), vm(later_in.shape, BF16),
        vm(up.shape, F32), vm(down.shape, F32),
    )

    def plane(count, columns):
        leading = (2, 2, 2), (2, 2), (2,), (2,), (), ()
        return [vm((count, *lead, block, columns), BF16) for lead in leading]

    scratch = [
        vm((tokens, width), BF16), vm((tokens, width), BF16), vm((tokens, width), BF16),
        vm((tokens, half), BF16), vm((half, tokens), BF16), vm((tokens, half), BF16),
        vm((width, half), BF16), vm((half, width), BF16),
        vm((half, width), BF16), vm((width, half), BF16),
        vm((2, n - 1, hb, width), BF16), vm((2, max(n - 2, 1), hb, width), BF16),
        vm((2, n - 1, chunk, half), BF16), vm((2, max(n - 2, 1), chunk, half), BF16),
        vm((up_rows, half), BF16), vm((up_rows, half), BF16),
        vm((group, half), BF16), vm((tokens, half), BF16), vm((tokens, half), F32),
        *plane(n - 1, chunk), *plane(2, chunk // 2), *plane(2 * n - 1, chunk // 2),
        *plane(2, chunk // 4),
    ]
    remote_copies = 19 * (n - 1) + 6 * n + 30
    local_copies = 2 * n + 9
    return pl.pallas_call(
        functools.partial(layer, n),
        out_shape=results,
        in_specs=[any_space] * 8,
        out_specs=(pl.BlockSpec(memory_space=vm),) * 5,
        scratch_shapes=scratch + [
            pltpu.SemaphoreType.DMA((SENDS,)),
            pltpu.SemaphoreType.DMA((remote_copies,)),
            pltpu.SemaphoreType.DMA((local_copies,)),
        ],
        compiler_params=pltpu.CompilerParams(
            collective_id=0, has_side_effects=True, vmem_limit_bytes=VMEM_BYTES
        ),
        name="layer",
    )(later_in, earlier_in, hidden, cot, up, down, up_sum, down_sum)


def hand_on(*refs):
    count = (len(refs) - 1) // 2
    sources, results, gone = refs[:count], refs[count : 2 * count], refs[-1]
    copies = [
        pltpu.make_async_copy(source, result, gone.at[i])
        for i, (source, result) in enumerate(zip(sources, results))
    ]
    for copy in copies:
        copy.start()
    for copy in copies:
        copy.wait()


def handed_on(arrays):
    count = len(arrays)
    held = [pltpu.with_memory_space_constraint(a, pltpu.VMEM) for a in arrays]
    return pl.pallas_call(
        hand_on,
        out_shape=tuple(pltpu.HBM(a.shape, a.dtype) for a in arrays),
        in_specs=[pl.BlockSpec(memory_space=pltpu.VMEM)] * count,
        out_specs=(pl.BlockSpec(memory_space=pltpu.HBM),) * count,
        scratch_shapes=[pltpu.SemaphoreType.DMA((count,))],
        compiler_params=pltpu.CompilerParams(vmem_limit_bytes=1 << 20),
        name="hand_on",
    )(*held)


def portable(n_fs, later_in, earlier_in, hidden, cot, up, down, up_sum, down_sum):
    def split_sum(partial, axis):
        return lax.psum_scatter(partial.astype(F32), axis, scatter_dimension=0, tiled=True)

    up_full = lax.all_gather(up, "fs", axis=0, tiled=True)
    down_full = lax.all_gather(down, "fs", axis=0, tiled=True)
    rows = lax.all_gather(later_in, "tp", axis=0, tiled=True)
    lifted = jnp.maximum(hidden.astype(F32), 0.0)
    gd = split_sum(dot(squared(hidden), cot, 0, 0), "fs")
    pre = (2.0 * dot(cot, down_full, 1, 1) * lifted).astype(BF16)
    gu = split_sum(dot(earlier_in, pre, 0, 0), "fs")
    eg = split_sum(dot(pre, up_full, 1, 1).astype(BF16), "tp").astype(BF16)
    later_hidden = dot(rows, up_full).astype(BF16)
    out = split_sum(dot(squared(later_hidden), down_full).astype(BF16), "tp").astype(BF16)
    scale = float(earlier_in.shape[0] * n_fs) ** (-0.5)
    return out, later_hidden, eg, up_sum + scale * gu, down_sum + scale * gd


def solution(mesh):
    n_fs, n_tp = mesh.shape["fs"], mesh.shape["tp"]

    def shards(*args):
        later_input, up_weight, down_weight = args[0], args[4], args[5]
        planes = n_fs // 2
        fits = (
            n_tp == 4 and n_fs % 2 == 0 and 2 < planes <= 4
            and down_weight.shape[0] % LANES == 0 and up_weight.shape[0] % LANES == 0
            and later_input.shape[0] % LANES == 0
        )
        return handed_on(fused(planes, *args)) if fits else portable(n_fs, *args)

    in_specs = (
        P(("fs", "tp"), None), P("fs", None), P("fs", "tp"), P("fs", None),
        P("fs", "tp"), P(("tp", "fs"), None), P("fs", "tp"), P(("tp", "fs"), None),
    )
    out_specs = (
        P(("fs", "tp"), None), P("fs", "tp"), P(("fs", "tp"), None),
        P("fs", "tp"), P(("tp", "fs"), None),
    )
    return jax.shard_map(shards, mesh=mesh, in_specs=in_specs, out_specs=out_specs, check_vma=False)
```
